32 devices in a mesh: rep: 2 (over x), fs: 8 (over z, y), tp: 2 (over core).
Axes of the slice: x: 2, y: 2, z: 4, core: 2. Of those that a mesh axis runs over, the one named last changes fastest.
Arguments:
- inputs: bfloat16 [4096, 2048], P(('rep', 'fs')), may hold values from -6 to 6
- cotangent: bfloat16 [4096, 2048], P(('rep', 'fs')), may hold values from -0.119628906 to 0.119628906
- up_weight: bfloat16 [2048, 4096], P('fs', 'tp'), may hold values from -0.125 to 0.125
- down_weight: bfloat16 [4096, 2048], P('tp', 'fs'), may hold values from -0.09375 to 0.09375
Outputs:
- grad_inputs: float32 [4096, 2048], P(('rep', 'fs'))
- grad_up: float32 [2048, 4096], P('fs', 'tp')
- grad_down: float32 [4096, 2048], P('tp', 'fs')
- norms_up: float32 [2048], P('fs')
- norms_down: float32 [4096], P('tp')
The draws below stay inside these ranges and needn't reach their ends.
All inputs are finite; a program needn't handle non-finite values.
Results may differ from the reference program's by a relative error of at most 0.0029.
Values may be sent and summed in bfloat16 or wider, within the bound.
A program may use at most 128 MiB of HBM per device.

```python
import jax
import jax.numpy as jnp
from jax import lax

D = 2048
FF = 4096
TOKENS = 4096


def spiked(array, rng, source, target, parts, factor):
    owner, partner = [(jnp.arange(array.shape[dim]) // (array.shape[dim] // parts)).reshape([-1 if axis == dim else 1 for axis in range(array.ndim)]) for dim in (source, target)]
    chosen = jax.random.permutation(rng, parts)[partner]
    strong = (owner == chosen) | (owner == (partner + parts // 2) % parts)
    return jnp.where(strong, factor * array, array)


def block_scale(own_key, shape, pieces, low, largest):
    def one(axis_at, shards_of):
        draws = jax.random.uniform(jax.random.fold_in(jax.random.fold_in(own_key, 6), axis_at), (shards_of,), jnp.float32, low / len(pieces), largest / len(pieces))
        return jnp.repeat(jnp.exp(draws), shape[axis_at] // shards_of).reshape((-1,) + (1,) * (len(shape) - axis_at - 1))

    level = one(*pieces[0])
    for cut in pieces[1:]:
        level = level * one(*cut)
    return level


def gaussian(rng, shape, spread, bound, pieces=(), held_as=jnp.bfloat16):
    array = spread * jax.random.normal(rng, shape, jnp.float32)
    if pieces:
        array = array * block_scale(rng, shape, pieces, -0.22, 0.18)
    return jnp.clip(array, -bound, bound).astype(held_as)


def noise_with(stream_key, shape, scale, bound, split, heavy, held_as=jnp.bfloat16):
    result = scale * jax.random.normal(stream_key, shape, jnp.float32)
    if split:
        result = result * block_scale(stream_key, shape, split, -0.22, 0.18)
    return jnp.clip(spiked(result, jax.random.fold_in(stream_key, 3), *heavy), -bound, bound).astype(held_as)


def setup_inputs(seed: int = 0) -> dict:
    arg_keys = jax.random.split(jax.random.key(seed), 5)
    return {
        "inputs": noise_with(arg_keys[0], (TOKENS, D), 1.0, 6.0, ((0, 16),), (0, 1, 16, 2.0)),
        "cotangent": noise_with(arg_keys[1], (TOKENS, D), 0.02, 0.119628906, ((0, 16),), (0, 1, 16, 2.0)),
        "up_weight": gaussian(arg_keys[2], (D, FF), D ** -0.5, 0.125, ((0, 8), (1, 2))),
        "down_weight": gaussian(arg_keys[3], (FF, D), FF ** -0.5, 0.09375, ((0, 2), (1, 8))),
    }


def contract(left, right, left_dim, right_dim):
    return lax.dot_general(left, right, (((left_dim,), (right_dim,)), ((), ())), preferred_element_type=jnp.float32)


def reference(inputs, cotangent, up_weight, down_weight):
    pre_act = jnp.dot(inputs, up_weight, preferred_element_type=jnp.float32)
    rectified = jnp.maximum(pre_act, 0.0)
    hidden = (rectified * rectified).astype(jnp.bfloat16)
    act_grad = contract(cotangent, down_weight, 1, 1)
    pre_grad = (2.0 * rectified * act_grad).astype(jnp.bfloat16)
    grad_down = contract(hidden, cotangent, 0, 0)
    grad_up = contract(inputs, pre_grad, 0, 0)
    grad_inputs = contract(pre_grad, up_weight, 1, 1)
    norms_up = jnp.sum(grad_up * grad_up, axis=1)
    norms_down = jnp.sum(grad_down * grad_down, axis=1)
    return (grad_inputs, grad_up, grad_down, norms_up, norms_down)
```

```python
import functools

import jax
import jax.numpy as jnp
from jax import lax
from jax.experimental import pallas as pl
from jax.experimental.pallas import tpu as pltpu
from jax.sharding import PartitionSpec as P

NARROW = jnp.bfloat16
CHUNKS = 2


def contract(left, right, left_dim, right_dim):
    return lax.dot_general(
        left, right, (((left_dim,), (right_dim,)), ((), ())), preferred_element_type=jnp.float32
    )


def own_block(blocks, axis, shift=0):
    size = lax.axis_size(axis)
    return lax.dynamic_index_in_dim(
        blocks, lax.rem(lax.axis_index(axis) + shift, size), 0, keepdims=False
    )


def rotate(block, axis, shift):
    size = lax.axis_size(axis)
    return lax.ppermute(block, axis, [(at, (at + shift) % size) for at in range(size)])


def scatter_sum(blocks, axis):
    total = own_block(blocks, axis)
    for shift in range(1, lax.axis_size(axis)):
        sent = own_block(blocks, axis, shift).astype(NARROW)
        total = total + rotate(sent, axis, shift).astype(jnp.float32)
    return total


def gather_blocks(block, axis):
    size = lax.axis_size(axis)
    me = lax.axis_index(axis)
    held = [block] + [rotate(block, axis, shift) for shift in range(1, size)]
    placed = []
    for at in range(size):
        pick = held[0]
        for shift in range(1, size):
            pick = jnp.where(lax.rem(me - at + size, size) == shift, held[shift], pick)
        placed.append(pick)
    return jnp.stack(placed)


def fs_sum(blocks, ahead=None):
    groups = lax.axis_size("fs")
    pair = 2 if groups % 2 == 0 else 1
    far = groups // pair
    me = lax.axis_index("fs")
    blocks = blocks.reshape((far, pair) + blocks.shape[1:])

    def near_block(shift):
        return lax.dynamic_index_in_dim(
            blocks, lax.rem(lax.rem(me, pair) + shift, pair), 1, keepdims=False
        )

    held = near_block(0)
    for shift in range(1, pair):
        perm = [(at, at - at % pair + (at + shift) % pair) for at in range(groups)]
        got = lax.ppermute(near_block(shift).astype(NARROW), "fs", perm)
        held = held + got.astype(jnp.float32)

    if ahead is not None:
        held, ahead = lax.optimization_barrier((held, ahead))

    def far_block(shift):
        return lax.dynamic_index_in_dim(held, lax.rem(me // pair + shift, far), 0, keepdims=False)

    total = far_block(0)
    for shift in range(1, far):
        perm = [(at, (at + shift * pair) % groups) for at in range(groups)]
        got = lax.ppermute(far_block(shift).astype(NARROW), "fs", perm)
        total = total + got.astype(jnp.float32)
    return total, ahead


def exchange(blocks, axis):
    return lax.all_to_all(blocks, axis, 0, 0)


def small_sum(value, axis):
    size = lax.axis_size(axis)
    if size & (size - 1):
        return lax.psum(value, axis)
    bit = 1
    while bit < size:
        value = value + lax.ppermute(value, axis, [(at, at ^ bit) for at in range(size)])
        bit *= 2
    return value


def token_plan(inputs, cotangent, up_weight, down_weight):
    reps, groups, cores = (lax.axis_size(axis) for axis in ("rep", "fs", "tp"))
    rows, width = inputs.shape
    depth, units = up_weight.shape
    mine = units // groups
    part = depth // reps
    half = width // cores

    few = mine // reps
    up = own_block(up_weight.reshape(reps, part, groups, mine).transpose(0, 2, 1, 3), "rep")
    down = own_block(down_weight.reshape(groups, reps, few, depth).transpose(1, 0, 2, 3), "rep")
    both = jnp.concatenate([up, down.reshape(groups, part, mine)], axis=1)
    both = gather_blocks(exchange(both, "fs"), "rep")
    up = both[:, :, :part].transpose(1, 0, 2, 3).reshape(width, mine)
    down = both[:, :, part:].reshape(reps, groups, few, depth)
    down = down.transpose(0, 2, 1, 3).reshape(mine, width)
    tokens = lax.all_gather(
        own_block(inputs.reshape(cores, rows // cores, width), "tp"), ("fs", "tp"), axis=0, tiled=True
    )
    cot = lax.all_gather(
        own_block(cotangent.reshape(cores, rows // cores, width), "tp"), ("fs", "tp"), axis=0, tiled=True
    )

    pre_act = contract(tokens, up, 1, 0)
    act_grad = contract(cot, down, 1, 1)
    rectified = jnp.maximum(pre_act, 0.0)
    hidden = (rectified * rectified).astype(jnp.bfloat16)
    pre_grad = (2.0 * rectified * act_grad).astype(jnp.bfloat16)

    up_rows = up.reshape(cores, half, mine)
    share = contract(pre_grad, own_block(up_rows, "tp"), 1, 1)
    for shift in range(1, cores):
        sent = contract(pre_grad, own_block(up_rows, "tp", shift), 1, 1).astype(NARROW)
        share = share + rotate(sent, "tp", shift).astype(jnp.float32)
    chunks = CHUNKS if half % (128 * CHUNKS) == 0 else 1
    share = share.reshape(groups, rows, half)
    step = half // chunks
    def spread(term):
        term = term.reshape(groups, reps, part, mine).transpose(1, 0, 2, 3)
        return exchange(scatter_sum(term, "rep").astype(NARROW), "fs")

    def whole(term):
        term = gather_blocks(term, "rep")
        return term.transpose(0, 2, 1, 3).reshape(depth, units).astype(jnp.float32)

    spreads = (spread(contract(cot, hidden, 0, 0)), spread(contract(tokens, pre_grad, 0, 0)))
    sums = []
    for at in range(chunks):
        ahead = spreads if at == chunks - 1 else None
        total, ahead = fs_sum(share[:, :, at * step : (at + 1) * step], ahead)
        sums.append(total)
    share = jnp.concatenate(sums, axis=1)
    share = gather_blocks(share, "tp")
    grad_inputs = share.transpose(1, 0, 2).reshape(rows, width)

    down_turned, grad_up = whole(ahead[0]), whole(ahead[1])
    norms_up = small_sum(jnp.sum(grad_up * grad_up, axis=1), "tp")
    norms_down = small_sum(jnp.sum(down_turned * down_turned, axis=0), "fs")
    return (grad_inputs, grad_up, down_turned.T, norms_up, norms_down)


def weight_plan(inputs, cotangent, up_weight, down_weight):
    up_whole = lax.all_gather(up_weight, "fs", axis=0, tiled=True)
    pre_act = jnp.dot(inputs, up_whole, preferred_element_type=jnp.float32)
    act_grad = contract(cotangent, lax.all_gather(down_weight, "fs", axis=1, tiled=True), 1, 1)
    rectified = jnp.maximum(pre_act, 0.0)
    hidden = (rectified * rectified).astype(jnp.bfloat16)
    pre_grad = (2.0 * rectified * act_grad).astype(jnp.bfloat16)
    up_part = lax.psum_scatter(
        contract(inputs, pre_grad, 0, 0), "fs", scatter_dimension=0, tiled=True
    )
    down_part = lax.psum_scatter(
        contract(cotangent, hidden, 0, 0), "fs", scatter_dimension=0, tiled=True
    )
    grad_up, down_turned = lax.psum((up_part, down_part), "rep")
    grad_inputs = lax.psum(contract(pre_grad, up_whole, 1, 1), "tp")
    norms_up = lax.psum(jnp.sum(grad_up * grad_up, axis=1), "tp")
    norms_down = lax.psum(jnp.sum(down_turned * down_turned, axis=0), "fs")
    grad_down = down_turned.T
    return (grad_inputs, grad_up, grad_down, norms_up, norms_down)


MESH = pl.DeviceIdType.MESH
SPLITS = 2


def dot(left, right, left_dim, right_dim):
    return lax.dot_general(
        left, right, (((left_dim,), (right_dim,)), ((), ())), preferred_element_type=jnp.float32
    )


class Slots:
    def __init__(self):
        self.size = 0
        self.base = {}

    def add(self, name, *shape):
        self.base[name] = (self.size, shape)
        count = 1
        for extent in shape:
            count *= extent
        self.size += count

    def at(self, name, *index):
        start, shape = self.base[name]
        place = 0
        for extent, position in zip(shape, index, strict=True):
            place = place * extent + position
        return start + place


def plane_slots(lines, splits):
    sent, got, local = Slots(), Slots(), Slots()
    for table in (sent, got):
        table.add("pair", splits, 2)
        table.add("near_x", 2, 2)
        table.add("near_y", 2, 2)
        table.add("far", 2, 2)
        table.add("core_tokens", 2, 3)
        table.add("core_up", splits, lines)
        table.add("core_pre", splits)
        table.add("spread_y", splits, 2)
        table.add("spread_x", splits, 2, 2)
        table.add("share", 3)
        table.add("core_share")
        table.add("reduce_up", splits, 2, lines)
        table.add("reduce_down", splits, 2, lines)
    sent.add("line_up", splits, 2, 2, lines)
    sent.add("line_down", splits, 2, 2, lines)
    got.add("line", splits, 2, 2, lines)
    local.add("tokens", 2)
    local.add("weights", splits, 2)
    local.add("share")
    local.add("out", 2)
    return sent, got, local


def plane_kernel(
    lines, splits, sent, got, local,
    tokens_hbm, cot_hbm, up_hbm, down_hbm,
    share_out, up_out, down_out,
    tokens, cots, ups, downs, other_up, pre_act, act_grad, pre_grad, other_pre, turned,
    leaving, rising, falling, partial, spread, spread_far, share_leaving, share_got, share_sum,
    send_sems, got_sems, local_sems,
):
    rows, width = tokens_hbm.shape
    depth, units = up_hbm.shape
    mine = units // 4
    step = mine // splits
    wide = 2 * depth
    half = rows // 2
    bit = half // 2
    near = lines // 2
    mid = width // 2

    x = lax.axis_index("rep")
    fs = lax.axis_index("fs")
    core = lax.axis_index("tp")
    z, y = fs // 2, fs % 2
    me = 2 * x + y
    at_x, at_y, at_far = 2 * (1 - x) + y, 2 * x + 1 - y, 2 * (1 - x) + 1 - y
    to_x = (1 - x, fs, core)
    to_y = (x, 2 * z + 1 - y, core)
    to_far = (1 - x, 2 * z + 1 - y, core)
    to_core = (x, fs, 1 - core)
    to_up = (x, fs + 2, core)
    to_down = (x, fs - 2, core)
    has_up, has_down = z < lines - 1, z > 0
    pending = []

    def when(cond, act):
        if cond is None:
            act()
        else:
            pl.when(cond)(act)

    def send(src, dst, sem, to, key, *index, cond=None, got_key=None):
        copy = pltpu.make_async_remote_copy(
            src_ref=src, dst_ref=dst,
            send_sem=send_sems.at[sent.at(key, *index)],
            recv_sem=got_sems.at[got.at(got_key or key, *index)],
            device_id=to, device_id_type=MESH,
        )
        when(cond, copy.start)
        pending.append((cond, copy))

    def arrived(dst, key, *index):
        return pltpu.make_async_remote_copy(
            src_ref=dst, dst_ref=dst, send_sem=send_sems.at[0],
            recv_sem=got_sems.at[got.at(key, *index)],
            device_id=to_core, device_id_type=MESH,
        )

    def fetch(src, dst, key, *index):
        copy = pltpu.make_async_copy(src, dst, local_sems.at[local.at(key, *index)])
        copy.start()
        return copy

    def up_piece(k, line, side):
        return ups.at[k, line, pl.ds(pl.multiple_of(side * depth, depth), depth), :]

    def down_piece(k, line, side):
        return downs.at[k, line, :, pl.ds(pl.multiple_of(side * depth, depth), depth)]

    def piece(w, k, line, side):
        return (up_piece, down_piece)[w](k, line, side)

    def own(w, owner, k):
        at = pl.ds(pl.multiple_of(owner * mine + k * step, step), step)
        return up_hbm.at[:, at] if w == 0 else down_hbm.at[at, :]

    def band(t, owner, first, count):
        return (tokens, cots)[t].at[pl.ds(pl.multiple_of(owner * rows + first, bit), count), :]

    gets = {}
    for k in range(splits):
        for w in range(2):
            gets[k, w] = fetch(own(w, me, k), piece(w, k, z, y), "weights", k, w)
        if k == 0:
            for t, src in ((0, tokens_hbm), (1, cot_hbm)):
                gets[t] = fetch(src, band(t, me, 0, rows), "tokens", t)

    barrier = pltpu.get_barrier_semaphore()
    for to in (to_x, to_y, to_far, to_core):
        pl.semaphore_signal(barrier, inc=1, device_id=to, device_id_type=MESH)

    @pl.when(has_up)
    def _():
        pl.semaphore_signal(barrier, inc=1, device_id=to_up, device_id_type=MESH)

    @pl.when(has_down)
    def _():
        pl.semaphore_signal(barrier, inc=1, device_id=to_down, device_id_type=MESH)

    pl.semaphore_wait(barrier, 4 + has_up.astype(jnp.int32) + has_down.astype(jnp.int32))

    def pair_send(k):
        for w in range(2):
            send(own(w, at_y, k), piece(w, k, z, y), None, to_y, "pair", k, w)

    def line_send(k, side):
        for w in range(2):
            ref = piece(w, k, z, side)
            send(ref, ref, None, to_up, "line_up", k, w, side, z, cond=has_up, got_key="line")
            send(ref, ref, None, to_down, "line_down", k, w, side, z, cond=has_down, got_key="line")

    def pair_wait(k):
        for w in range(2):
            arrived(piece(w, k, z, 1 - y), "pair", k, w).wait_recv()

    first = core * half

    def near_send(t):
        for p in range(2):
            ref = band(t, me, first + p * bit, bit)
            send(ref, ref, None, to_x, "near_x", t, p)
            ref = band(t, me, first + (1 - p) * bit, bit)
            send(ref, ref, None, to_y, "near_y", t, 1 - p)

    def relay(t):
        ref = band(t, at_x, first, bit)
        arrived(ref, "near_x", t, 0).wait_recv()
        send(ref, ref, None, to_y, "far", t, 0)
        ref = band(t, at_y, first + bit, bit)
        arrived(ref, "near_y", t, 1).wait_recv()
        send(ref, ref, None, to_x, "far", t, 1)
        arrived(band(t, at_x, first + bit, bit), "near_x", t, 1).wait_recv()
        arrived(band(t, at_y, first, bit), "near_y", t, 0).wait_recv()
        for i, owner in enumerate((at_x, at_y)):
            ref = band(t, owner, first, half)
            send(ref, ref, None, to_core, "core_tokens", t, i)

    def far_wait(t):
        for p in range(2):
            arrived(band(t, at_far, first + p * bit, bit), "far", t, p).wait_recv()
        ref = band(t, at_far, first, half)
        send(ref, ref, None, to_core, "core_tokens", t, 2)

    def core_wait(t):
        for i, owner in enumerate((at_x, at_y, at_far)):
            arrived(band(t, owner, (1 - core) * half, half), "core_tokens", t, i).wait_recv()

    def core_up_send(k, line, cond):
        other = (1 - core) * near
        inside = jnp.logical_and(line >= other, line < other + near)
        if cond is not None:
            inside = jnp.logical_and(inside, cond)
        send(ups.at[k, line], other_up.at[k, line], None, to_core, "core_up", k, line, cond=inside)

    def from_line(k, line, cond, onward, to, key):
        for w in range(2):
            for side in range(2):
                ref = piece(w, k, line, side)
                when(cond, arrived(ref, "line", k, w, side, line).wait_recv)
                send(
                    ref, ref, None, to, key, k, w, side, line,
                    cond=jnp.logical_and(cond, onward), got_key="line",
                )
        core_up_send(k, line, cond)

    def forward(k, line, fresh):
        cols = pl.ds(pl.multiple_of(line * wide, wide), wide)
        a = dot(tokens[:, cols], ups[k, line], 1, 0)
        pre_act[...] = a if fresh else pre_act[...] + a

    def backward(k, line, fresh):
        cols = pl.ds(pl.multiple_of(line * wide, wide), wide)
        a = dot(cots[:, cols], downs[k, line], 1, 1)
        act_grad[...] = a if fresh else act_grad[...] + a

    def gather_step(k, d, compute):
        below, above = z - d, z + d
        for line, cond, onward, to, key in (
            (below, below >= 0, has_up, to_up, "line_up"),
            (above, above < lines, has_down, to_down, "line_down"),
        ):
            at = lax.rem(line + lines, lines)
            from_line(k, at, cond, onward, to, key)
            if compute:

                @pl.when(cond)
                def _():
                    forward(k, at, False)
                    backward(k, at, False)

    def activate(k):
        def body(i, carry):
            at = pl.ds(pl.multiple_of(i * rows, rows), rows)
            r = jnp.maximum(pre_act[at, :], 0.0)
            g = (2.0 * r * act_grad[at, :]).astype(jnp.bfloat16)
            pre_grad[k, at, :] = g
            turned[k, 0, :, at] = g.T
            turned[k, 1, :, at] = (r * r).astype(jnp.bfloat16).T
            return carry

        lax.fori_loop(0, 4, body, 0)
        send(pre_grad.at[k], other_pre.at[k], None, to_core, "core_pre", k)

    def term(k, w, owner):
        cols = pl.ds(pl.multiple_of(owner * wide, wide), wide)
        return dot(turned[k, w], (tokens, cots)[w][:, cols], 1, 0)

    def reduce_to(k, w, owner, cond, has_in, inbox, in_key, to):
        at = lax.rem(owner + lines, lines)
        box = inbox.at[k, w, at]
        wait = arrived(box, in_key, k, w, at)
        out = leaving.at[k, w, at]

        @pl.when(cond)
        def _():
            partial[...] = term(k, w, at)

            @pl.when(has_in)
            def _():
                wait.wait_recv()
                out[...] = (partial[...] + box[...].astype(jnp.float32)).astype(jnp.bfloat16)

            @pl.when(jnp.logical_not(has_in))
            def _():
                out[...] = partial[...].astype(jnp.bfloat16)

        send(out, box, None, to, in_key, k, w, at, cond=cond)

    def reduce_step(k, w, i):
        reduce_to(k, w, lines - 1 - i, z < lines - 1 - i, has_down, rising, "reduce_up", to_up)
        reduce_to(k, w, i + 0 * z, z > i, has_up, falling, "reduce_down", to_down)

    def reduce_own(k, w):
        partial[...] = term(k, w, z)
        for cond, inbox, key in ((has_down, rising, "reduce_up"), (has_up, falling, "reduce_down")):
            box = inbox.at[k, w, z]
            wait = arrived(box, key, k, w, z)

            @pl.when(cond)
            def _():
                wait.wait_recv()
                partial[...] += box[...].astype(jnp.float32)

        here = spread.at[w, me, k]
        here[...] = partial[:, pl.ds(pl.multiple_of(y * depth, depth), depth)].astype(jnp.bfloat16)
        there = spread_far.at[k, w]
        there[...] = partial[:, pl.ds(pl.multiple_of((1 - y) * depth, depth), depth)].astype(jnp.bfloat16)
        send(there, here, None, to_y, "spread_y", k, w)
        send(here, here, None, to_x, "spread_x", k, w, 0)

    def spread_relay(k, w):
        ref = spread.at[w, at_y, k]
        arrived(ref, "spread_y", k, w).wait_recv()
        send(ref, ref, None, to_x, "spread_x", k, w, 1)

    def spread_wait(k, w):
        arrived(spread.at[w, at_x, k], "spread_x", k, w, 0).wait_recv()
        arrived(spread.at[w, at_far, k], "spread_x", k, w, 1).wait_recv()

    def share_term(owner):
        at = pl.ds(pl.multiple_of(owner * rows, rows), rows)
        parts = []
        for i in range(near):
            line = core * near + i
            total = None
            for k in range(splits):
                for grads, weights in ((pre_grad, ups), (other_pre, other_up)):
                    a = dot(grads[k, at, :], weights[k, line], 1, 1)
                    total = a if total is None else total + a
            parts.append(total)
        return parts

    def share_send():
        for k in range(splits):
            arrived(other_pre.at[k], "core_pre", k).wait_recv()
            for i in range(near):
                line = core * near + i
                arrived(other_up.at[k, line], "core_up", k, line).wait_recv()
        for j, (owner, to) in enumerate(((at_far, to_far), (at_x, to_x), (at_y, to_y))):
            for i, part in enumerate(share_term(owner)):
                share_leaving[j, :, i * wide : (i + 1) * wide] = part.astype(jnp.bfloat16)
            send(share_leaving.at[j], share_got.at[j], None, to, "share", j)
        for i, part in enumerate(share_term(me)):
            share_sum[:, i * wide : (i + 1) * wide] = part

    def share_end():
        for j in range(3):
            arrived(share_got.at[j], "share", j).wait_recv()
            share_sum[...] += share_got[j].astype(jnp.float32)
        place = share_out.at[:, pl.ds(pl.multiple_of(core * mid, mid), mid)]
        send(share_sum, place, None, to_core, "core_share")
        return fetch(share_sum, place, "share")

    pair_send(0)
    for w in range(2):
        gets[0, w].wait()
    line_send(0, y)
    gets[0].wait()
    near_send(0)
    for k in range(1, splits):
        pair_send(k)
    gets[1].wait()
    near_send(1)
    pair_wait(0)
    line_send(0, 1 - y)
    core_up_send(0, z, None)
    for k in range(1, splits):
        for w in range(2):
            gets[k, w].wait()
        line_send(k, y)
    relay(0)
    gather_step(0, 1, False)
    for k in range(1, splits):
        pair_wait(k)
        line_send(k, 1 - y)
        core_up_send(k, z, None)
    far_wait(0)
    relay(1)
    for d in range(2, lines):
        gather_step(0, d, False)
    core_wait(0)
    for i in range(lines):
        forward(0, lax.rem(z + i, lines), i == 0)
    far_wait(1)
    core_wait(1)
    for i in range(lines):
        backward(0, lax.rem(z + i, lines), i == 0)

    for k in range(splits):
        activate(k)
        last = k == splits - 1
        if last:
            share_send()
        steps = [functools.partial(reduce_step, k, w, i) for w in range(2) for i in range(lines - 1)]
        steps.insert(lines, functools.partial(reduce_own, k, 0))
        steps.append(functools.partial(reduce_own, k, 1))
        fills = []
        if not last:
            def begin(k=k):
                forward(k + 1, z, True)
                backward(k + 1, z, True)

            fills = [begin] + [functools.partial(gather_step, k + 1, d, True) for d in range(1, lines)]
        every = max(1, len(steps) // max(1, len(fills)))
        while steps or fills:
            for _ in range(every):
                if steps:
                    steps.pop(0)()
            if fills:
                fills.pop(0)()
        for w in range(2):
            spread_relay(k, w)

    out = share_end()
    for k in range(splits):
        for w in range(2):
            spread_wait(k, w)
    ends = [fetch(spread.at[w], ref, "out", w) for w, ref in enumerate((up_out, down_out))]
    arrived(share_out.at[:, pl.ds(pl.multiple_of((1 - core) * mid, mid), mid)], "core_share").wait_recv()
    for cond, copy in pending:
        when(cond, copy.wait_send)
    out.wait()
    for end in ends:
        end.wait()


def plane_fits(inputs, up_weight, down_weight):
    reps, groups, cores = (lax.axis_size(axis) for axis in ("rep", "fs", "tp"))
    if reps != 2 or cores != 2 or groups % 4:
        return False
    rows, width = inputs.shape
    depth, units = up_weight.shape
    step = units // 4 // SPLITS
    even = rows % 64 == 0 and depth % 128 == 0 and step % 128 == 0 and width == groups * depth
    held = 2 * 4 * rows * width * 2 + 4 * (units // 4) * width * 2
    return even and held <= 16 * 2**20


def plane_plan(inputs, cotangent, up_weight, down_weight):
    groups = lax.axis_size("fs")
    lines, splits = groups // 2, SPLITS
    rows, width = inputs.shape
    depth, units = up_weight.shape
    step = units // 4 // splits
    wide = 2 * depth
    plane = 4 * rows
    sent, got, local = plane_slots(lines, splits)
    narrow, full = jnp.bfloat16, jnp.float32
    anywhere = pl.BlockSpec(memory_space=pl.ANY)
    share, up, down = pl.pallas_call(
        functools.partial(plane_kernel, lines, splits, sent, got, local),
        out_shape=(
            jax.ShapeDtypeStruct((rows, width), full),
            jax.ShapeDtypeStruct((4, splits, step, depth), narrow),
            jax.ShapeDtypeStruct((4, splits, step, depth), narrow),
        ),
        in_specs=[anywhere] * 4,
        out_specs=(anywhere,) * 3,
        scratch_shapes=[
            pltpu.VMEM((plane, width), narrow),
            pltpu.VMEM((plane, width), narrow),
            pltpu.VMEM((splits, lines, wide, step), narrow),
            pltpu.VMEM((splits, lines, step, wide), narrow),
            pltpu.VMEM((splits, lines, wide, step), narrow),
            pltpu.VMEM((plane, step), full),
            pltpu.VMEM((plane, step), full),
            pltpu.VMEM((splits, plane, step), narrow),
            pltpu.VMEM((splits, plane, step), narrow),
            pltpu.VMEM((splits, 2, step, plane), narrow),
            pltpu.VMEM((splits, 2, lines, step, wide), narrow),
            pltpu.VMEM((splits, 2, lines, step, wide), narrow),
            pltpu.VMEM((splits, 2, lines, step, wide), narrow),
            pltpu.VMEM((step, wide), full),
            pltpu.VMEM((2, 4, splits, step, depth), narrow),
            pltpu.VMEM((splits, 2, step, depth), narrow),
            pltpu.VMEM((3, rows, width // 2), narrow),
            pltpu.VMEM((3, rows, width // 2), narrow),
            pltpu.VMEM((rows, width // 2), full),
            pltpu.SemaphoreType.DMA((sent.size,)),
            pltpu.SemaphoreType.DMA((got.size,)),
            pltpu.SemaphoreType.DMA((local.size,)),
        ],
        compiler_params=pltpu.CompilerParams(
            collective_id=0, has_side_effects=True, vmem_limit_bytes=63 * 2**20
        ),
        name="plane",
    )(inputs, cotangent, up_weight, down_weight)
    grad_up = up.reshape(units, depth).T.astype(full)
    grad_down = down.reshape(units, depth).astype(full)
    norms_up = small_sum(jnp.sum(grad_up * grad_up, axis=1), "tp")
    norms_down = small_sum(jnp.sum(grad_down * grad_down, axis=1), "fs")
    return (share, grad_up, grad_down, norms_up, norms_down)


def shards(inputs, cotangent, up_weight, down_weight):
    tokens = inputs.size * lax.axis_size("fs") // lax.axis_size("tp")
    weights = up_weight.size * lax.axis_size("fs")
    plan = token_plan if tokens <= weights else weight_plan
    if plane_fits(inputs, up_weight, down_weight):
        plan = plane_plan
    return plan(inputs, cotangent, up_weight, down_weight)


def solution(mesh):
    return jax.shard_map(
        shards,
        mesh=mesh,
        in_specs=(P(("rep", "fs"), None), P(("rep", "fs"), None), P("fs", "tp"), P("tp", "fs")),
        out_specs=(P(("rep", "fs"), None), P("fs", "tp"), P("tp", "fs"), P("fs"), P("tp")),
        check_vma=False,
    )
```

```python
import functools

import jax
import jax.numpy as jnp
from jax import lax
from jax.experimental import pallas as pl
from jax.experimental.pallas import tpu as pltpu
from jax.sharding import PartitionSpec as P

NARROW = jnp.bfloat16
CHUNKS = 2


def contract(left, right, left_dim, right_dim):
    return lax.dot_general(
        left, right, (((left_dim,), (right_dim,)), ((), ())), preferred_element_type=jnp.float32
    )


def own_block(blocks, axis, shift=0):
    size = lax.axis_size(axis)
    return lax.dynamic_index_in_dim(
        blocks, lax.rem(lax.axis_index(axis) + shift, size), 0, keepdims=False
    )


def rotate(block, axis, shift):
    size = lax.axis_size(axis)
    return lax.ppermute(block, axis, [(at, (at + shift) % size) for at in range(size)])


def scatter_sum(blocks, axis):
    total = own_block(blocks, axis)
    for shift in range(1, lax.axis_size(axis)):
        sent = own_block(blocks, axis, shift).astype(NARROW)
        total = total + rotate(sent, axis, shift).astype(jnp.float32)
    return total


def gather_blocks(block, axis):
    size = lax.axis_size(axis)
    me = lax.axis_index(axis)
    held = [block] + [rotate(block, axis, shift) for shift in range(1, size)]
    placed = []
    for at in range(size):
        pick = held[0]
        for shift in range(1, size):
            pick = jnp.where(lax.rem(me - at + size, size) == shift, held[shift], pick)
        placed.append(pick)
    return jnp.stack(placed)


def fs_sum(blocks, ahead=None):
    groups = lax.axis_size("fs")
    pair = 2 if groups % 2 == 0 else 1
    far = groups // pair
    me = lax.axis_index("fs")
    blocks = blocks.reshape((far, pair) + blocks.shape[1:])

    def near_block(shift):
        return lax.dynamic_index_in_dim(
            blocks, lax.rem(lax.rem(me, pair) + shift, pair), 1, keepdims=False
        )

    held = near_block(0)
    for shift in range(1, pair):
        perm = [(at, at - at % pair + (at + shift) % pair) for at in range(groups)]
        got = lax.ppermute(near_block(shift).astype(NARROW), "fs", perm)
        held = held + got.astype(jnp.float32)

    if ahead is not None:
        held, ahead = lax.optimization_barrier((held, ahead))

    def far_block(shift):
        return lax.dynamic_index_in_dim(held, lax.rem(me // pair + shift, far), 0, keepdims=False)

    total = far_block(0)
    for shift in range(1, far):
        perm = [(at, (at + shift * pair) % groups) for at in range(groups)]
        got = lax.ppermute(far_block(shift).astype(NARROW), "fs", perm)
        total = total + got.astype(jnp.float32)
    return total, ahead


def exchange(blocks, axis):
    return lax.all_to_all(blocks, axis, 0, 0)


def small_sum(value, axis):
    size = lax.axis_size(axis)
    if size & (size - 1):
        return lax.psum(value, axis)
    bit = 1
    while bit < size:
        value = value + lax.ppermute(value, axis, [(at, at ^ bit) for at in range(size)])
        bit *= 2
    return value


def token_plan(inputs, cotangent, up_weight, down_weight):
    reps, groups, cores = (lax.axis_size(axis) for axis in ("rep", "fs", "tp"))
    rows, width = inputs.shape
    depth, units = up_weight.shape
    mine = units // groups
    part = depth // reps
    half = width // cores

    few = mine // reps
    up = own_block(up_weight.reshape(reps, part, groups, mine).transpose(0, 2, 1, 3), "rep")
    down = own_block(down_weight.reshape(groups, reps, few, depth).transpose(1, 0, 2, 3), "rep")
    both = jnp.concatenate([up, down.reshape(groups, part, mine)], axis=1)
    both = gather_blocks(exchange(both, "fs"), "rep")
    up = both[:, :, :part].transpose(1, 0, 2, 3).reshape(width, mine)
    down = both[:, :, part:].reshape(reps, groups, few, depth)
    down = down.transpose(0, 2, 1, 3).reshape(mine, width)
    tokens = lax.all_gather(
        own_block(inputs.reshape(cores, rows // cores, width), "tp"), ("fs", "tp"), axis=0, tiled=True
    )
    cot = lax.all_gather(
        own_block(cotangent.reshape(cores, rows // cores, width), "tp"), ("fs", "tp"), axis=0, tiled=True
    )

    pre_act = contract(tokens, up, 1, 0)
    act_grad = contract(cot, down, 1, 1)
    rectified = jnp.maximum(pre_act, 0.0)
    hidden = (rectified * rectified).astype(jnp.bfloat16)
    pre_grad = (2.0 * rectified * act_grad).astype(jnp.bfloat16)

    up_rows = up.reshape(cores, half, mine)
    share = contract(pre_grad, own_block(up_rows, "tp"), 1, 1)
    for shift in range(1, cores):
        sent = contract(pre_grad, own_block(up_rows, "tp", shift), 1, 1).astype(NARROW)
        share = share + rotate(sent, "tp", shift).astype(jnp.float32)
    chunks = CHUNKS if half % (128 * CHUNKS) == 0 else 1
    share = share.reshape(groups, rows, half)
    step = half // chunks
    def spread(term):
        term = term.reshape(groups, reps, part, mine).transpose(1, 0, 2, 3)
        return exchange(scatter_sum(term, "rep").astype(NARROW), "fs")

    def whole(term):
        term = gather_blocks(term, "rep")
        return term.transpose(0, 2, 1, 3).reshape(depth, units).astype(jnp.float32)

    spreads = (spread(contract(cot, hidden, 0, 0)), spread(contract(tokens, pre_grad, 0, 0)))
    sums = []
    for at in range(chunks):
        ahead = spreads if at == chunks - 1 else None
        total, ahead = fs_sum(share[:, :, at * step : (at + 1) * step], ahead)
        sums.append(total)
    share = jnp.concatenate(sums, axis=1)
    share = gather_blocks(share, "tp")
    grad_inputs = share.transpose(1, 0, 2).reshape(rows, width)

    down_turned, grad_up = whole(ahead[0]), whole(ahead[1])
    norms_up = small_sum(jnp.sum(grad_up * grad_up, axis=1), "tp")
    norms_down = small_sum(jnp.sum(down_turned * down_turned, axis=0), "fs")
    return (grad_inputs, grad_up, down_turned.T, norms_up, norms_down)


def weight_plan(inputs, cotangent, up_weight, down_weight):
    up_whole = lax.all_gather(up_weight, "fs", axis=0, tiled=True)
    pre_act = jnp.dot(inputs, up_whole, preferred_element_type=jnp.float32)
    act_grad = contract(cotangent, lax.all_gather(down_weight, "fs", axis=1, tiled=True), 1, 1)
    rectified = jnp.maximum(pre_act, 0.0)
    hidden = (rectified * rectified).astype(jnp.bfloat16)
    pre_grad = (2.0 * rectified * act_grad).astype(jnp.bfloat16)
    up_part = lax.psum_scatter(
        contract(inputs, pre_grad, 0, 0), "fs", scatter_dimension=0, tiled=True
    )
    down_part = lax.psum_scatter(
        contract(cotangent, hidden, 0, 0), "fs", scatter_dimension=0, tiled=True
    )
    grad_up, down_turned = lax.psum((up_part, down_part), "rep")
    grad_inputs = lax.psum(contract(pre_grad, up_whole, 1, 1), "tp")
    norms_up = lax.psum(jnp.sum(grad_up * grad_up, axis=1), "tp")
    norms_down = lax.psum(jnp.sum(down_turned * down_turned, axis=0), "fs")
    grad_down = down_turned.T
    return (grad_inputs, grad_up, grad_down, norms_up, norms_down)


MESH = pl.DeviceIdType.MESH
SPLITS = 2


def dot(left, right, left_dim, right_dim):
    return lax.dot_general(
        left, right, (((left_dim,), (right_dim,)), ((), ())), preferred_element_type=jnp.float32
    )


class Slots:
    def __init__(self):
        self.size = 0
        self.base = {}

    def add(self, name, *shape):
        self.base[name] = (self.size, shape)
        count = 1
        for extent in shape:
            count *= extent
        self.size += count

    def at(self, name, *index):
        start, shape = self.base[name]
        place = 0
        for extent, position in zip(shape, index, strict=True):
            place = place * extent + position
        return start + place


def plane_slots(lines, splits):
    sent, got, local = Slots(), Slots(), Slots()
    for table in (sent, got):
        table.add("pair", splits, 2)
        table.add("near_x", 2, 2)
        table.add("near_y", 2, 2)
        table.add("far", 2, 2)
        table.add("core_tokens", 2, 3)
        table.add("core_up", splits, lines)
        table.add("core_pre", splits)
        table.add("spread_y", splits, 2)
        table.add("spread_x", splits, 2, 2)
        table.add("share", 3)
        table.add("core_share")
        table.add("reduce", 2, splits, 2, lines)
    sent.add("line_up", splits, 2, 2, lines)
    sent.add("line_down", splits, 2, 2, lines)
    got.add("line", splits, 2, 2, lines)
    local.add("tokens", 2)
    local.add("weights", splits, 2)
    local.add("share")
    local.add("out", 2)
    return sent, got, local


def plane_kernel(
    lines, splits, sent, got, local,
    tokens_hbm, cot_hbm, up_hbm, down_hbm,
    share_out, up_out, down_out,
    acts, ups, downs, other_up, pre_act, act_grad, pre_grad, other_pre, turned,
    leaving, inbox, partial, spread, spread_far, share_leaving, share_got, share_sum,
    send_sems, got_sems, local_sems,
):
    rows, width = tokens_hbm.shape
    depth, units = up_hbm.shape
    mine = units // 4
    step = mine // splits
    wide = 2 * depth
    half = rows // 2
    bit = half // 2
    near = lines // 2
    mid = width // 2

    x = lax.axis_index("rep")
    fs = lax.axis_index("fs")
    core = lax.axis_index("tp")
    z, y = fs // 2, fs % 2
    me = 2 * x + y
    at_x, at_y, at_far = 2 * (1 - x) + y, 2 * x + 1 - y, 2 * (1 - x) + 1 - y
    to_x = (1 - x, fs, core)
    to_y = (x, 2 * z + 1 - y, core)
    to_far = (1 - x, 2 * z + 1 - y, core)
    to_core = (x, fs, 1 - core)
    to_up = (x, fs + 2, core)
    to_down = (x, fs - 2, core)
    has_up, has_down = z < lines - 1, z > 0
    middle = jnp.logical_and(has_up, has_down)
    end = jnp.logical_not(middle)
    pending = []

    def when(cond, act):
        if cond is None:
            act()
        else:
            pl.when(cond)(act)

    def remote(src, dst, to, key, *index, got_key=None):
        return pltpu.make_async_remote_copy(
            src_ref=src, dst_ref=dst,
            send_sem=send_sems.at[sent.at(key, *index)],
            recv_sem=got_sems.at[got.at(got_key or key, *index)],
            device_id=to, device_id_type=MESH,
        )

    def send(src, dst, to, key, *index, cond=None, got_key=None):
        copy = remote(src, dst, to, key, *index, got_key=got_key)
        when(cond, copy.start)
        pending.append((cond, copy))

    def arrived(dst, key, *index):
        return pltpu.make_async_remote_copy(
            src_ref=dst, dst_ref=dst, send_sem=send_sems.at[0],
            recv_sem=got_sems.at[got.at(key, *index)],
            device_id=to_core, device_id_type=MESH,
        )

    def fetch(src, dst, key, *index):
        copy = pltpu.make_async_copy(src, dst, local_sems.at[local.at(key, *index)])
        copy.start()
        return copy

    def up_piece(k, line, side):
        return ups.at[k, line, pl.ds(pl.multiple_of(side * depth, depth), depth), :]

    def down_piece(k, line, side):
        return downs.at[k, line, :, pl.ds(pl.multiple_of(side * depth, depth), depth)]

    def piece(w, k, line, side):
        return (up_piece, down_piece)[w](k, line, side)

    def own(w, owner, k):
        at = pl.ds(pl.multiple_of(owner * mine + k * step, step), step)
        return up_hbm.at[:, at] if w == 0 else down_hbm.at[at, :]

    def band(t, owner, first, count):
        return acts.at[t, pl.ds(pl.multiple_of(owner * rows + first, bit), count), :]

    gets = {}
    for k in range(splits):
        for w in range(2):
            gets[k, w] = fetch(own(w, me, k), piece(w, k, z, y), "weights", k, w)
        if k == 0:
            for t, src in ((0, tokens_hbm), (1, cot_hbm)):
                gets[t] = fetch(src, band(t, me, 0, rows), "tokens", t)

    barrier = pltpu.get_barrier_semaphore()
    for to in (to_x, to_y, to_far, to_core):
        pl.semaphore_signal(barrier, inc=1, device_id=to, device_id_type=MESH)

    @pl.when(has_up)
    def _():
        pl.semaphore_signal(barrier, inc=1, device_id=to_up, device_id_type=MESH)

    @pl.when(has_down)
    def _():
        pl.semaphore_signal(barrier, inc=1, device_id=to_down, device_id_type=MESH)

    pl.semaphore_wait(barrier, 4 + has_up.astype(jnp.int32) + has_down.astype(jnp.int32))

    def pair_send(k):
        for w in range(2):
            send(own(w, at_y, k), piece(w, k, z, y), to_y, "pair", k, w)

    def line_send(k, side, who=None):
        up_cond, down_cond = has_up, has_down
        if who is not None:
            up_cond, down_cond = jnp.logical_and(has_up, who), jnp.logical_and(has_down, who)
        for w in range(2):
            ref = piece(w, k, z, side)
            send(ref, ref, to_up, "line_up", k, w, side, z, cond=up_cond, got_key="line")
            send(ref, ref, to_down, "line_down", k, w, side, z, cond=down_cond, got_key="line")

    def pair_wait(k):
        for w in range(2):
            arrived(piece(w, k, z, 1 - y), "pair", k, w).wait_recv()

    first = core * half

    def near_send(t):
        for p in range(2):
            ref = band(t, me, first + p * bit, bit)
            send(ref, ref, to_x, "near_x", t, p)
            ref = band(t, me, first + (1 - p) * bit, bit)
            send(ref, ref, to_y, "near_y", t, 1 - p)

    def relay(t):
        ref = band(t, at_x, first, bit)
        arrived(ref, "near_x", t, 0).wait_recv()
        send(ref, ref, to_y, "far", t, 0)
        ref = band(t, at_y, first + bit, bit)
        arrived(ref, "near_y", t, 1).wait_recv()
        send(ref, ref, to_x, "far", t, 1)
        arrived(band(t, at_x, first + bit, bit), "near_x", t, 1).wait_recv()
        arrived(band(t, at_y, first, bit), "near_y", t, 0).wait_recv()
        for i, owner in enumerate((at_x, at_y)):
            ref = band(t, owner, first, half)
            send(ref, ref, to_core, "core_tokens", t, i)

    def far_wait(t):
        for p in range(2):
            arrived(band(t, at_far, first + p * bit, bit), "far", t, p).wait_recv()
        ref = band(t, at_far, first, half)
        send(ref, ref, to_core, "core_tokens", t, 2)

    def core_wait(t):
        for i, owner in enumerate((at_x, at_y, at_far)):
            arrived(band(t, owner, (1 - core) * half, half), "core_tokens", t, i).wait_recv()

    def core_up_send(k, line, cond):
        other = (1 - core) * near
        inside = jnp.logical_and(line >= other, line < other + near)
        if cond is not None:
            inside = jnp.logical_and(inside, cond)
        send(ups.at[k, line], other_up.at[k, line], to_core, "core_up", k, line, cond=inside)

    def beside(d):
        below, above = z - d, z + d
        return (
            (lax.rem(below + lines, lines), below >= 0, has_up, to_up, "line_up"),
            (lax.rem(above, lines), above < lines, has_down, to_down, "line_down"),
        )

    def gather_step(k, d, who=None):
        for line, cond, onward, to, key in beside(d):
            if who is not None:
                cond = jnp.logical_and(cond, who)
            for w in range(2):
                for side in range(2):
                    ref = piece(w, k, line, side)
                    when(cond, arrived(ref, "line", k, w, side, line).wait_recv)
                    send(
                        ref, ref, to, key, k, w, side, line,
                        cond=jnp.logical_and(cond, onward), got_key="line",
                    )
            core_up_send(k, line, cond)

    def forward(k, line, fresh):
        cols = pl.ds(pl.multiple_of(line * wide, wide), wide)
        a = dot(acts[0, :, cols], ups[k, line], 1, 0)
        pre_act[...] = a if fresh else pre_act[...] + a

    def backward(k, line, fresh):
        cols = pl.ds(pl.multiple_of(line * wide, wide), wide)
        a = dot(acts[1, :, cols], downs[k, line], 1, 1)
        act_grad[...] = a if fresh else act_grad[...] + a

    def compute_step(k, d):
        for line, cond, _, _, _ in beside(d):

            @pl.when(cond)
            def _():
                forward(k, line, False)
                backward(k, line, False)

    def activate(k):
        def body(i, carry):
            at = pl.ds(pl.multiple_of(i * rows, rows), rows)
            r = jnp.maximum(pre_act[at, :], 0.0)
            g = (2.0 * r * act_grad[at, :]).astype(jnp.bfloat16)
            pre_grad[k, at, :] = g
            turned[k, 0, :, at] = g.T
            turned[k, 1, :, at] = (r * r).astype(jnp.bfloat16).T
            return carry

        lax.fori_loop(0, 4, body, 0)
        send(pre_grad.at[k], other_pre.at[k], to_core, "core_pre", k)

    def term(k, w, owner):
        cols = pl.ds(pl.multiple_of(owner * wide, wide), wide)
        return dot(turned[k, w], acts[w, :, cols], 1, 0)

    def route(k, w, t):
        turn = lax.rem(t // (lines - 1) + z // near, 2)
        j = lax.rem(t, lines - 1)
        owner = (1 - turn) * (lines - 1 - j) + turn * j
        sign = 1 - 2 * turn
        cond = (owner - z) * sign > 0
        source = z - sign
        has_in = jnp.logical_and(source >= 0, source < lines)
        box = inbox.at[turn, k, w, owner]
        out = leaving.at[k, w, owner]
        copy = pltpu.make_async_remote_copy(
            src_ref=out, dst_ref=box,
            send_sem=send_sems.at[sent.at("reduce", turn, k, w, owner)],
            recv_sem=got_sems.at[got.at("reduce", turn, k, w, owner)],
            device_id=(x, fs + 2 * sign, core), device_id_type=MESH,
        )
        return owner, cond, has_in, box, out, copy

    def pieces(k, w):
        def body(t, carry):
            owner, cond, has_in, box, out, copy = route(k, w, t)

            @pl.when(cond)
            def _():
                partial[...] = term(k, w, owner)

                @pl.when(has_in)
                def _():
                    copy.wait_recv()
                    out[...] = (partial[...] + box[...].astype(jnp.float32)).astype(jnp.bfloat16)

                @pl.when(jnp.logical_not(has_in))
                def _():
                    out[...] = partial[...].astype(jnp.bfloat16)

                copy.start()

            return carry

        lax.fori_loop(0, 2 * (lines - 1), body, 0)

    def pieces_end(k, w):
        def body(t, carry):
            _, cond, _, _, _, copy = route(k, w, t)
            pl.when(cond)(copy.wait_send)
            return carry

        lax.fori_loop(0, 2 * (lines - 1), body, 0)

    def spread_copies(k, w):
        here, there, near_ref = spread.at[w, me, k], spread_far.at[k, w], spread.at[w, at_y, k]
        return (
            remote(there, here, to_y, "spread_y", k, w),
            remote(here, here, to_x, "spread_x", k, w, 0),
            remote(near_ref, near_ref, to_x, "spread_x", k, w, 1),
        )

    def reduce_own(k, w):
        partial[...] = term(k, w, z)
        for turn, cond in ((0, has_down), (1, has_up)):
            box = inbox.at[turn, k, w, z]
            wait = arrived(box, "reduce", turn, k, w, z)

            @pl.when(cond)
            def _():
                wait.wait_recv()
                partial[...] += box[...].astype(jnp.float32)

        here, there = spread.at[w, me, k], spread_far.at[k, w]
        there[...] = partial[:, pl.ds(pl.multiple_of((1 - y) * depth, depth), depth)].astype(jnp.bfloat16)
        here[...] = partial[:, pl.ds(pl.multiple_of(y * depth, depth), depth)].astype(jnp.bfloat16)
        to_near, to_side, _ = spread_copies(k, w)
        to_near.start()
        to_side.start()

    def spread_relay(k, w):
        arrived(spread.at[w, at_y, k], "spread_y", k, w).wait_recv()
        spread_copies(k, w)[2].start()

    def spread_wait(k, w):
        arrived(spread.at[w, at_x, k], "spread_x", k, w, 0).wait_recv()
        arrived(spread.at[w, at_far, k], "spread_x", k, w, 1).wait_recv()

    def share_term(owner):
        at = pl.ds(pl.multiple_of(owner * rows, rows), rows)
        parts = []
        for i in range(near):
            line = core * near + i
            total = None
            for k in range(splits):
                for grads, weights in ((pre_grad, ups), (other_pre, other_up)):
                    a = dot(grads[k, at, :], weights[k, line], 1, 1)
                    total = a if total is None else total + a
            parts.append(total)
        return parts

    def share_send():
        for k in range(splits):
            arrived(other_pre.at[k], "core_pre", k).wait_recv()
            for i in range(near):
                line = core * near + i
                arrived(other_up.at[k, line], "core_up", k, line).wait_recv()
        for j, (owner, to) in enumerate(((at_far, to_far), (at_x, to_x), (at_y, to_y))):
            for i, part in enumerate(share_term(owner)):
                share_leaving[j, :, i * wide : (i + 1) * wide] = part.astype(jnp.bfloat16)
            send(share_leaving.at[j], share_got.at[j], to, "share", j)
        for i, part in enumerate(share_term(me)):
            share_sum[:, i * wide : (i + 1) * wide] = part

    def share_end():
        for j in range(3):
            arrived(share_got.at[j], "share", j).wait_recv()
            share_sum[...] += share_got[j].astype(jnp.float32)
        place = share_out.at[:, pl.ds(pl.multiple_of(core * mid, mid), mid)]
        send(share_sum, place, to_core, "core_share")
        return fetch(share_sum, place, "share")

    pair_send(0)
    for w in range(2):
        gets[0, w].wait()
    line_send(0, y)
    for t in range(2):
        gets[t].wait()
        near_send(t)
    pair_wait(0)
    line_send(0, 1 - y)
    core_up_send(0, z, None)
    for k in range(1, splits):
        pair_send(k)
        for w in range(2):
            gets[k, w].wait()
        line_send(k, y, end)
    relay(0)
    gather_step(0, 1)
    for k in range(1, splits):
        pair_wait(k)
        line_send(k, 1 - y, end)
        core_up_send(k, z, None)
    for d in range(2, lines - 1):
        gather_step(0, d)
    relay(1)
    for k in range(1, splits):
        for side in (y, 1 - y):
            line_send(k, side, middle)
    far_wait(0)
    gather_step(0, lines - 1)
    core_wait(0)
    for i in range(lines):
        forward(0, lax.rem(z + i, lines), i == 0)
    for k in range(1, splits):
        gather_step(k, 1, middle)
    far_wait(1)
    core_wait(1)
    for i in range(lines):
        backward(0, lax.rem(z + i, lines), i == 0)
    activate(0)
    for k in range(1, splits):
        for d in range(2, lines - 1):
            gather_step(k, d, middle)

    def both_pieces(k):
        @pl.when(end)
        def _():
            for w in range(2):
                pieces(k, w)

    both_pieces(0)
    for k in range(1, splits):
        forward(k, z, True)
        backward(k, z, True)
        for d in range(1, lines):
            gather_step(k, d, end)
            compute_step(k, d)
        activate(k)
        both_pieces(k)
    share_send()

    grads = [(k, w) for k in range(splits) for w in range(2)]

    @pl.when(middle)
    def _():
        for at, (k, w) in enumerate(grads):
            pieces(k, w)
            if at:
                spread_relay(*grads[at - 1])
            reduce_own(k, w)
        spread_relay(*grads[-1])

    @pl.when(end)
    def _():
        for at, (k, w) in enumerate(grads):
            reduce_own(k, w)
            if at:
                spread_relay(*grads[at - 1])
        spread_relay(*grads[-1])

    out = share_end()
    for k, w in grads:
        spread_wait(k, w)
    ends = [fetch(spread.at[w], ref, "out", w) for w, ref in enumerate((up_out, down_out))]
    arrived(share_out.at[:, pl.ds(pl.multiple_of((1 - core) * mid, mid), mid)], "core_share").wait_recv()
    for cond, copy in pending:
        when(cond, copy.wait_send)
    for k, w in grads:
        pieces_end(k, w)
        for copy in spread_copies(k, w):
            copy.wait_send()
    out.wait()
    for copy in ends:
        copy.wait()


def plane_fits(inputs, up_weight, down_weight):
    reps, groups, cores = (lax.axis_size(axis) for axis in ("rep", "fs", "tp"))
    if reps != 2 or cores != 2 or groups % 4:
        return False
    rows, width = inputs.shape
    depth, units = up_weight.shape
    step = units // 4 // SPLITS
    even = rows % 64 == 0 and depth % 128 == 0 and step % 128 == 0 and width == groups * depth
    held = 2 * 4 * rows * width * 2 + 4 * (units // 4) * width * 2
    return even and held <= 16 * 2**20


def plane_plan(inputs, cotangent, up_weight, down_weight):
    groups = lax.axis_size("fs")
    lines, splits = groups // 2, SPLITS
    rows, width = inputs.shape
    depth, units = up_weight.shape
    step = units // 4 // splits
    wide = 2 * depth
    plane = 4 * rows
    sent, got, local = plane_slots(lines, splits)
    narrow, full = jnp.bfloat16, jnp.float32
    anywhere = pl.BlockSpec(memory_space=pl.ANY)
    share, up, down = pl.pallas_call(
        functools.partial(plane_kernel, lines, splits, sent, got, local),
        out_shape=(
            jax.ShapeDtypeStruct((rows, width), full),
            jax.ShapeDtypeStruct((4, splits, step, depth), narrow),
            jax.ShapeDtypeStruct((4, splits, step, depth), narrow),
        ),
        in_specs=[anywhere] * 4,
        out_specs=(anywhere,) * 3,
        scratch_shapes=[
            pltpu.VMEM((2, plane, width), narrow),
            pltpu.VMEM((splits, lines, wide, step), narrow),
            pltpu.VMEM((splits, lines, step, wide), narrow),
            pltpu.VMEM((splits, lines, wide, step), narrow),
            pltpu.VMEM((plane, step), full),
            pltpu.VMEM((plane, step), full),
            pltpu.VMEM((splits, plane, step), narrow),
            pltpu.VMEM((splits, plane, step), narrow),
            pltpu.VMEM((splits, 2, step, plane), narrow),
            pltpu.VMEM((splits, 2, lines, step, wide), narrow),
            pltpu.VMEM((2, splits, 2, lines, step, wide), narrow),
            pltpu.VMEM((step, wide), full),
            pltpu.VMEM((2, 4, splits, step, depth), narrow),
            pltpu.VMEM((splits, 2, step, depth), narrow),
            pltpu.VMEM((3, rows, width // 2), narrow),
            pltpu.VMEM((3, rows, width // 2), narrow),
            pltpu.VMEM((rows, width // 2), full),
            pltpu.SemaphoreType.DMA((sent.size,)),
            pltpu.SemaphoreType.DMA((got.size,)),
            pltpu.SemaphoreType.DMA((local.size,)),
        ],
        compiler_params=pltpu.CompilerParams(
            collective_id=0, has_side_effects=True, vmem_limit_bytes=63 * 2**20
        ),
        name="plane",
    )(inputs, cotangent, up_weight, down_weight)
    grad_up = up.reshape(units, depth).T.astype(full)
    grad_down = down.reshape(units, depth).astype(full)
    norms_up = small_sum(jnp.sum(grad_up * grad_up, axis=1), "tp")
    norms_down = small_sum(jnp.sum(grad_down * grad_down, axis=1), "fs")
    return (share, grad_up, grad_down, norms_up, norms_down)


def shards(inputs, cotangent, up_weight, down_weight):
    tokens = inputs.size * lax.axis_size("fs") // lax.axis_size("tp")
    weights = up_weight.size * lax.axis_size("fs")
    plan = token_plan if tokens <= weights else weight_plan
    if plane_fits(inputs, up_weight, down_weight):
        plan = plane_plan
    return plan(inputs, cotangent, up_weight, down_weight)


def solution(mesh):
    return jax.shard_map(
        shards,
        mesh=mesh,
        in_specs=(P(("rep", "fs"), None), P(("rep", "fs"), None), P("fs", "tp"), P("tp", "fs")),
        out_specs=(P(("rep", "fs"), None), P("fs", "tp"), P("tp", "fs"), P("fs"), P("tp")),
        check_vma=False,
    )
```

```python
import functools

import jax
import jax.numpy as jnp
from jax import lax
from jax.experimental import pallas as pl
from jax.experimental.pallas import tpu as pltpu
from jax.sharding import PartitionSpec as P

NARROW = jnp.bfloat16
CHUNKS = 2


def contract(left, right, left_dim, right_dim):
    return lax.dot_general(
        left, right, (((left_dim,), (right_dim,)), ((), ())), preferred_element_type=jnp.float32
    )


def own_block(blocks, axis, shift=0):
    size = lax.axis_size(axis)
    return lax.dynamic_index_in_dim(
        blocks, lax.rem(lax.axis_index(axis) + shift, size), 0, keepdims=False
    )


def rotate(block, axis, shift):
    size = lax.axis_size(axis)
    return lax.ppermute(block, axis, [(at, (at + shift) % size) for at in range(size)])


def scatter_sum(blocks, axis):
    total = own_block(blocks, axis)
    for shift in range(1, lax.axis_size(axis)):
        sent = own_block(blocks, axis, shift).astype(NARROW)
        total = total + rotate(sent, axis, shift).astype(jnp.float32)
    return total


def gather_blocks(block, axis):
    size = lax.axis_size(axis)
    me = lax.axis_index(axis)
    held = [block] + [rotate(block, axis, shift) for shift in range(1, size)]
    placed = []
    for at in range(size):
        pick = held[0]
        for shift in range(1, size):
            pick = jnp.where(lax.rem(me - at + size, size) == shift, held[shift], pick)
        placed.append(pick)
    return jnp.stack(placed)


def fs_sum(blocks, ahead=None):
    groups = lax.axis_size("fs")
    pair = 2 if groups % 2 == 0 else 1
    far = groups // pair
    me = lax.axis_index("fs")
    blocks = blocks.reshape((far, pair) + blocks.shape[1:])

    def near_block(shift):
        return lax.dynamic_index_in_dim(
            blocks, lax.rem(lax.rem(me, pair) + shift, pair), 1, keepdims=False
        )

    held = near_block(0)
    for shift in range(1, pair):
        perm = [(at, at - at % pair + (at + shift) % pair) for at in range(groups)]
        got = lax.ppermute(near_block(shift).astype(NARROW), "fs", perm)
        held = held + got.astype(jnp.float32)

    if ahead is not None:
        held, ahead = lax.optimization_barrier((held, ahead))

    def far_block(shift):
        return lax.dynamic_index_in_dim(held, lax.rem(me // pair + shift, far), 0, keepdims=False)

    total = far_block(0)
    for shift in range(1, far):
        perm = [(at, (at + shift * pair) % groups) for at in range(groups)]
        got = lax.ppermute(far_block(shift).astype(NARROW), "fs", perm)
        total = total + got.astype(jnp.float32)
    return total, ahead


def exchange(blocks, axis):
    return lax.all_to_all(blocks, axis, 0, 0)


def small_sum(value, axis):
    size = lax.axis_size(axis)
    if size & (size - 1):
        return lax.psum(value, axis)
    bit = 1
    while bit < size:
        value = value + lax.ppermute(value, axis, [(at, at ^ bit) for at in range(size)])
        bit *= 2
    return value


def token_plan(inputs, cotangent, up_weight, down_weight):
    reps, groups, cores = (lax.axis_size(axis) for axis in ("rep", "fs", "tp"))
    rows, width = inputs.shape
    depth, units = up_weight.shape
    mine = units // groups
    part = depth // reps
    half = width // cores

    few = mine // reps
    up = own_block(up_weight.reshape(reps, part, groups, mine).transpose(0, 2, 1, 3), "rep")
    down = own_block(down_weight.reshape(groups, reps, few, depth).transpose(1, 0, 2, 3), "rep")
    both = jnp.concatenate([up, down.reshape(groups, part, mine)], axis=1)
    both = gather_blocks(exchange(both, "fs"), "rep")
    up = both[:, :, :part].transpose(1, 0, 2, 3).reshape(width, mine)
    down = both[:, :, part:].reshape(reps, groups, few, depth)
    down = down.transpose(0, 2, 1, 3).reshape(mine, width)
    tokens = lax.all_gather(
        own_block(inputs.reshape(cores, rows // cores, width), "tp"), ("fs", "tp"), axis=0, tiled=True
    )
    cot = lax.all_gather(
        own_block(cotangent.reshape(cores, rows // cores, width), "tp"), ("fs", "tp"), axis=0, tiled=True
    )

    pre_act = contract(tokens, up, 1, 0)
    act_grad = contract(cot, down, 1, 1)
    rectified = jnp.maximum(pre_act, 0.0)
    hidden = (rectified * rectified).astype(jnp.bfloat16)
    pre_grad = (2.0 * rectified * act_grad).astype(jnp.bfloat16)

    up_rows = up.reshape(cores, half, mine)
    share = contract(pre_grad, own_block(up_rows, "tp"), 1, 1)
    for shift in range(1, cores):
        sent = contract(pre_grad, own_block(up_rows, "tp", shift), 1, 1).astype(NARROW)
        share = share + rotate(sent, "tp", shift).astype(jnp.float32)
    chunks = CHUNKS if half % (128 * CHUNKS) == 0 else 1
    share = share.reshape(groups, rows, half)
    step = half // chunks
    def spread(term):
        term = term.reshape(groups, reps, part, mine).transpose(1, 0, 2, 3)
        return exchange(scatter_sum(term, "rep").astype(NARROW), "fs")

    def whole(term):
        term = gather_blocks(term, "rep")
        return term.transpose(0, 2, 1, 3).reshape(depth, units).astype(jnp.float32)

    spreads = (spread(contract(cot, hidden, 0, 0)), spread(contract(tokens, pre_grad, 0, 0)))
    sums = []
    for at in range(chunks):
        ahead = spreads if at == chunks - 1 else None
        total, ahead = fs_sum(share[:, :, at * step : (at + 1) * step], ahead)
        sums.append(total)
    share = jnp.concatenate(sums, axis=1)
    share = gather_blocks(share, "tp")
    grad_inputs = share.transpose(1, 0, 2).reshape(rows, width)

    down_turned, grad_up = whole(ahead[0]), whole(ahead[1])
    norms_up = small_sum(jnp.sum(grad_up * grad_up, axis=1), "tp")
    norms_down = small_sum(jnp.sum(down_turned * down_turned, axis=0), "fs")
    return (grad_inputs, grad_up, down_turned.T, norms_up, norms_down)


def weight_plan(inputs, cotangent, up_weight, down_weight):
    up_whole = lax.all_gather(up_weight, "fs", axis=0, tiled=True)
    pre_act = jnp.dot(inputs, up_whole, preferred_element_type=jnp.float32)
    act_grad = contract(cotangent, lax.all_gather(down_weight, "fs", axis=1, tiled=True), 1, 1)
    rectified = jnp.maximum(pre_act, 0.0)
    hidden = (rectified * rectified).astype(jnp.bfloat16)
    pre_grad = (2.0 * rectified * act_grad).astype(jnp.bfloat16)
    up_part = lax.psum_scatter(
        contract(inputs, pre_grad, 0, 0), "fs", scatter_dimension=0, tiled=True
    )
    down_part = lax.psum_scatter(
        contract(cotangent, hidden, 0, 0), "fs", scatter_dimension=0, tiled=True
    )
    grad_up, down_turned = lax.psum((up_part, down_part), "rep")
    grad_inputs = lax.psum(contract(pre_grad, up_whole, 1, 1), "tp")
    norms_up = lax.psum(jnp.sum(grad_up * grad_up, axis=1), "tp")
    norms_down = lax.psum(jnp.sum(down_turned * down_turned, axis=0), "fs")
    grad_down = down_turned.T
    return (grad_inputs, grad_up, grad_down, norms_up, norms_down)


MESH = pl.DeviceIdType.MESH
SPLITS = 2


def dot(left, right, left_dim, right_dim):
    return lax.dot_general(
        left, right, (((left_dim,), (right_dim,)), ((), ())), preferred_element_type=jnp.float32
    )


class Slots:
    def __init__(self):
        self.size = 0
        self.base = {}

    def add(self, name, *shape):
        self.base[name] = (self.size, shape)
        count = 1
        for extent in shape:
            count *= extent
        self.size += count

    def at(self, name, *index):
        start, shape = self.base[name]
        place = 0
        for extent, position in zip(shape, index, strict=True):
            place = place * extent + position
        return start + place


def plane_slots(lines, splits):
    sent, got, local = Slots(), Slots(), Slots()
    for table in (sent, got):
        table.add("pair", splits, 2)
        table.add("near_x", 2, 2)
        table.add("near_y", 2, 2)
        table.add("far", 2, 2)
        table.add("core_tokens", 2, 3)
        table.add("core_up", splits, lines)
        table.add("core_pre", splits)
        table.add("spread_y", splits, 2)
        table.add("spread_x", splits, 2, 2)
        table.add("share", 3)
        table.add("core_share")
        table.add("core_norms")
        table.add("reduce", 2, splits, 2, lines)
    sent.add("norms", 2, 2, lines)
    got.add("norms", lines, 4)
    sent.add("line_up", splits, 2, 2, lines)
    sent.add("line_down", splits, 2, 2, lines)
    got.add("line", splits, 2, 2, lines)
    local.add("tokens", 2)
    local.add("weights", splits, 2)
    local.add("share")
    local.add("out", 2)
    return sent, got, local


def plane_kernel(
    lines, splits, sent, got, local,
    tokens_hbm, cot_hbm, up_hbm, down_hbm,
    share_out, up_out, down_out, up_norms, down_norms,
    acts, ups, downs, other_up, pre_act, act_grad, pre_grad, other_pre, turned,
    leaving, inbox, partial, spread, spread_far, share_leaving, share_got, share_sum,
    row_norms, col_norms,
    send_sems, got_sems, local_sems,
):
    rows, width = tokens_hbm.shape
    depth, units = up_hbm.shape
    mine = units // 4
    step = mine // splits
    wide = 2 * depth
    half = rows // 2
    bit = half // 2
    near = lines // 2
    mid = width // 2

    x = lax.axis_index("rep")
    fs = lax.axis_index("fs")
    core = lax.axis_index("tp")
    z, y = fs // 2, fs % 2
    me = 2 * x + y
    at_x, at_y, at_far = 2 * (1 - x) + y, 2 * x + 1 - y, 2 * (1 - x) + 1 - y
    to_x = (1 - x, fs, core)
    to_y = (x, 2 * z + 1 - y, core)
    to_far = (1 - x, 2 * z + 1 - y, core)
    to_core = (x, fs, 1 - core)
    to_up = (x, fs + 2, core)
    to_down = (x, fs - 2, core)
    has_up, has_down = z < lines - 1, z > 0
    middle = jnp.logical_and(has_up, has_down)
    end = jnp.logical_not(middle)
    pending = []

    def when(cond, act):
        if cond is None:
            act()
        else:
            pl.when(cond)(act)

    def remote(src, dst, to, key, *index, got_key=None):
        return pltpu.make_async_remote_copy(
            src_ref=src, dst_ref=dst,
            send_sem=send_sems.at[sent.at(key, *index)],
            recv_sem=got_sems.at[got.at(got_key or key, *index)],
            device_id=to, device_id_type=MESH,
        )

    def send(src, dst, to, key, *index, cond=None, got_key=None):
        copy = remote(src, dst, to, key, *index, got_key=got_key)
        when(cond, copy.start)
        pending.append((cond, copy))

    def arrived(dst, key, *index):
        return pltpu.make_async_remote_copy(
            src_ref=dst, dst_ref=dst, send_sem=send_sems.at[0],
            recv_sem=got_sems.at[got.at(key, *index)],
            device_id=to_core, device_id_type=MESH,
        )

    def fetch(src, dst, key, *index):
        copy = pltpu.make_async_copy(src, dst, local_sems.at[local.at(key, *index)])
        copy.start()
        return copy

    def up_piece(k, line, side):
        return ups.at[k, line, pl.ds(pl.multiple_of(side * depth, depth), depth), :]

    def down_piece(k, line, side):
        return downs.at[k, line, :, pl.ds(pl.multiple_of(side * depth, depth), depth)]

    def piece(w, k, line, side):
        return (up_piece, down_piece)[w](k, line, side)

    def own(w, owner, k):
        at = pl.ds(pl.multiple_of(owner * mine + k * step, step), step)
        return up_hbm.at[:, at] if w == 0 else down_hbm.at[at, :]

    def band(t, owner, first, count):
        return acts.at[t, pl.ds(pl.multiple_of(owner * rows + first, bit), count), :]

    gets = {}
    for k in range(splits):
        for w in range(2):
            gets[k, w] = fetch(own(w, me, k), piece(w, k, z, y), "weights", k, w)
        if k == 0:
            for t, src in ((0, tokens_hbm), (1, cot_hbm)):
                gets[t] = fetch(src, band(t, me, 0, rows), "tokens", t)

    others = [
        (i, j, d, ((x + i) % 2, (z + d) % lines * 2 + (y + j) % 2, core))
        for i in range(2)
        for j in range(2)
        for d in range(lines)
        if i or j or d
    ]
    barrier = pltpu.get_barrier_semaphore()
    for to in [to_core] + [other[-1] for other in others]:
        pl.semaphore_signal(barrier, inc=1, device_id=to, device_id_type=MESH)
    pl.semaphore_wait(barrier, 1 + len(others))

    def pair_send(k):
        for w in range(2):
            send(own(w, at_y, k), piece(w, k, z, y), to_y, "pair", k, w)

    def line_send(k, side, who=None):
        up_cond, down_cond = has_up, has_down
        if who is not None:
            up_cond, down_cond = jnp.logical_and(has_up, who), jnp.logical_and(has_down, who)
        for w in range(2):
            ref = piece(w, k, z, side)
            send(ref, ref, to_up, "line_up", k, w, side, z, cond=up_cond, got_key="line")
            send(ref, ref, to_down, "line_down", k, w, side, z, cond=down_cond, got_key="line")

    def pair_wait(k):
        for w in range(2):
            arrived(piece(w, k, z, 1 - y), "pair", k, w).wait_recv()

    first = core * half

    def near_send(t):
        for p in range(2):
            ref = band(t, me, first + p * bit, bit)
            send(ref, ref, to_x, "near_x", t, p)
            ref = band(t, me, first + (1 - p) * bit, bit)
            send(ref, ref, to_y, "near_y", t, 1 - p)

    def relay(t):
        ref = band(t, at_x, first, bit)
        arrived(ref, "near_x", t, 0).wait_recv()
        send(ref, ref, to_y, "far", t, 0)
        ref = band(t, at_y, first + bit, bit)
        arrived(ref, "near_y", t, 1).wait_recv()
        send(ref, ref, to_x, "far", t, 1)
        arrived(band(t, at_x, first + bit, bit), "near_x", t, 1).wait_recv()
        arrived(band(t, at_y, first, bit), "near_y", t, 0).wait_recv()
        for i, owner in enumerate((at_x, at_y)):
            ref = band(t, owner, first, half)
            send(ref, ref, to_core, "core_tokens", t, i)

    def far_wait(t):
        for p in range(2):
            arrived(band(t, at_far, first + p * bit, bit), "far", t, p).wait_recv()
        ref = band(t, at_far, first, half)
        send(ref, ref, to_core, "core_tokens", t, 2)

    def core_wait(t):
        for i, owner in enumerate((at_x, at_y, at_far)):
            arrived(band(t, owner, (1 - core) * half, half), "core_tokens", t, i).wait_recv()

    def core_up_send(k, line, cond):
        other = (1 - core) * near
        inside = jnp.logical_and(line >= other, line < other + near)
        if cond is not None:
            inside = jnp.logical_and(inside, cond)
        send(ups.at[k, line], other_up.at[k, line], to_core, "core_up", k, line, cond=inside)

    def beside(d):
        below, above = z - d, z + d
        return (
            (lax.rem(below + lines, lines), below >= 0, has_up, to_up, "line_up"),
            (lax.rem(above, lines), above < lines, has_down, to_down, "line_down"),
        )

    def gather_step(k, d, who=None):
        for line, cond, onward, to, key in beside(d):
            if who is not None:
                cond = jnp.logical_and(cond, who)
            for w in range(2):
                for side in range(2):
                    ref = piece(w, k, line, side)
                    when(cond, arrived(ref, "line", k, w, side, line).wait_recv)
                    send(
                        ref, ref, to, key, k, w, side, line,
                        cond=jnp.logical_and(cond, onward), got_key="line",
                    )
            core_up_send(k, line, cond)

    def forward(k, line, fresh):
        cols = pl.ds(pl.multiple_of(line * wide, wide), wide)
        a = dot(acts[0, :, cols], ups[k, line], 1, 0)
        pre_act[...] = a if fresh else pre_act[...] + a

    def backward(k, line, fresh):
        cols = pl.ds(pl.multiple_of(line * wide, wide), wide)
        a = dot(acts[1, :, cols], downs[k, line], 1, 1)
        act_grad[...] = a if fresh else act_grad[...] + a

    def compute_step(k, d):
        for line, cond, _, _, _ in beside(d):

            @pl.when(cond)
            def _():
                forward(k, line, False)
                backward(k, line, False)

    def activate(k):
        def body(i, carry):
            at = pl.ds(pl.multiple_of(i * rows, rows), rows)
            r = jnp.maximum(pre_act[at, :], 0.0)
            g = (2.0 * r * act_grad[at, :]).astype(jnp.bfloat16)
            pre_grad[k, at, :] = g
            turned[k, 0, :, at] = g.T
            turned[k, 1, :, at] = (r * r).astype(jnp.bfloat16).T
            return carry

        lax.fori_loop(0, 4, body, 0)
        send(pre_grad.at[k], other_pre.at[k], to_core, "core_pre", k)

    def term(k, w, owner):
        cols = pl.ds(pl.multiple_of(owner * wide, wide), wide)
        return dot(turned[k, w], acts[w, :, cols], 1, 0)

    def route(k, w, t):
        turn = lax.rem(t // (lines - 1) + z // near, 2)
        j = lax.rem(t, lines - 1)
        owner = (1 - turn) * (lines - 1 - j) + turn * j
        sign = 1 - 2 * turn
        cond = (owner - z) * sign > 0
        source = z - sign
        has_in = jnp.logical_and(source >= 0, source < lines)
        box = inbox.at[turn, k, w, owner]
        out = leaving.at[k, w, owner]
        copy = pltpu.make_async_remote_copy(
            src_ref=out, dst_ref=box,
            send_sem=send_sems.at[sent.at("reduce", turn, k, w, owner)],
            recv_sem=got_sems.at[got.at("reduce", turn, k, w, owner)],
            device_id=(x, fs + 2 * sign, core), device_id_type=MESH,
        )
        return owner, cond, has_in, box, out, copy

    def pieces(k, w):
        def body(t, carry):
            owner, cond, has_in, box, out, copy = route(k, w, t)

            @pl.when(cond)
            def _():
                partial[...] = term(k, w, owner)

                @pl.when(has_in)
                def _():
                    copy.wait_recv()
                    out[...] = (partial[...] + box[...].astype(jnp.float32)).astype(jnp.bfloat16)

                @pl.when(jnp.logical_not(has_in))
                def _():
                    out[...] = partial[...].astype(jnp.bfloat16)

                copy.start()

            return carry

        lax.fori_loop(0, 2 * (lines - 1), body, 0)

    def pieces_end(k, w):
        def body(t, carry):
            _, cond, _, _, _, copy = route(k, w, t)
            pl.when(cond)(copy.wait_send)
            return carry

        lax.fori_loop(0, 2 * (lines - 1), body, 0)

    def spread_copies(k, w):
        here, there, near_ref = spread.at[w, me, k], spread_far.at[k, w], spread.at[w, at_y, k]
        return (
            remote(there, here, to_y, "spread_y", k, w),
            remote(here, here, to_x, "spread_x", k, w, 0),
            remote(near_ref, near_ref, to_x, "spread_x", k, w, 1),
        )

    def reduce_own(k, w):
        partial[...] = term(k, w, z)
        for turn, cond in ((0, has_down), (1, has_up)):
            box = inbox.at[turn, k, w, z]
            wait = arrived(box, "reduce", turn, k, w, z)

            @pl.when(cond)
            def _():
                wait.wait_recv()
                partial[...] += box[...].astype(jnp.float32)

        if w == 1:
            square = partial[...] * partial[...]
            folded = square[:, :128]
            for at in range(128, wide, 128):
                folded += square[:, at : at + 128]
            row_norms[z, me, :, k * step : (k + 1) * step] = jnp.broadcast_to(
                jnp.sum(folded.T, axis=0, keepdims=True), (8, step)
            )
        here, there = spread.at[w, me, k], spread_far.at[k, w]
        there[...] = partial[:, pl.ds(pl.multiple_of((1 - y) * depth, depth), depth)].astype(jnp.bfloat16)
        here[...] = partial[:, pl.ds(pl.multiple_of(y * depth, depth), depth)].astype(jnp.bfloat16)
        to_near, to_side, _ = spread_copies(k, w)
        to_near.start()
        to_side.start()

    def spread_relay(k, w):
        arrived(spread.at[w, at_y, k], "spread_y", k, w).wait_recv()
        spread_copies(k, w)[2].start()

    def spread_wait(k, w):
        arrived(spread.at[w, at_x, k], "spread_x", k, w, 0).wait_recv()
        arrived(spread.at[w, at_far, k], "spread_x", k, w, 1).wait_recv()

    def norm_copies():
        ref = row_norms.at[z, me]
        for i, j, d, to in others:
            yield pltpu.make_async_remote_copy(
                src_ref=ref, dst_ref=ref,
                send_sem=send_sems.at[sent.at("norms", i, j, d)],
                recv_sem=got_sems.at[got.at("norms", z, me)],
                device_id=to, device_id_type=MESH,
            )

    def norms_send():
        for copy in norm_copies():
            copy.start()

    def norms_end():
        for i, j, d, _ in others:
            line, owner = (z + d) % lines, 2 * ((x + i) % 2) + (y + j) % 2
            arrived(row_norms.at[line, owner], "norms", line, owner).wait_recv()
        for owner in range(4):
            total = row_norms[0, owner, 0:1, :]
            for line in range(1, lines):
                total += row_norms[line, owner, 0:1, :]
            down_norms[:, owner * mine : (owner + 1) * mine] = total

    def col_send():
        total = jnp.zeros((8, depth), jnp.float32)
        for owner in range(4):
            for k in range(splits):
                block = spread[0, owner, k].astype(jnp.float32)
                total += jnp.sum((block * block).reshape(step // 8, 8, depth), axis=0)
        col_norms[0] = jnp.broadcast_to(jnp.sum(total, axis=0, keepdims=True), (8, depth))
        send(col_norms.at[0], col_norms.at[1], to_core, "core_norms")

    def col_end():
        arrived(col_norms.at[1], "core_norms").wait_recv()
        up_norms[...] = col_norms[0, 0:1, :] + col_norms[1, 0:1, :]

    def share_term(owner):
        at = pl.ds(pl.multiple_of(owner * rows, rows), rows)
        parts = []
        for i in range(near):
            line = core * near + i
            total = None
            for k in range(splits):
                for grads, weights in ((pre_grad, ups), (other_pre, other_up)):
                    a = dot(grads[k, at, :], weights[k, line], 1, 1)
                    total = a if total is None else total + a
            parts.append(total)
        return parts

    def share_send():
        for k in range(splits):
            arrived(other_pre.at[k], "core_pre", k).wait_recv()
            for i in range(near):
                line = core * near + i
                arrived(other_up.at[k, line], "core_up", k, line).wait_recv()
        for j, (owner, to) in enumerate(((at_far, to_far), (at_x, to_x), (at_y, to_y))):
            for i, part in enumerate(share_term(owner)):
                share_leaving[j, :, i * wide : (i + 1) * wide] = part.astype(jnp.bfloat16)
            send(share_leaving.at[j], share_got.at[j], to, "share", j)
        for i, part in enumerate(share_term(me)):
            share_sum[:, i * wide : (i + 1) * wide] = part

    def share_end():
        for j in range(3):
            arrived(share_got.at[j], "share", j).wait_recv()
            share_sum[...] += share_got[j].astype(jnp.float32)
        place = share_out.at[:, pl.ds(pl.multiple_of(core * mid, mid), mid)]
        send(share_sum, place, to_core, "core_share")
        return fetch(share_sum, place, "share")

    pair_send(0)
    for w in range(2):
        gets[0, w].wait()
    line_send(0, y)
    for t in range(2):
        gets[t].wait()
        near_send(t)
    pair_wait(0)
    line_send(0, 1 - y)
    core_up_send(0, z, None)
    for k in range(1, splits):
        pair_send(k)
        for w in range(2):
            gets[k, w].wait()
        line_send(k, y, end)
    relay(0)
    gather_step(0, 1)
    for k in range(1, splits):
        pair_wait(k)
        line_send(k, 1 - y, end)
        core_up_send(k, z, None)
    for d in range(2, lines - 1):
        gather_step(0, d)
    relay(1)
    for k in range(1, splits):
        for side in (y, 1 - y):
            line_send(k, side, middle)
    far_wait(0)
    gather_step(0, lines - 1)
    core_wait(0)
    for i in range(lines):
        forward(0, lax.rem(z + i, lines), i == 0)
    for k in range(1, splits):
        gather_step(k, 1, middle)
    far_wait(1)
    core_wait(1)
    for i in range(lines):
        backward(0, lax.rem(z + i, lines), i == 0)
    activate(0)
    for k in range(1, splits):
        for d in range(2, lines - 1):
            gather_step(k, d, middle)

    def both_pieces(k):
        @pl.when(end)
        def _():
            for w in range(2):
                pieces(k, w)

    both_pieces(0)
    for k in range(1, splits):
        forward(k, z, True)
        backward(k, z, True)
        for d in range(1, lines):
            gather_step(k, d, end)
            compute_step(k, d)
        activate(k)
        both_pieces(k)
    share_send()

    grads = [(k, w) for k in range(splits) for w in range(2)]

    @pl.when(middle)
    def _():
        for at, (k, w) in enumerate(grads):
            pieces(k, w)
            if at:
                spread_relay(*grads[at - 1])
            reduce_own(k, w)
        norms_send()
        spread_relay(*grads[-1])

    @pl.when(end)
    def _():
        for at, (k, w) in enumerate(grads):
            reduce_own(k, w)
            if at:
                spread_relay(*grads[at - 1])
        norms_send()
        spread_relay(*grads[-1])

    out = share_end()
    for k in range(splits):
        spread_wait(k, 0)
    col_send()
    norms_end()
    for k in range(splits):
        spread_wait(k, 1)
    col_end()
    ends = [fetch(spread.at[w], ref, "out", w) for w, ref in enumerate((up_out, down_out))]
    arrived(share_out.at[:, pl.ds(pl.multiple_of((1 - core) * mid, mid), mid)], "core_share").wait_recv()
    for cond, copy in pending:
        when(cond, copy.wait_send)
    for copy in norm_copies():
        copy.wait_send()
    for k, w in grads:
        pieces_end(k, w)
        for copy in spread_copies(k, w):
            copy.wait_send()
    out.wait()
    for copy in ends:
        copy.wait()


def plane_fits(inputs, up_weight, down_weight):
    reps, groups, cores = (lax.axis_size(axis) for axis in ("rep", "fs", "tp"))
    if reps != 2 or cores != 2 or groups % 4:
        return False
    rows, width = inputs.shape
    depth, units = up_weight.shape
    step = units // 4 // SPLITS
    even = rows % 64 == 0 and depth % 128 == 0 and step % 128 == 0 and width == groups * depth
    held = 2 * 4 * rows * width * 2 + 4 * (units // 4) * width * 2
    return even and held <= 16 * 2**20


def plane_plan(inputs, cotangent, up_weight, down_weight):
    groups = lax.axis_size("fs")
    lines, splits = groups // 2, SPLITS
    rows, width = inputs.shape
    depth, units = up_weight.shape
    step = units // 4 // splits
    wide = 2 * depth
    plane = 4 * rows
    sent, got, local = plane_slots(lines, splits)
    narrow, full = jnp.bfloat16, jnp.float32
    anywhere = pl.BlockSpec(memory_space=pl.ANY)
    share, up, down, norms_up, norms_down = pl.pallas_call(
        functools.partial(plane_kernel, lines, splits, sent, got, local),
        out_shape=(
            jax.ShapeDtypeStruct((rows, width), full),
            jax.ShapeDtypeStruct((4, splits, step, depth), narrow),
            jax.ShapeDtypeStruct((4, splits, step, depth), narrow),
            jax.ShapeDtypeStruct((1, depth), full),
            jax.ShapeDtypeStruct((1, units), full),
        ),
        in_specs=[anywhere] * 4,
        out_specs=(anywhere,) * 3 + (pl.BlockSpec(memory_space=pltpu.VMEM),) * 2,
        scratch_shapes=[
            pltpu.VMEM((2, plane, width), narrow),
            pltpu.VMEM((splits, lines, wide, step), narrow),
            pltpu.VMEM((splits, lines, step, wide), narrow),
            pltpu.VMEM((splits, lines, wide, step), narrow),
            pltpu.VMEM((plane, step), full),
            pltpu.VMEM((plane, step), full),
            pltpu.VMEM((splits, plane, step), narrow),
            pltpu.VMEM((splits, plane, step), narrow),
            pltpu.VMEM((splits, 2, step, plane), narrow),
            pltpu.VMEM((splits, 2, lines, step, wide), narrow),
            pltpu.VMEM((2, splits, 2, lines, step, wide), narrow),
            pltpu.VMEM((step, wide), full),
            pltpu.VMEM((2, 4, splits, step, depth), narrow),
            pltpu.VMEM((splits, 2, step, depth), narrow),
            pltpu.VMEM((3, rows, width // 2), narrow),
            pltpu.VMEM((3, rows, width // 2), narrow),
            pltpu.VMEM((rows, width // 2), full),
            pltpu.VMEM((lines, 4, 8, units // 4), full),
            pltpu.VMEM((2, 8, depth), full),
            pltpu.SemaphoreType.DMA((sent.size,)),
            pltpu.SemaphoreType.DMA((got.size,)),
            pltpu.SemaphoreType.DMA((local.size,)),
        ],
        compiler_params=pltpu.CompilerParams(
            collective_id=0, has_side_effects=True, vmem_limit_bytes=63 * 2**20
        ),
        name="plane",
    )(inputs, cotangent, up_weight, down_weight)
    grad_up = up.reshape(units, depth).T.astype(full)
    grad_down = down.reshape(units, depth).astype(full)
    return (share, grad_up, grad_down, norms_up.reshape(depth), norms_down.reshape(units))


def shards(inputs, cotangent, up_weight, down_weight):
    tokens = inputs.size * lax.axis_size("fs") // lax.axis_size("tp")
    weights = up_weight.size * lax.axis_size("fs")
    plan = token_plan if tokens <= weights else weight_plan
    if plane_fits(inputs, up_weight, down_weight):
        plan = plane_plan
    return plan(inputs, cotangent, up_weight, down_weight)


def solution(mesh):
    return jax.shard_map(
        shards,
        mesh=mesh,
        in_specs=(P(("rep", "fs"), None), P(("rep", "fs"), None), P("fs", "tp"), P("tp", "fs")),
        out_specs=(P(("rep", "fs"), None), P("fs", "tp"), P("tp", "fs"), P("fs"), P("tp")),
        check_vma=False,
    )
```

```python
import functools

import jax
import jax.numpy as jnp
from jax import lax
from jax.experimental import pallas as pl
from jax.experimental.pallas import tpu as pltpu
from jax.sharding import PartitionSpec as P

NARROW = jnp.bfloat16
CHUNKS = 2


def contract(left, right, left_dim, right_dim):
    return lax.dot_general(
        left, right, (((left_dim,), (right_dim,)), ((), ())), preferred_element_type=jnp.float32
    )


def own_block(blocks, axis, shift=0):
    size = lax.axis_size(axis)
    return lax.dynamic_index_in_dim(
        blocks, lax.rem(lax.axis_index(axis) + shift, size), 0, keepdims=False
    )


def rotate(block, axis, shift):
    size = lax.axis_size(axis)
    return lax.ppermute(block, axis, [(at, (at + shift) % size) for at in range(size)])


def scatter_sum(blocks, axis):
    total = own_block(blocks, axis)
    for shift in range(1, lax.axis_size(axis)):
        sent = own_block(blocks, axis, shift).astype(NARROW)
        total = total + rotate(sent, axis, shift).astype(jnp.float32)
    return total


def gather_blocks(block, axis):
    size = lax.axis_size(axis)
    me = lax.axis_index(axis)
    held = [block] + [rotate(block, axis, shift) for shift in range(1, size)]
    placed = []
    for at in range(size):
        pick = held[0]
        for shift in range(1, size):
            pick = jnp.where(lax.rem(me - at + size, size) == shift, held[shift], pick)
        placed.append(pick)
    return jnp.stack(placed)


def fs_sum(blocks, ahead=None):
    groups = lax.axis_size("fs")
    pair = 2 if groups % 2 == 0 else 1
    far = groups // pair
    me = lax.axis_index("fs")
    blocks = blocks.reshape((far, pair) + blocks.shape[1:])

    def near_block(shift):
        return lax.dynamic_index_in_dim(
            blocks, lax.rem(lax.rem(me, pair) + shift, pair), 1, keepdims=False
        )

    held = near_block(0)
    for shift in range(1, pair):
        perm = [(at, at - at % pair + (at + shift) % pair) for at in range(groups)]
        got = lax.ppermute(near_block(shift).astype(NARROW), "fs", perm)
        held = held + got.astype(jnp.float32)

    if ahead is not None:
        held, ahead = lax.optimization_barrier((held, ahead))

    def far_block(shift):
        return lax.dynamic_index_in_dim(held, lax.rem(me // pair + shift, far), 0, keepdims=False)

    total = far_block(0)
    for shift in range(1, far):
        perm = [(at, (at + shift * pair) % groups) for at in range(groups)]
        got = lax.ppermute(far_block(shift).astype(NARROW), "fs", perm)
        total = total + got.astype(jnp.float32)
    return total, ahead


def exchange(blocks, axis):
    return lax.all_to_all(blocks, axis, 0, 0)


def small_sum(value, axis):
    size = lax.axis_size(axis)
    if size & (size - 1):
        return lax.psum(value, axis)
    bit = 1
    while bit < size:
        value = value + lax.ppermute(value, axis, [(at, at ^ bit) for at in range(size)])
        bit *= 2
    return value


def token_plan(inputs, cotangent, up_weight, down_weight):
    reps, groups, cores = (lax.axis_size(axis) for axis in ("rep", "fs", "tp"))
    rows, width = inputs.shape
    depth, units = up_weight.shape
    mine = units // groups
    part = depth // reps
    half = width // cores

    few = mine // reps
    up = own_block(up_weight.reshape(reps, part, groups, mine).transpose(0, 2, 1, 3), "rep")
    down = own_block(down_weight.reshape(groups, reps, few, depth).transpose(1, 0, 2, 3), "rep")
    both = jnp.concatenate([up, down.reshape(groups, part, mine)], axis=1)
    both = gather_blocks(exchange(both, "fs"), "rep")
    up = both[:, :, :part].transpose(1, 0, 2, 3).reshape(width, mine)
    down = both[:, :, part:].reshape(reps, groups, few, depth)
    down = down.transpose(0, 2, 1, 3).reshape(mine, width)
    tokens = lax.all_gather(
        own_block(inputs.reshape(cores, rows // cores, width), "tp"), ("fs", "tp"), axis=0, tiled=True
    )
    cot = lax.all_gather(
        own_block(cotangent.reshape(cores, rows // cores, width), "tp"), ("fs", "tp"), axis=0, tiled=True
    )

    pre_act = contract(tokens, up, 1, 0)
    act_grad = contract(cot, down, 1, 1)
    rectified = jnp.maximum(pre_act, 0.0)
    hidden = (rectified * rectified).astype(jnp.bfloat16)
    pre_grad = (2.0 * rectified * act_grad).astype(jnp.bfloat16)

    up_rows = up.reshape(cores, half, mine)
    share = contract(pre_grad, own_block(up_rows, "tp"), 1, 1)
    for shift in range(1, cores):
        sent = contract(pre_grad, own_block(up_rows, "tp", shift), 1, 1).astype(NARROW)
        share = share + rotate(sent, "tp", shift).astype(jnp.float32)
    chunks = CHUNKS if half % (128 * CHUNKS) == 0 else 1
    share = share.reshape(groups, rows, half)
    step = half // chunks
    def spread(term):
        term = term.reshape(groups, reps, part, mine).transpose(1, 0, 2, 3)
        return exchange(scatter_sum(term, "rep").astype(NARROW), "fs")

    def whole(term):
        term = gather_blocks(term, "rep")
        return term.transpose(0, 2, 1, 3).reshape(depth, units).astype(jnp.float32)

    spreads = (spread(contract(cot, hidden, 0, 0)), spread(contract(tokens, pre_grad, 0, 0)))
    sums = []
    for at in range(chunks):
        ahead = spreads if at == chunks - 1 else None
        total, ahead = fs_sum(share[:, :, at * step : (at + 1) * step], ahead)
        sums.append(total)
    share = jnp.concatenate(sums, axis=1)
    share = gather_blocks(share, "tp")
    grad_inputs = share.transpose(1, 0, 2).reshape(rows, width)

    down_turned, grad_up = whole(ahead[0]), whole(ahead[1])
    norms_up = small_sum(jnp.sum(grad_up * grad_up, axis=1), "tp")
    norms_down = small_sum(jnp.sum(down_turned * down_turned, axis=0), "fs")
    return (grad_inputs, grad_up, down_turned.T, norms_up, norms_down)


def weight_plan(inputs, cotangent, up_weight, down_weight):
    up_whole = lax.all_gather(up_weight, "fs", axis=0, tiled=True)
    pre_act = jnp.dot(inputs, up_whole, preferred_element_type=jnp.float32)
    act_grad = contract(cotangent, lax.all_gather(down_weight, "fs", axis=1, tiled=True), 1, 1)
    rectified = jnp.maximum(pre_act, 0.0)
    hidden = (rectified * rectified).astype(jnp.bfloat16)
    pre_grad = (2.0 * rectified * act_grad).astype(jnp.bfloat16)
    up_part = lax.psum_scatter(
        contract(inputs, pre_grad, 0, 0), "fs", scatter_dimension=0, tiled=True
    )
    down_part = lax.psum_scatter(
        contract(cotangent, hidden, 0, 0), "fs", scatter_dimension=0, tiled=True
    )
    grad_up, down_turned = lax.psum((up_part, down_part), "rep")
    grad_inputs = lax.psum(contract(pre_grad, up_whole, 1, 1), "tp")
    norms_up = lax.psum(jnp.sum(grad_up * grad_up, axis=1), "tp")
    norms_down = lax.psum(jnp.sum(down_turned * down_turned, axis=0), "fs")
    grad_down = down_turned.T
    return (grad_inputs, grad_up, grad_down, norms_up, norms_down)


MESH = pl.DeviceIdType.MESH
SPLITS = 4
LAG = 2


def dot(left, right, left_dim, right_dim):
    return lax.dot_general(
        left, right, (((left_dim,), (right_dim,)), ((), ())), preferred_element_type=jnp.float32
    )


class Slots:
    def __init__(self):
        self.size = 0
        self.base = {}

    def add(self, name, *shape):
        self.base[name] = (self.size, shape)
        count = 1
        for extent in shape:
            count *= extent
        self.size += count

    def at(self, name, *index):
        start, shape = self.base[name]
        place = 0
        for extent, position in zip(shape, index, strict=True):
            place = place * extent + position
        return start + place


def plane_slots(lines, splits):
    sent, got, local = Slots(), Slots(), Slots()
    for table in (sent, got):
        table.add("pair", splits, 2)
        table.add("near_x", 2, 2)
        table.add("near_y", 2, 2)
        table.add("far", 2, 2)
        table.add("core_tokens", 2, 3)
        table.add("core_up", splits, lines)
        table.add("core_pre", splits)
        table.add("spread_y", splits, 2)
        table.add("spread_x", splits, 2, 2)
        table.add("share", 3)
        table.add("core_share")
        table.add("core_norms")
        table.add("reduce", 2, splits, 2, lines)
    sent.add("norms", 2, 2, lines)
    got.add("norms", lines, 4)
    sent.add("line_up", splits, 2, 2, lines)
    sent.add("line_down", splits, 2, 2, lines)
    got.add("line", splits, 2, 2, lines)
    local.add("tokens", 2)
    local.add("weights", splits, 2)
    local.add("share")
    local.add("out", 2)
    return sent, got, local


def plane_kernel(
    lines, splits, sent, got, local,
    tokens_hbm, cot_hbm, up_hbm, down_hbm,
    share_out, up_out, down_out, up_norms, down_norms,
    acts, ups, downs, other_up, pre_grad, other_pre, turned,
    leaving, inbox, partial, spread, spread_far, share_leaving, share_got, share_sum,
    row_norms, col_norms,
    send_sems, got_sems, local_sems,
):
    rows, width = tokens_hbm.shape
    depth, units = up_hbm.shape
    mine = units // 4
    step = mine // splits
    wide = 2 * depth
    half = rows // 2
    part = half // 4
    near = lines // 2
    mid = width // 2

    x = lax.axis_index("rep")
    fs = lax.axis_index("fs")
    core = lax.axis_index("tp")
    z, y = fs // 2, fs % 2
    me = 2 * x + y
    at_x, at_y, at_far = 2 * (1 - x) + y, 2 * x + 1 - y, 2 * (1 - x) + 1 - y
    to_x = (1 - x, fs, core)
    to_y = (x, 2 * z + 1 - y, core)
    to_far = (1 - x, 2 * z + 1 - y, core)
    to_core = (x, fs, 1 - core)
    to_up = (x, fs + 2, core)
    to_down = (x, fs - 2, core)
    has_up, has_down = z < lines - 1, z > 0
    middle = jnp.logical_and(has_up, has_down)
    end = jnp.logical_not(middle)
    pending = []

    def when(cond, act):
        if cond is None:
            act()
        else:
            pl.when(cond)(act)

    def remote(src, dst, to, key, *index, got_key=None):
        return pltpu.make_async_remote_copy(
            src_ref=src, dst_ref=dst,
            send_sem=send_sems.at[sent.at(key, *index)],
            recv_sem=got_sems.at[got.at(got_key or key, *index)],
            device_id=to, device_id_type=MESH,
        )

    def send(src, dst, to, key, *index, cond=None, got_key=None):
        copy = remote(src, dst, to, key, *index, got_key=got_key)
        when(cond, copy.start)
        pending.append((cond, copy))

    def arrived(dst, key, *index):
        return pltpu.make_async_remote_copy(
            src_ref=dst, dst_ref=dst, send_sem=send_sems.at[0],
            recv_sem=got_sems.at[got.at(key, *index)],
            device_id=to_core, device_id_type=MESH,
        )

    def fetch(src, dst, key, *index):
        copy = pltpu.make_async_copy(src, dst, local_sems.at[local.at(key, *index)])
        copy.start()
        return copy

    def up_piece(k, line, side):
        return ups.at[k, line, pl.ds(pl.multiple_of(side * depth, depth), depth), :]

    def down_piece(k, line, side):
        return downs.at[k, line, :, pl.ds(pl.multiple_of(side * depth, depth), depth)]

    def piece(w, k, line, side):
        return (up_piece, down_piece)[w](k, line, side)

    def own(w, owner, k):
        at = pl.ds(pl.multiple_of(owner * mine + k * step, step), step)
        return up_hbm.at[:, at] if w == 0 else down_hbm.at[at, :]

    def band(t, owner, first, count):
        return acts.at[t, pl.ds(pl.multiple_of(owner * rows + first, part), count), :]

    gets = {}
    for k in range(splits):
        for w in range(2):
            gets[k, w] = fetch(own(w, me, k), piece(w, k, z, y), "weights", k, w)
        if k == 0:
            for t, src in ((0, tokens_hbm), (1, cot_hbm)):
                gets[t] = fetch(src, band(t, me, 0, rows), "tokens", t)

    others = [
        (i, j, d, ((x + i) % 2, (z + d) % lines * 2 + (y + j) % 2, core))
        for i in range(2)
        for j in range(2)
        for d in range(lines)
        if i or j or d
    ]
    barrier = pltpu.get_barrier_semaphore()
    for to in (to_x, to_y, to_core):
        pl.semaphore_signal(barrier, inc=1, device_id=to, device_id_type=MESH)
    for cond, to in ((has_up, to_up), (has_down, to_down)):

        @pl.when(cond)
        def _():
            pl.semaphore_signal(barrier, inc=1, device_id=to, device_id_type=MESH)

    pl.semaphore_wait(barrier, 3 + has_up.astype(jnp.int32) + has_down.astype(jnp.int32))

    def pair_send(k):
        for w in range(2):
            send(own(w, at_y, k), piece(w, k, z, y), to_y, "pair", k, w)

    def line_send(k, side):
        for w in range(2):
            ref = piece(w, k, z, side)
            send(ref, ref, to_up, "line_up", k, w, side, z, cond=has_up, got_key="line")
            send(ref, ref, to_down, "line_down", k, w, side, z, cond=has_down, got_key="line")

    def pair_wait(k):
        for w in range(2):
            arrived(piece(w, k, z, 1 - y), "pair", k, w).wait_recv()

    first = core * half

    cuts = ((0, part), (part, half - part))

    def cut(t, owner, p):
        return band(t, owner, first + cuts[p][0], cuts[p][1])

    def near_send(t):
        for p in range(2):
            ref = cut(t, me, p)
            send(ref, ref, to_x, "near_x", t, p)
            ref = cut(t, me, 1 - p)
            send(ref, ref, to_y, "near_y", t, 1 - p)

    def relay(t):
        ref = cut(t, at_x, 0)
        arrived(ref, "near_x", t, 0).wait_recv()
        send(ref, ref, to_y, "far", t, 0)
        ref = cut(t, at_y, 1)
        arrived(ref, "near_y", t, 1).wait_recv()
        send(ref, ref, to_x, "far", t, 1)

    def near_wait(t):
        arrived(cut(t, at_x, 1), "near_x", t, 1).wait_recv()
        arrived(cut(t, at_y, 0), "near_y", t, 0).wait_recv()
        for i, owner in enumerate((at_x, at_y)):
            ref = band(t, owner, first, half)
            send(ref, ref, to_core, "core_tokens", t, i)

    def far_wait(t):
        for p in range(2):
            arrived(cut(t, at_far, p), "far", t, p).wait_recv()
        ref = band(t, at_far, first, half)
        send(ref, ref, to_core, "core_tokens", t, 2)

    def core_wait(t, *which):
        for i in which:
            owner = (at_x, at_y, at_far)[i]
            arrived(band(t, owner, (1 - core) * half, half), "core_tokens", t, i).wait_recv()

    def core_up_send(k, line, cond):
        other = (1 - core) * near
        inside = jnp.logical_and(line >= other, line < other + near)
        if cond is not None:
            inside = jnp.logical_and(inside, cond)
        send(ups.at[k, line], other_up.at[k, line], to_core, "core_up", k, line, cond=inside)

    def beside(d):
        below, above = z - d, z + d
        return (
            (lax.rem(below + lines, lines), below >= 0, has_up, to_up, "line_up"),
            (lax.rem(above, lines), above < lines, has_down, to_down, "line_down"),
        )

    def gather_step(k, d, who=None):
        for line, cond, onward, to, key in beside(d):
            if who is not None:
                cond = jnp.logical_and(cond, who)
            for w in range(2):
                for side in (y, 1 - y):
                    ref = piece(w, k, line, side)
                    when(cond, arrived(ref, "line", k, w, side, line).wait_recv)
                    send(
                        ref, ref, to, key, k, w, side, line,
                        cond=jnp.logical_and(cond, onward), got_key="line",
                    )
            core_up_send(k, line, cond)

    def compute(k, owner):
        at = pl.ds(pl.multiple_of(owner * rows, rows), rows)
        pre_act = dot(acts[0, at, :], ups[k].reshape(width, step), 1, 0)
        act_grad = dot(acts[1, at, :wide], downs[k, 0], 1, 1)
        for line in range(1, lines):
            act_grad += dot(acts[1, at, line * wide : (line + 1) * wide], downs[k, line], 1, 1)
        r = jnp.maximum(pre_act, 0.0)
        g = (2.0 * r * act_grad).astype(jnp.bfloat16)
        pre_grad[k, at, :] = g
        turned[k, 0, :, at] = g.T
        turned[k, 1, :, at] = (r * r).astype(jnp.bfloat16).T

    def compute_all(k):
        def body(owner, carry):
            compute(k, owner)
            return carry

        lax.fori_loop(0, 4, body, 0)
        hand_over(k)

    def hand_over(k):
        send(pre_grad.at[k], other_pre.at[k], to_core, "core_pre", k)

    def term(k, w, owner):
        cols = pl.ds(pl.multiple_of(owner * wide, wide), wide)
        return dot(turned[k, w], acts[w, :, cols], 1, 0)

    def route(k, w, t):
        turn = lax.rem(t // (lines - 1) + z // near, 2)
        j = lax.rem(t, lines - 1)
        owner = (1 - turn) * (lines - 1 - j) + turn * j
        sign = 1 - 2 * turn
        cond = (owner - z) * sign > 0
        source = z - sign
        has_in = jnp.logical_and(source >= 0, source < lines)
        box = inbox.at[turn, k, w, owner]
        out = leaving.at[k, w, owner]
        copy = pltpu.make_async_remote_copy(
            src_ref=out, dst_ref=box,
            send_sem=send_sems.at[sent.at("reduce", turn, k, w, owner)],
            recv_sem=got_sems.at[got.at("reduce", turn, k, w, owner)],
            device_id=(x, fs + 2 * sign, core), device_id_type=MESH,
        )
        return owner, cond, has_in, box, out, copy

    def pieces(k, w, turn):
        def body(t, carry):
            owner, cond, has_in, box, out, copy = route(k, w, t)

            @pl.when(cond)
            def _():
                partial[...] = term(k, w, owner)

                @pl.when(has_in)
                def _():
                    copy.wait_recv()
                    out[...] = (partial[...] + box[...].astype(jnp.float32)).astype(jnp.bfloat16)

                @pl.when(jnp.logical_not(has_in))
                def _():
                    out[...] = partial[...].astype(jnp.bfloat16)

                copy.start()

            return carry

        lax.fori_loop(turn * (lines - 1), (turn + 1) * (lines - 1), body, 0)

    def pieces_end(k, w):
        def body(t, carry):
            _, cond, _, _, _, copy = route(k, w, t)
            pl.when(cond)(copy.wait_send)
            return carry

        lax.fori_loop(0, 2 * (lines - 1), body, 0)

    def spread_copies(k, w):
        here, there, near_ref = spread.at[w, me, k], spread_far.at[k, w], spread.at[w, at_y, k]
        return (
            remote(there, here, to_y, "spread_y", k, w),
            remote(here, here, to_x, "spread_x", k, w, 0),
            remote(near_ref, near_ref, to_x, "spread_x", k, w, 1),
        )

    def reduce_own(k, w):
        partial[...] = term(k, w, z)
        for turn, cond in ((0, has_down), (1, has_up)):
            box = inbox.at[turn, k, w, z]
            wait = arrived(box, "reduce", turn, k, w, z)

            @pl.when(cond)
            def _():
                wait.wait_recv()
                partial[...] += box[...].astype(jnp.float32)

        if w == 1:
            square = partial[...] * partial[...]
            folded = square[:, :128]
            for at in range(128, wide, 128):
                folded += square[:, at : at + 128]
            row_norms[z, me, :, k * step : (k + 1) * step] = jnp.broadcast_to(
                jnp.sum(folded.T, axis=0, keepdims=True), (8, step)
            )
        here, there = spread.at[w, me, k], spread_far.at[k, w]
        there[...] = partial[:, pl.ds(pl.multiple_of((1 - y) * depth, depth), depth)].astype(jnp.bfloat16)
        here[...] = partial[:, pl.ds(pl.multiple_of(y * depth, depth), depth)].astype(jnp.bfloat16)
        to_near, to_side, _ = spread_copies(k, w)
        to_near.start()
        to_side.start()

    def spread_relay(k, w):
        arrived(spread.at[w, at_y, k], "spread_y", k, w).wait_recv()
        spread_copies(k, w)[2].start()

    def spread_wait(k, w):
        arrived(spread.at[w, at_x, k], "spread_x", k, w, 0).wait_recv()
        arrived(spread.at[w, at_far, k], "spread_x", k, w, 1).wait_recv()

    def norm_copies():
        ref = row_norms.at[z, me]
        for i, j, d, to in others:
            yield pltpu.make_async_remote_copy(
                src_ref=ref, dst_ref=ref,
                send_sem=send_sems.at[sent.at("norms", i, j, d)],
                recv_sem=got_sems.at[got.at("norms", z, me)],
                device_id=to, device_id_type=MESH,
            )

    def norms_send():
        for copy in norm_copies():
            copy.start()

    def norms_end():
        for i, j, d, _ in others:
            line, owner = (z + d) % lines, 2 * ((x + i) % 2) + (y + j) % 2
            arrived(row_norms.at[line, owner], "norms", line, owner).wait_recv()
        for owner in range(4):
            total = row_norms[0, owner, 0:1, :]
            for line in range(1, lines):
                total += row_norms[line, owner, 0:1, :]
            down_norms[:, owner * mine : (owner + 1) * mine] = total

    def col_send():
        total = jnp.zeros((8, depth), jnp.float32)
        for owner in range(4):
            for k in range(splits):
                block = spread[0, owner, k].astype(jnp.float32)
                total += jnp.sum((block * block).reshape(step // 8, 8, depth), axis=0)
        col_norms[0] = jnp.broadcast_to(jnp.sum(total, axis=0, keepdims=True), (8, depth))
        send(col_norms.at[0], col_norms.at[1], to_core, "core_norms")

    def col_end():
        arrived(col_norms.at[1], "core_norms").wait_recv()
        up_norms[...] = col_norms[0, 0:1, :] + col_norms[1, 0:1, :]

    def share_term(owner):
        at = pl.ds(pl.multiple_of(owner * rows, rows), rows)
        parts = []
        for i in range(near):
            line = core * near + i
            total = None
            for k in range(splits):
                for grads, weights in ((pre_grad, ups), (other_pre, other_up)):
                    a = dot(grads[k, at, :], weights[k, line], 1, 1)
                    total = a if total is None else total + a
            parts.append(total)
        return parts

    def share_send():
        for k in range(splits):
            arrived(other_pre.at[k], "core_pre", k).wait_recv()
            for i in range(near):
                line = core * near + i
                arrived(other_up.at[k, line], "core_up", k, line).wait_recv()
        for j, (owner, to) in enumerate(((at_far, to_far), (at_x, to_x), (at_y, to_y))):
            for i, part in enumerate(share_term(owner)):
                share_leaving[j, :, i * wide : (i + 1) * wide] = part.astype(jnp.bfloat16)
            send(share_leaving.at[j], share_got.at[j], to, "share", j)
        for i, part in enumerate(share_term(me)):
            share_sum[:, i * wide : (i + 1) * wide] = part

    def share_end():
        for j in range(3):
            arrived(share_got.at[j], "share", j).wait_recv()
            share_sum[...] += share_got[j].astype(jnp.float32)
        place = share_out.at[:, pl.ds(pl.multiple_of(core * mid, mid), mid)]
        send(share_sum, place, to_core, "core_share")
        return fetch(share_sum, place, "share")

    def line_own(k, side):
        if side is not y:
            pair_wait(k)
        line_send(k, side)
        if side is not y:
            core_up_send(k, z, None)

    def gets_wait(k):
        for w in range(2):
            gets[k, w].wait()

    def finish(at):
        pieces(*grads[at], 1)
        if at:
            spread_relay(*grads[at - 1])
        reduce_own(*grads[at])

    other = 1 - y
    pair_send(0)
    gets_wait(0)
    line_own(0, y)
    gets[0].wait()
    near_send(0)
    if splits > 1:
        pair_send(1)
    gets[1].wait()
    near_send(1)
    for k in range(2, splits):
        pair_send(k)
    line_own(0, other)
    if splits > 1:
        gets_wait(1)
        line_own(1, y)
    relay(0)
    gather_step(0, 1)
    near_wait(0)
    for d in range(2, lines - 1):
        gather_step(0, d)
    if splits > 1:
        line_own(1, other)
        gather_step(1, 1, middle)
    relay(1)
    for k in range(2, splits):
        gets_wait(k)
        line_own(k, y)
    near_wait(1)
    gather_step(0, lines - 1)
    core_wait(0, 0, 1)
    core_wait(1, 0, 1)
    if splits > 1:
        for d in range(2, lines - 1):
            gather_step(1, d, middle)
    for owner in (me, at_x, at_y):
        compute(0, owner)
    for k in range(2, splits):
        line_own(k, other)
    far_wait(0)
    far_wait(1)
    core_wait(0, 2)
    core_wait(1, 2)
    compute(0, at_far)
    hand_over(0)

    grads = [(k, w) for k in range(splits) for w in range(2)]
    jobs = []
    for at, (k, w) in enumerate(grads):
        jobs.append(functools.partial(pieces, k, w, 0))
        if at >= LAG:
            jobs.append(functools.partial(finish, at - LAG))
    jobs += [functools.partial(finish, at) for at in range(max(0, len(grads) - LAG), len(grads) - 1)]
    jobs.append(functools.partial(pieces, *grads[-1], 1))

    def both_pieces(k):
        @pl.when(end)
        def _():
            for w in range(2):
                pieces(k, w, 0)

        if k >= splits - 2 and k:

            @pl.when(middle)
            def _():
                jobs.pop(0)()

    both_pieces(0)
    for k in range(1, splits):
        if k + 1 < splits:
            for d in range(1, lines - 1):
                gather_step(k + 1, d, middle)
        for d in range(1, lines):
            gather_step(k, d, end)
        compute_all(k)
        both_pieces(k)
    share_send()

    @pl.when(middle)
    def _():
        while jobs:
            jobs.pop(0)()

    @pl.when(end)
    def _():
        for at, (k, w) in enumerate(grads[:-1]):
            reduce_own(k, w)
            if at:
                spread_relay(*grads[at - 1])

    out = share_end()
    if len(grads) > 1:
        spread_relay(*grads[-2])
    reduce_own(*grads[-1])
    norms_send()
    spread_relay(*grads[-1])
    for k in range(splits):
        spread_wait(k, 0)
    col_send()
    norms_end()
    for k in range(splits):
        spread_wait(k, 1)
    col_end()
    ends = [fetch(spread.at[w], ref, "out", w) for w, ref in enumerate((up_out, down_out))]
    arrived(share_out.at[:, pl.ds(pl.multiple_of((1 - core) * mid, mid), mid)], "core_share").wait_recv()
    for cond, copy in pending:
        when(cond, copy.wait_send)
    for copy in norm_copies():
        copy.wait_send()
    for k, w in grads:
        pieces_end(k, w)
        for copy in spread_copies(k, w):
            copy.wait_send()
    out.wait()
    for copy in ends:
        copy.wait()


def plane_fits(inputs, up_weight, down_weight):
    reps, groups, cores = (lax.axis_size(axis) for axis in ("rep", "fs", "tp"))
    if reps != 2 or cores != 2 or groups % 4:
        return False
    rows, width = inputs.shape
    depth, units = up_weight.shape
    step = units // 4 // SPLITS
    even = rows % 128 == 0 and depth % 128 == 0 and step % 128 == 0 and width == groups * depth
    held = 2 * 4 * rows * width * 2 + 4 * (units // 4) * width * 2
    return even and held <= 16 * 2**20


def plane_plan(inputs, cotangent, up_weight, down_weight):
    groups = lax.axis_size("fs")
    lines, splits = groups // 2, SPLITS
    rows, width = inputs.shape
    depth, units = up_weight.shape
    step = units // 4 // splits
    wide = 2 * depth
    plane = 4 * rows
    sent, got, local = plane_slots(lines, splits)
    narrow, full = jnp.bfloat16, jnp.float32
    anywhere = pl.BlockSpec(memory_space=pl.ANY)
    share, up, down, norms_up, norms_down = pl.pallas_call(
        functools.partial(plane_kernel, lines, splits, sent, got, local),
        out_shape=(
            jax.ShapeDtypeStruct((rows, width), full),
            jax.ShapeDtypeStruct((4, splits, step, depth), narrow),
            jax.ShapeDtypeStruct((4, splits, step, depth), narrow),
            jax.ShapeDtypeStruct((1, depth), full),
            jax.ShapeDtypeStruct((1, units), full),
        ),
        in_specs=[anywhere] * 4,
        out_specs=(anywhere,) * 3 + (pl.BlockSpec(memory_space=pltpu.VMEM),) * 2,
        scratch_shapes=[
            pltpu.VMEM((2, plane, width), narrow),
            pltpu.VMEM((splits, lines, wide, step), narrow),
            pltpu.VMEM((splits, lines, step, wide), narrow),
            pltpu.VMEM((splits, lines, wide, step), narrow),
            pltpu.VMEM((splits, plane, step), narrow),
            pltpu.VMEM((splits, plane, step), narrow),
            pltpu.VMEM((splits, 2, step, plane), narrow),
            pltpu.VMEM((splits, 2, lines, step, wide), narrow),
            pltpu.VMEM((2, splits, 2, lines, step, wide), narrow),
            pltpu.VMEM((step, wide), full),
            pltpu.VMEM((2, 4, splits, step, depth), narrow),
            pltpu.VMEM((splits, 2, step, depth), narrow),
            pltpu.VMEM((3, rows, width // 2), narrow),
            pltpu.VMEM((3, rows, width // 2), narrow),
            pltpu.VMEM((rows, width // 2), full),
            pltpu.VMEM((lines, 4, 8, units // 4), full),
            pltpu.VMEM((2, 8, depth), full),
            pltpu.SemaphoreType.DMA((sent.size,)),
            pltpu.SemaphoreType.DMA((got.size,)),
            pltpu.SemaphoreType.DMA((local.size,)),
        ],
        compiler_params=pltpu.CompilerParams(
            collective_id=0, has_side_effects=True, vmem_limit_bytes=63 * 2**20
        ),
        name="plane",
    )(inputs, cotangent, up_weight, down_weight)
    grad_up = up.reshape(units, depth).T.astype(full)
    grad_down = down.reshape(units, depth).astype(full)
    return (share, grad_up, grad_down, norms_up.reshape(depth), norms_down.reshape(units))


def shards(inputs, cotangent, up_weight, down_weight):
    tokens = inputs.size * lax.axis_size("fs") // lax.axis_size("tp")
    weights = up_weight.size * lax.axis_size("fs")
    plan = token_plan if tokens <= weights else weight_plan
    if plane_fits(inputs, up_weight, down_weight):
        plan = plane_plan
    return plan(inputs, cotangent, up_weight, down_weight)


def solution(mesh):
    return jax.shard_map(
        shards,
        mesh=mesh,
        in_specs=(P(("rep", "fs"), None), P(("rep", "fs"), None), P("fs", "tp"), P("tp", "fs")),
        out_specs=(P(("rep", "fs"), None), P("fs", "tp"), P("tp", "fs"), P("fs"), P("tp")),
        check_vma=False,
    )
```

```python
import functools

import jax
import jax.numpy as jnp
from jax import lax
from jax.experimental import pallas as pl
from jax.experimental.pallas import tpu as pltpu
from jax.sharding import PartitionSpec as P

NARROW = jnp.bfloat16
CHUNKS = 2


def contract(left, right, left_dim, right_dim):
    return lax.dot_general(
        left, right, (((left_dim,), (right_dim,)), ((), ())), preferred_element_type=jnp.float32
    )


def own_block(blocks, axis, shift=0):
    size = lax.axis_size(axis)
    return lax.dynamic_index_in_dim(
        blocks, lax.rem(lax.axis_index(axis) + shift, size), 0, keepdims=False
    )


def rotate(block, axis, shift):
    size = lax.axis_size(axis)
    return lax.ppermute(block, axis, [(at, (at + shift) % size) for at in range(size)])


def scatter_sum(blocks, axis):
    total = own_block(blocks, axis)
    for shift in range(1, lax.axis_size(axis)):
        sent = own_block(blocks, axis, shift).astype(NARROW)
        total = total + rotate(sent, axis, shift).astype(jnp.float32)
    return total


def gather_blocks(block, axis):
    size = lax.axis_size(axis)
    me = lax.axis_index(axis)
    held = [block] + [rotate(block, axis, shift) for shift in range(1, size)]
    placed = []
    for at in range(size):
        pick = held[0]
        for shift in range(1, size):
            pick = jnp.where(lax.rem(me - at + size, size) == shift, held[shift], pick)
        placed.append(pick)
    return jnp.stack(placed)


def fs_sum(blocks, ahead=None):
    groups = lax.axis_size("fs")
    pair = 2 if groups % 2 == 0 else 1
    far = groups // pair
    me = lax.axis_index("fs")
    blocks = blocks.reshape((far, pair) + blocks.shape[1:])

    def near_block(shift):
        return lax.dynamic_index_in_dim(
            blocks, lax.rem(lax.rem(me, pair) + shift, pair), 1, keepdims=False
        )

    held = near_block(0)
    for shift in range(1, pair):
        perm = [(at, at - at % pair + (at + shift) % pair) for at in range(groups)]
        got = lax.ppermute(near_block(shift).astype(NARROW), "fs", perm)
        held = held + got.astype(jnp.float32)

    if ahead is not None:
        held, ahead = lax.optimization_barrier((held, ahead))

    def far_block(shift):
        return lax.dynamic_index_in_dim(held, lax.rem(me // pair + shift, far), 0, keepdims=False)

    total = far_block(0)
    for shift in range(1, far):
        perm = [(at, (at + shift * pair) % groups) for at in range(groups)]
        got = lax.ppermute(far_block(shift).astype(NARROW), "fs", perm)
        total = total + got.astype(jnp.float32)
    return total, ahead


def exchange(blocks, axis):
    return lax.all_to_all(blocks, axis, 0, 0)


def small_sum(value, axis):
    size = lax.axis_size(axis)
    if size & (size - 1):
        return lax.psum(value, axis)
    bit = 1
    while bit < size:
        value = value + lax.ppermute(value, axis, [(at, at ^ bit) for at in range(size)])
        bit *= 2
    return value


def token_plan(inputs, cotangent, up_weight, down_weight):
    reps, groups, cores = (lax.axis_size(axis) for axis in ("rep", "fs", "tp"))
    rows, width = inputs.shape
    depth, units = up_weight.shape
    mine = units // groups
    part = depth // reps
    half = width // cores

    few = mine // reps
    up = own_block(up_weight.reshape(reps, part, groups, mine).transpose(0, 2, 1, 3), "rep")
    down = own_block(down_weight.reshape(groups, reps, few, depth).transpose(1, 0, 2, 3), "rep")
    both = jnp.concatenate([up, down.reshape(groups, part, mine)], axis=1)
    both = gather_blocks(exchange(both, "fs"), "rep")
    up = both[:, :, :part].transpose(1, 0, 2, 3).reshape(width, mine)
    down = both[:, :, part:].reshape(reps, groups, few, depth)
    down = down.transpose(0, 2, 1, 3).reshape(mine, width)
    tokens = lax.all_gather(
        own_block(inputs.reshape(cores, rows // cores, width), "tp"), ("fs", "tp"), axis=0, tiled=True
    )
    cot = lax.all_gather(
        own_block(cotangent.reshape(cores, rows // cores, width), "tp"), ("fs", "tp"), axis=0, tiled=True
    )

    pre_act = contract(tokens, up, 1, 0)
    act_grad = contract(cot, down, 1, 1)
    rectified = jnp.maximum(pre_act, 0.0)
    hidden = (rectified * rectified).astype(jnp.bfloat16)
    pre_grad = (2.0 * rectified * act_grad).astype(jnp.bfloat16)

    up_rows = up.reshape(cores, half, mine)
    share = contract(pre_grad, own_block(up_rows, "tp"), 1, 1)
    for shift in range(1, cores):
        sent = contract(pre_grad, own_block(up_rows, "tp", shift), 1, 1).astype(NARROW)
        share = share + rotate(sent, "tp", shift).astype(jnp.float32)
    chunks = CHUNKS if half % (128 * CHUNKS) == 0 else 1
    share = share.reshape(groups, rows, half)
    step = half // chunks
    def spread(term):
        term = term.reshape(groups, reps, part, mine).transpose(1, 0, 2, 3)
        return exchange(scatter_sum(term, "rep").astype(NARROW), "fs")

    def whole(term):
        term = gather_blocks(term, "rep")
        return term.transpose(0, 2, 1, 3).reshape(depth, units).astype(jnp.float32)

    spreads = (spread(contract(cot, hidden, 0, 0)), spread(contract(tokens, pre_grad, 0, 0)))
    sums = []
    for at in range(chunks):
        ahead = spreads if at == chunks - 1 else None
        total, ahead = fs_sum(share[:, :, at * step : (at + 1) * step], ahead)
        sums.append(total)
    share = jnp.concatenate(sums, axis=1)
    share = gather_blocks(share, "tp")
    grad_inputs = share.transpose(1, 0, 2).reshape(rows, width)

    down_turned, grad_up = whole(ahead[0]), whole(ahead[1])
    norms_up = small_sum(jnp.sum(grad_up * grad_up, axis=1), "tp")
    norms_down = small_sum(jnp.sum(down_turned * down_turned, axis=0), "fs")
    return (grad_inputs, grad_up, down_turned.T, norms_up, norms_down)


def weight_plan(inputs, cotangent, up_weight, down_weight):
    up_whole = lax.all_gather(up_weight, "fs", axis=0, tiled=True)
    pre_act = jnp.dot(inputs, up_whole, preferred_element_type=jnp.float32)
    act_grad = contract(cotangent, lax.all_gather(down_weight, "fs", axis=1, tiled=True), 1, 1)
    rectified = jnp.maximum(pre_act, 0.0)
    hidden = (rectified * rectified).astype(jnp.bfloat16)
    pre_grad = (2.0 * rectified * act_grad).astype(jnp.bfloat16)
    up_part = lax.psum_scatter(
        contract(inputs, pre_grad, 0, 0), "fs", scatter_dimension=0, tiled=True
    )
    down_part = lax.psum_scatter(
        contract(cotangent, hidden, 0, 0), "fs", scatter_dimension=0, tiled=True
    )
    grad_up, down_turned = lax.psum((up_part, down_part), "rep")
    grad_inputs = lax.psum(contract(pre_grad, up_whole, 1, 1), "tp")
    norms_up = lax.psum(jnp.sum(grad_up * grad_up, axis=1), "tp")
    norms_down = lax.psum(jnp.sum(down_turned * down_turned, axis=0), "fs")
    grad_down = down_turned.T
    return (grad_inputs, grad_up, grad_down, norms_up, norms_down)


MESH = pl.DeviceIdType.MESH
SPLITS = 4


def dot(left, right, left_dim, right_dim):
    return lax.dot_general(
        left, right, (((left_dim,), (right_dim,)), ((), ())), preferred_element_type=jnp.float32
    )


class Slots:
    def __init__(self):
        self.size = 0
        self.base = {}

    def add(self, name, *shape):
        self.base[name] = (self.size, shape)
        count = 1
        for extent in shape:
            count *= extent
        self.size += count

    def at(self, name, *index):
        start, shape = self.base[name]
        place = 0
        for extent, position in zip(shape, index, strict=True):
            place = place * extent + position
        return start + place


def plane_slots(lines, splits):
    sent, got, local = Slots(), Slots(), Slots()
    for table in (sent, got):
        table.add("pair", splits, 2)
        table.add("near_x", 2, 2)
        table.add("near_y", 2, 2)
        table.add("far", 2, 2)
        table.add("core_tokens", 2, 3)
        table.add("core_up", splits, lines)
        table.add("core_pre", splits)
        table.add("spread_y", splits, 2)
        table.add("spread_x", splits, 2, 2)
        table.add("share", 3)
        table.add("core_share")
        table.add("core_extra")
        table.add("core_norms")
        table.add("reduce", 2, splits, 2, lines)
    sent.add("norms", 2, 2, lines)
    got.add("norms", lines, 4)
    sent.add("line_up", splits, 2, 2, lines)
    sent.add("line_down", splits, 2, 2, lines)
    got.add("line", splits, 2, 2, lines)
    local.add("tokens", 2)
    local.add("weights", splits, 2)
    local.add("core_share")
    local.add("core_extra")
    local.add("up", splits, 4)
    local.add("down", splits)
    return sent, got, local


def plane_kernel(
    lines, splits, sent, got, local,
    tokens_hbm, cot_hbm, up_hbm, down_hbm,
    share_out, extra_out, up_out, down_out, up_norms, down_norms,
    acts, ups, downs, other_up, pre_grad, other_pre, turned,
    leaving, inbox, partial, spread, spread_far, share_leaving, share_got, share_sum,
    row_norms, col_norms, up_turned,
    send_sems, got_sems, local_sems,
):
    rows, width = tokens_hbm.shape
    depth, units = up_hbm.shape
    mine = units // 4
    step = mine // splits
    wide = 2 * depth
    half = rows // 2
    part = half // 4
    near = lines // 2
    mid = width // 2

    x = lax.axis_index("rep")
    fs = lax.axis_index("fs")
    core = lax.axis_index("tp")
    z, y = fs // 2, fs % 2
    me = 2 * x + y
    at_x, at_y, at_far = 2 * (1 - x) + y, 2 * x + 1 - y, 2 * (1 - x) + 1 - y
    to_x = (1 - x, fs, core)
    to_y = (x, 2 * z + 1 - y, core)
    to_far = (1 - x, 2 * z + 1 - y, core)
    to_core = (x, fs, 1 - core)
    to_up = (x, fs + 2, core)
    to_down = (x, fs - 2, core)
    has_up, has_down = z < lines - 1, z > 0
    middle = jnp.logical_and(has_up, has_down)
    end = jnp.logical_not(middle)
    pending = []

    def when(cond, act):
        if cond is None:
            act()
        else:
            pl.when(cond)(act)

    def remote(src, dst, to, key, *index, got_key=None):
        return pltpu.make_async_remote_copy(
            src_ref=src, dst_ref=dst,
            send_sem=send_sems.at[sent.at(key, *index)],
            recv_sem=got_sems.at[got.at(got_key or key, *index)],
            device_id=to, device_id_type=MESH,
        )

    def send(src, dst, to, key, *index, cond=None, got_key=None):
        copy = remote(src, dst, to, key, *index, got_key=got_key)
        when(cond, copy.start)
        pending.append((cond, copy))

    def arrived(dst, key, *index):
        return pltpu.make_async_remote_copy(
            src_ref=dst, dst_ref=dst, send_sem=send_sems.at[0],
            recv_sem=got_sems.at[got.at(key, *index)],
            device_id=to_core, device_id_type=MESH,
        )

    def fetch(src, dst, key, *index):
        copy = pltpu.make_async_copy(src, dst, local_sems.at[local.at(key, *index)])
        copy.start()
        return copy

    def up_piece(k, line, side):
        return ups.at[k, line, pl.ds(pl.multiple_of(side * depth, depth), depth), :]

    def down_piece(k, line, side):
        return downs.at[k, line, :, pl.ds(pl.multiple_of(side * depth, depth), depth)]

    def piece(w, k, line, side):
        return (up_piece, down_piece)[w](k, line, side)

    def own(w, owner, k):
        at = pl.ds(pl.multiple_of(owner * mine + k * step, step), step)
        return up_hbm.at[:, at] if w == 0 else down_hbm.at[at, :]

    def band(t, owner, first, count):
        return acts.at[t, pl.ds(pl.multiple_of(owner * rows + first, part), count), :]

    gets = {}
    for k in range(splits):
        for w in range(2):
            gets[k, w] = fetch(own(w, me, k), piece(w, k, z, y), "weights", k, w)
        if k == 0:
            for t, src in ((0, tokens_hbm), (1, cot_hbm)):
                gets[t] = fetch(src, band(t, me, 0, rows), "tokens", t)

    others = [
        (i, j, d, ((x + i) % 2, (z + d) % lines * 2 + (y + j) % 2, core))
        for i in range(2)
        for j in range(2)
        for d in range(lines)
        if i or j or d
    ]
    barrier = pltpu.get_barrier_semaphore()
    for to in (to_x, to_y, to_core):
        pl.semaphore_signal(barrier, inc=1, device_id=to, device_id_type=MESH)
    for cond, to in ((has_up, to_up), (has_down, to_down)):

        @pl.when(cond)
        def _():
            pl.semaphore_signal(barrier, inc=1, device_id=to, device_id_type=MESH)

    pl.semaphore_wait(barrier, 3 + has_up.astype(jnp.int32) + has_down.astype(jnp.int32))

    def pair_send(k):
        for w in range(2):
            send(own(w, at_y, k), piece(w, k, z, y), to_y, "pair", k, w)

    def line_send(k, side):
        for w in range(2):
            ref = piece(w, k, z, side)
            send(ref, ref, to_up, "line_up", k, w, side, z, cond=has_up, got_key="line")
            send(ref, ref, to_down, "line_down", k, w, side, z, cond=has_down, got_key="line")

    def pair_wait(k):
        for w in range(2):
            arrived(piece(w, k, z, 1 - y), "pair", k, w).wait_recv()

    first = core * half

    cuts = ((0, part), (part, half - part))

    def cut(t, owner, p):
        return band(t, owner, first + cuts[p][0], cuts[p][1])

    def near_send(t):
        for p in range(2):
            ref = cut(t, me, p)
            send(ref, ref, to_x, "near_x", t, p)
            ref = cut(t, me, 1 - p)
            send(ref, ref, to_y, "near_y", t, 1 - p)

    def relay(t):
        ref = cut(t, at_x, 0)
        arrived(ref, "near_x", t, 0).wait_recv()
        send(ref, ref, to_y, "far", t, 0)
        ref = cut(t, at_y, 1)
        arrived(ref, "near_y", t, 1).wait_recv()
        send(ref, ref, to_x, "far", t, 1)

    def near_wait(t):
        arrived(cut(t, at_x, 1), "near_x", t, 1).wait_recv()
        arrived(cut(t, at_y, 0), "near_y", t, 0).wait_recv()
        for i, owner in enumerate((at_x, at_y)):
            ref = band(t, owner, first, half)
            send(ref, ref, to_core, "core_tokens", t, i)

    def far_wait(t):
        for p in range(2):
            arrived(cut(t, at_far, p), "far", t, p).wait_recv()
        ref = band(t, at_far, first, half)
        send(ref, ref, to_core, "core_tokens", t, 2)

    def core_wait(t, *which):
        for i in which:
            owner = (at_x, at_y, at_far)[i]
            arrived(band(t, owner, (1 - core) * half, half), "core_tokens", t, i).wait_recv()

    def core_up_send(k, line, cond):
        other = (1 - core) * near
        inside = jnp.logical_and(line >= other, line < other + near)
        if cond is not None:
            inside = jnp.logical_and(inside, cond)
        send(ups.at[k, line], other_up.at[k, line], to_core, "core_up", k, line, cond=inside)

    def beside(d):
        below, above = z - d, z + d
        return (
            (lax.rem(below + lines, lines), below >= 0, has_up, to_up, "line_up"),
            (lax.rem(above, lines), above < lines, has_down, to_down, "line_down"),
        )

    def gather_step(k, d, who=None):
        for line, cond, onward, to, key in beside(d):
            if who is not None:
                cond = jnp.logical_and(cond, who)
            for w in range(2):
                for side in (y, 1 - y):
                    ref = piece(w, k, line, side)
                    when(cond, arrived(ref, "line", k, w, side, line).wait_recv)
                    send(
                        ref, ref, to, key, k, w, side, line,
                        cond=jnp.logical_and(cond, onward), got_key="line",
                    )
            core_up_send(k, line, cond)

    def compute(k, owner):
        at = pl.ds(pl.multiple_of(owner * rows, rows), rows)
        pre_act = dot(acts[0, at, :], ups[k].reshape(width, step), 1, 0)
        act_grad = dot(acts[1, at, :wide], downs[k, 0], 1, 1)
        for line in range(1, lines):
            act_grad += dot(acts[1, at, line * wide : (line + 1) * wide], downs[k, line], 1, 1)
        r = jnp.maximum(pre_act, 0.0)
        g = (2.0 * r * act_grad).astype(jnp.bfloat16)
        pre_grad[k, at, :] = g
        turned[k, 0, :, at] = g.T
        turned[k, 1, :, at] = (r * r).astype(jnp.bfloat16).T

    def compute_all(k):
        def body(owner, carry):
            compute(k, owner)
            return carry

        lax.fori_loop(0, 4, body, 0)
        hand_over(k)

    def hand_over(k):
        send(pre_grad.at[k], other_pre.at[k], to_core, "core_pre", k)

    def term(k, w, owner):
        cols = pl.ds(pl.multiple_of(owner * wide, wide), wide)
        return dot(turned[k, w], acts[w, :, cols], 1, 0)

    def route(k, w, t):
        turn = lax.rem(t // (lines - 1) + z // near, 2)
        j = lax.rem(t, lines - 1)
        owner = (1 - turn) * (lines - 1 - j) + turn * j
        sign = 1 - 2 * turn
        cond = (owner - z) * sign > 0
        source = z - sign
        has_in = jnp.logical_and(source >= 0, source < lines)
        box = inbox.at[turn, k, w, owner]
        out = leaving.at[k, w, owner]
        copy = pltpu.make_async_remote_copy(
            src_ref=out, dst_ref=box,
            send_sem=send_sems.at[sent.at("reduce", turn, k, w, owner)],
            recv_sem=got_sems.at[got.at("reduce", turn, k, w, owner)],
            device_id=(x, fs + 2 * sign, core), device_id_type=MESH,
        )
        return owner, cond, has_in, box, out, copy

    def pieces(k, turn):
        def body(u, carry):
            w = lax.rem(u, 2)
            t = turn * (lines - 1) + u // 2
            owner, cond, has_in, box, out, copy = route(k, w, t)

            @pl.when(cond)
            def _():
                partial[...] = term(k, w, owner)

                @pl.when(has_in)
                def _():
                    copy.wait_recv()
                    out[...] = (partial[...] + box[...].astype(jnp.float32)).astype(jnp.bfloat16)

                @pl.when(jnp.logical_not(has_in))
                def _():
                    out[...] = partial[...].astype(jnp.bfloat16)

                copy.start()

            return carry

        lax.fori_loop(0, 2 * (lines - 1), body, 0)

    def pieces_end(k, w):
        def body(t, carry):
            _, cond, _, _, _, copy = route(k, w, t)
            pl.when(cond)(copy.wait_send)
            return carry

        lax.fori_loop(0, 2 * (lines - 1), body, 0)

    def spread_copies(k, w):
        here, there, near_ref = spread.at[w, me, k], spread_far.at[k, w], spread.at[w, at_y, k]
        return (
            remote(there, here, to_y, "spread_y", k, w),
            remote(here, here, to_x, "spread_x", k, w, 0),
            remote(near_ref, near_ref, to_x, "spread_x", k, w, 1),
        )

    def reduce_own(k, w):
        partial[...] = term(k, w, z)
        for turn, cond in ((0, has_down), (1, has_up)):
            box = inbox.at[turn, k, w, z]
            wait = arrived(box, "reduce", turn, k, w, z)

            @pl.when(cond)
            def _():
                wait.wait_recv()
                partial[...] += box[...].astype(jnp.float32)

        if w == 1:
            square = partial[...] * partial[...]
            folded = square[:, :128]
            for at in range(128, wide, 128):
                folded += square[:, at : at + 128]
            row_norms[z, me, :, k * step : (k + 1) * step] = jnp.broadcast_to(
                jnp.sum(folded.T, axis=0, keepdims=True), (8, step)
            )
        here, there = spread.at[w, me, k], spread_far.at[k, w]
        there[...] = partial[:, pl.ds(pl.multiple_of((1 - y) * depth, depth), depth)].astype(jnp.bfloat16)
        here[...] = partial[:, pl.ds(pl.multiple_of(y * depth, depth), depth)].astype(jnp.bfloat16)
        to_near, to_side, _ = spread_copies(k, w)
        to_near.start()
        to_side.start()

    def spread_relay(k, w):
        arrived(spread.at[w, at_y, k], "spread_y", k, w).wait_recv()
        spread_copies(k, w)[2].start()

    def spread_wait(k, w):
        arrived(spread.at[w, at_x, k], "spread_x", k, w, 0).wait_recv()
        arrived(spread.at[w, at_far, k], "spread_x", k, w, 1).wait_recv()

    def norm_copies():
        ref = row_norms.at[z, me]
        for i, j, d, to in others:
            yield pltpu.make_async_remote_copy(
                src_ref=ref, dst_ref=ref,
                send_sem=send_sems.at[sent.at("norms", i, j, d)],
                recv_sem=got_sems.at[got.at("norms", z, me)],
                device_id=to, device_id_type=MESH,
            )

    def norms_send():
        for copy in norm_copies():
            copy.start()

    def norms_end():
        for i, j, d, _ in others:
            line, owner = (z + d) % lines, 2 * ((x + i) % 2) + (y + j) % 2
            arrived(row_norms.at[line, owner], "norms", line, owner).wait_recv()
        for owner in range(4):
            total = row_norms[0, owner, 0:1, :]
            for line in range(1, lines):
                total += row_norms[line, owner, 0:1, :]
            down_norms[:, owner * mine : (owner + 1) * mine] = total

    def deliver(k):
        spread_wait(k, 0)
        total = jnp.zeros((8, depth), jnp.float32) if k == 0 else col_norms[0]
        copies = []
        for owner in range(4):
            block = spread[0, owner, k]
            wider = block.astype(jnp.float32)
            total += jnp.sum((wider * wider).reshape(step // 8, 8, depth), axis=0)
            at = pl.ds(owner * mine + k * step, step)
            up_turned[:, at] = block.T
            copies.append(fetch(up_turned.at[:, at], up_out.at[:, at], "up", k, owner))
        if k == splits - 1:
            total = jnp.broadcast_to(jnp.sum(total, axis=0, keepdims=True), (8, depth))
        col_norms[0] = total
        if k == splits - 1:
            send(col_norms.at[0], col_norms.at[1], to_core, "core_norms")
        spread_wait(k, 1)
        copies.append(fetch(spread.at[1, :, k], down_out.at[:, k], "down", k))
        return copies

    def col_end():
        arrived(col_norms.at[1], "core_norms").wait_recv()
        up_norms[...] = col_norms[0, 0:1, :] + col_norms[1, 0:1, :]

    def share_term(owner):
        at = pl.ds(pl.multiple_of(owner * rows, rows), rows)
        parts = []
        for i in range(near):
            line = core * near + i
            total = None
            for k in range(splits):
                for grads, weights in ((pre_grad, ups), (other_pre, other_up)):
                    a = dot(grads[k, at, :], weights[k, line], 1, 1)
                    total = a if total is None else total + a
            parts.append(total)
        return parts

    def share_send():
        for k in range(splits):
            arrived(other_pre.at[k], "core_pre", k).wait_recv()
            for i in range(near):
                line = core * near + i
                arrived(other_up.at[k, line], "core_up", k, line).wait_recv()
        for j, (owner, to) in enumerate(((at_far, to_far), (at_x, to_x), (at_y, to_y))):
            for i, part in enumerate(share_term(owner)):
                share_leaving[j, :, i * wide : (i + 1) * wide] = part.astype(jnp.bfloat16)
            send(share_leaving.at[j], share_got.at[j], to, "share", j)
        for i, part in enumerate(share_term(me)):
            share_sum[:, i * wide : (i + 1) * wide] = part

    share_keys = ("core_share", "core_extra")

    def share_end():
        for j in range(3):
            arrived(share_got.at[j], "share", j).wait_recv()
            if j:
                share_sum[...] += share_got[j].astype(jnp.float32)
        copies = []
        for src, ref, key in zip((share_sum, share_got.at[0]), (share_out, extra_out), share_keys, strict=True):
            place = ref.at[:, pl.ds(pl.multiple_of(core * mid, mid), mid)]
            send(src, place, to_core, key)
            copies.append(fetch(src, place, key))
        return copies

    def line_own(k, side):
        if side is not y:
            pair_wait(k)
        line_send(k, side)
        if side is not y:
            core_up_send(k, z, None)

    def gets_wait(k):
        for w in range(2):
            gets[k, w].wait()

    def own_pair(k):
        for w in range(2):
            if k:
                spread_relay(k - 1, w)
            reduce_own(k, w)

    def finish(k):
        pieces(k, 1)
        own_pair(k)

    other = 1 - y
    pair_send(0)
    gets_wait(0)
    line_own(0, y)
    gets[0].wait()
    near_send(0)
    if splits > 1:
        pair_send(1)
    gets[1].wait()
    near_send(1)
    for k in range(2, splits):
        pair_send(k)
    line_own(0, other)
    if splits > 1:
        gets_wait(1)
        line_own(1, y)
    relay(0)
    gather_step(0, 1)
    near_wait(0)
    for d in range(2, lines - 1):
        gather_step(0, d)
    if splits > 1:
        line_own(1, other)
        gather_step(1, 1, middle)
    relay(1)
    for k in range(2, splits):
        gets_wait(k)
        line_own(k, y)
    near_wait(1)
    gather_step(0, lines - 1)
    core_wait(0, 0, 1)
    core_wait(1, 0, 1)
    if splits > 1:
        for d in range(2, lines - 1):
            gather_step(1, d, middle)
    for owner in (me, at_x, at_y):
        compute(0, owner)
    for k in range(2, splits):
        line_own(k, other)
    far_wait(0)
    far_wait(1)
    core_wait(0, 2)
    core_wait(1, 2)
    compute(0, at_far)
    hand_over(0)

    grads = [(k, w) for k in range(splits) for w in range(2)]
    jobs = []
    for k in range(splits):
        jobs.append(functools.partial(pieces, k, 0))
        if k:
            jobs.append(functools.partial(finish, k - 1))
    jobs.append(functools.partial(pieces, splits - 1, 1))

    def both_pieces(k):
        @pl.when(end)
        def _():
            pieces(k, 0)

    both_pieces(0)
    for k in range(1, splits):
        if k + 1 < splits:
            for d in range(1, lines - 1):
                gather_step(k + 1, d, middle)
        for d in range(1, lines):
            gather_step(k, d, end)
        compute_all(k)
        both_pieces(k)
    share_send()

    @pl.when(middle)
    def _():
        for job in jobs:
            job()

    @pl.when(end)
    def _():
        for k in range(splits - 1):
            own_pair(k)

    ends = share_end()
    for k in range(splits - 2):
        ends += deliver(k)
    own_pair(splits - 1)
    norms_send()
    if splits > 1:
        ends += deliver(splits - 2)
    for w in range(2):
        spread_relay(splits - 1, w)
    norms_end()
    ends += deliver(splits - 1)
    col_end()
    for ref in (share_out, extra_out):
        arrived(ref.at[:, pl.ds(pl.multiple_of((1 - core) * mid, mid), mid)], share_keys[ref is extra_out]).wait_recv()
    for cond, copy in pending:
        when(cond, copy.wait_send)
    for copy in norm_copies():
        copy.wait_send()
    for k, w in grads:
        pieces_end(k, w)
        for copy in spread_copies(k, w):
            copy.wait_send()
    for copy in ends:
        copy.wait()


def plane_fits(inputs, up_weight, down_weight):
    reps, groups, cores = (lax.axis_size(axis) for axis in ("rep", "fs", "tp"))
    if reps != 2 or cores != 2 or groups % 4:
        return False
    rows, width = inputs.shape
    depth, units = up_weight.shape
    step = units // 4 // SPLITS
    even = rows % 128 == 0 and depth % 128 == 0 and step % 128 == 0 and width == groups * depth
    held = 2 * 4 * rows * width * 2 + 4 * (units // 4) * width * 2
    return even and held <= 16 * 2**20


def plane_plan(inputs, cotangent, up_weight, down_weight):
    groups = lax.axis_size("fs")
    lines, splits = groups // 2, SPLITS
    rows, width = inputs.shape
    depth, units = up_weight.shape
    step = units // 4 // splits
    wide = 2 * depth
    plane = 4 * rows
    sent, got, local = plane_slots(lines, splits)
    narrow, full = jnp.bfloat16, jnp.float32
    anywhere = pl.BlockSpec(memory_space=pl.ANY)
    share, extra, up, down, norms_up, norms_down = pl.pallas_call(
        functools.partial(plane_kernel, lines, splits, sent, got, local),
        out_shape=(
            jax.ShapeDtypeStruct((rows, width), full),
            jax.ShapeDtypeStruct((rows, width), narrow),
            jax.ShapeDtypeStruct((depth, units), narrow),
            jax.ShapeDtypeStruct((4, splits, step, depth), narrow),
            jax.ShapeDtypeStruct((1, depth), full),
            jax.ShapeDtypeStruct((1, units), full),
        ),
        in_specs=[anywhere] * 4,
        out_specs=(anywhere,) * 4 + (pl.BlockSpec(memory_space=pltpu.VMEM),) * 2,
        scratch_shapes=[
            pltpu.VMEM((2, plane, width), narrow),
            pltpu.VMEM((splits, lines, wide, step), narrow),
            pltpu.VMEM((splits, lines, step, wide), narrow),
            pltpu.VMEM((splits, lines, wide, step), narrow),
            pltpu.VMEM((splits, plane, step), narrow),
            pltpu.VMEM((splits, plane, step), narrow),
            pltpu.VMEM((splits, 2, step, plane), narrow),
            pltpu.VMEM((splits, 2, lines, step, wide), narrow),
            pltpu.VMEM((2, splits, 2, lines, step, wide), narrow),
            pltpu.VMEM((step, wide), full),
            pltpu.VMEM((2, 4, splits, step, depth), narrow),
            pltpu.VMEM((splits, 2, step, depth), narrow),
            pltpu.VMEM((3, rows, width // 2), narrow),
            pltpu.VMEM((3, rows, width // 2), narrow),
            pltpu.VMEM((rows, width // 2), full),
            pltpu.VMEM((lines, 4, 8, units // 4), full),
            pltpu.VMEM((2, 8, depth), full),
            pltpu.VMEM((depth, units), narrow),
            pltpu.SemaphoreType.DMA((sent.size,)),
            pltpu.SemaphoreType.DMA((got.size,)),
            pltpu.SemaphoreType.DMA((local.size,)),
        ],
        compiler_params=pltpu.CompilerParams(
            collective_id=0, has_side_effects=True, vmem_limit_bytes=63 * 2**20
        ),
        name="plane",
    )(inputs, cotangent, up_weight, down_weight)
    grad_up = up.astype(full)
    share = share + extra.astype(full)
    grad_down = down.reshape(units, depth).astype(full)
    return (share, grad_up, grad_down, norms_up.reshape(depth), norms_down.reshape(units))


def shards(inputs, cotangent, up_weight, down_weight):
    tokens = inputs.size * lax.axis_size("fs") // lax.axis_size("tp")
    weights = up_weight.size * lax.axis_size("fs")
    plan = token_plan if tokens <= weights else weight_plan
    if plane_fits(inputs, up_weight, down_weight):
        plan = plane_plan
    return plan(inputs, cotangent, up_weight, down_weight)


def solution(mesh):
    return jax.shard_map(
        shards,
        mesh=mesh,
        in_specs=(P(("rep", "fs"), None), P(("rep", "fs"), None), P("fs", "tp"), P("tp", "fs")),
        out_specs=(P(("rep", "fs"), None), P("fs", "tp"), P("tp", "fs"), P("fs"), P("tp")),
        check_vma=False,
    )
```

```python
import functools

import jax
import jax.numpy as jnp
from jax import lax
from jax.experimental import pallas as pl
from jax.experimental.pallas import tpu as pltpu
from jax.sharding import PartitionSpec as P

NARROW = jnp.bfloat16
CHUNKS = 2


def contract(left, right, left_dim, right_dim):
    return lax.dot_general(
        left, right, (((left_dim,), (right_dim,)), ((), ())), preferred_element_type=jnp.float32
    )


def own_block(blocks, axis, shift=0):
    size = lax.axis_size(axis)
    return lax.dynamic_index_in_dim(
        blocks, lax.rem(lax.axis_index(axis) + shift, size), 0, keepdims=False
    )


def rotate(block, axis, shift):
    size = lax.axis_size(axis)
    return lax.ppermute(block, axis, [(at, (at + shift) % size) for at in range(size)])


def scatter_sum(blocks, axis):
    total = own_block(blocks, axis)
    for shift in range(1, lax.axis_size(axis)):
        sent = own_block(blocks, axis, shift).astype(NARROW)
        total = total + rotate(sent, axis, shift).astype(jnp.float32)
    return total


def gather_blocks(block, axis):
    size = lax.axis_size(axis)
    me = lax.axis_index(axis)
    held = [block] + [rotate(block, axis, shift) for shift in range(1, size)]
    placed = []
    for at in range(size):
        pick = held[0]
        for shift in range(1, size):
            pick = jnp.where(lax.rem(me - at + size, size) == shift, held[shift], pick)
        placed.append(pick)
    return jnp.stack(placed)


def fs_sum(blocks, ahead=None):
    groups = lax.axis_size("fs")
    pair = 2 if groups % 2 == 0 else 1
    far = groups // pair
    me = lax.axis_index("fs")
    blocks = blocks.reshape((far, pair) + blocks.shape[1:])

    def near_block(shift):
        return lax.dynamic_index_in_dim(
            blocks, lax.rem(lax.rem(me, pair) + shift, pair), 1, keepdims=False
        )

    held = near_block(0)
    for shift in range(1, pair):
        perm = [(at, at - at % pair + (at + shift) % pair) for at in range(groups)]
        got = lax.ppermute(near_block(shift).astype(NARROW), "fs", perm)
        held = held + got.astype(jnp.float32)

    if ahead is not None:
        held, ahead = lax.optimization_barrier((held, ahead))

    def far_block(shift):
        return lax.dynamic_index_in_dim(held, lax.rem(me // pair + shift, far), 0, keepdims=False)

    total = far_block(0)
    for shift in range(1, far):
        perm = [(at, (at + shift * pair) % groups) for at in range(groups)]
        got = lax.ppermute(far_block(shift).astype(NARROW), "fs", perm)
        total = total + got.astype(jnp.float32)
    return total, ahead


def exchange(blocks, axis):
    return lax.all_to_all(blocks, axis, 0, 0)


def small_sum(value, axis):
    size = lax.axis_size(axis)
    if size & (size - 1):
        return lax.psum(value, axis)
    bit = 1
    while bit < size:
        value = value + lax.ppermute(value, axis, [(at, at ^ bit) for at in range(size)])
        bit *= 2
    return value


def token_plan(inputs, cotangent, up_weight, down_weight):
    reps, groups, cores = (lax.axis_size(axis) for axis in ("rep", "fs", "tp"))
    rows, width = inputs.shape
    depth, units = up_weight.shape
    mine = units // groups
    part = depth // reps
    half = width // cores

    few = mine // reps
    up = own_block(up_weight.reshape(reps, part, groups, mine).transpose(0, 2, 1, 3), "rep")
    down = own_block(down_weight.reshape(groups, reps, few, depth).transpose(1, 0, 2, 3), "rep")
    both = jnp.concatenate([up, down.reshape(groups, part, mine)], axis=1)
    both = gather_blocks(exchange(both, "fs"), "rep")
    up = both[:, :, :part].transpose(1, 0, 2, 3).reshape(width, mine)
    down = both[:, :, part:].reshape(reps, groups, few, depth)
    down = down.transpose(0, 2, 1, 3).reshape(mine, width)
    tokens = lax.all_gather(
        own_block(inputs.reshape(cores, rows // cores, width), "tp"), ("fs", "tp"), axis=0, tiled=True
    )
    cot = lax.all_gather(
        own_block(cotangent.reshape(cores, rows // cores, width), "tp"), ("fs", "tp"), axis=0, tiled=True
    )

    pre_act = contract(tokens, up, 1, 0)
    act_grad = contract(cot, down, 1, 1)
    rectified = jnp.maximum(pre_act, 0.0)
    hidden = (rectified * rectified).astype(jnp.bfloat16)
    pre_grad = (2.0 * rectified * act_grad).astype(jnp.bfloat16)

    up_rows = up.reshape(cores, half, mine)
    share = contract(pre_grad, own_block(up_rows, "tp"), 1, 1)
    for shift in range(1, cores):
        sent = contract(pre_grad, own_block(up_rows, "tp", shift), 1, 1).astype(NARROW)
        share = share + rotate(sent, "tp", shift).astype(jnp.float32)
    chunks = CHUNKS if half % (128 * CHUNKS) == 0 else 1
    share = share.reshape(groups, rows, half)
    step = half // chunks
    def spread(term):
        term = term.reshape(groups, reps, part, mine).transpose(1, 0, 2, 3)
        return exchange(scatter_sum(term, "rep").astype(NARROW), "fs")

    def whole(term):
        term = gather_blocks(term, "rep")
        return term.transpose(0, 2, 1, 3).reshape(depth, units).astype(jnp.float32)

    spreads = (spread(contract(cot, hidden, 0, 0)), spread(contract(tokens, pre_grad, 0, 0)))
    sums = []
    for at in range(chunks):
        ahead = spreads if at == chunks - 1 else None
        total, ahead = fs_sum(share[:, :, at * step : (at + 1) * step], ahead)
        sums.append(total)
    share = jnp.concatenate(sums, axis=1)
    share = gather_blocks(share, "tp")
    grad_inputs = share.transpose(1, 0, 2).reshape(rows, width)

    down_turned, grad_up = whole(ahead[0]), whole(ahead[1])
    norms_up = small_sum(jnp.sum(grad_up * grad_up, axis=1), "tp")
    norms_down = small_sum(jnp.sum(down_turned * down_turned, axis=0), "fs")
    return (grad_inputs, grad_up, down_turned.T, norms_up, norms_down)


def weight_plan(inputs, cotangent, up_weight, down_weight):
    up_whole = lax.all_gather(up_weight, "fs", axis=0, tiled=True)
    pre_act = jnp.dot(inputs, up_whole, preferred_element_type=jnp.float32)
    act_grad = contract(cotangent, lax.all_gather(down_weight, "fs", axis=1, tiled=True), 1, 1)
    rectified = jnp.maximum(pre_act, 0.0)
    hidden = (rectified * rectified).astype(jnp.bfloat16)
    pre_grad = (2.0 * rectified * act_grad).astype(jnp.bfloat16)
    up_part = lax.psum_scatter(
        contract(inputs, pre_grad, 0, 0), "fs", scatter_dimension=0, tiled=True
    )
    down_part = lax.psum_scatter(
        contract(cotangent, hidden, 0, 0), "fs", scatter_dimension=0, tiled=True
    )
    grad_up, down_turned = lax.psum((up_part, down_part), "rep")
    grad_inputs = lax.psum(contract(pre_grad, up_whole, 1, 1), "tp")
    norms_up = lax.psum(jnp.sum(grad_up * grad_up, axis=1), "tp")
    norms_down = lax.psum(jnp.sum(down_turned * down_turned, axis=0), "fs")
    grad_down = down_turned.T
    return (grad_inputs, grad_up, grad_down, norms_up, norms_down)


MESH = pl.DeviceIdType.MESH
SPLITS = 4


def dot(left, right, left_dim, right_dim):
    return lax.dot_general(
        left, right, (((left_dim,), (right_dim,)), ((), ())), preferred_element_type=jnp.float32
    )


class Slots:
    def __init__(self):
        self.size = 0
        self.base = {}

    def add(self, name, *shape):
        self.base[name] = (self.size, shape)
        count = 1
        for extent in shape:
            count *= extent
        self.size += count

    def at(self, name, *index):
        start, shape = self.base[name]
        place = 0
        for extent, position in zip(shape, index, strict=True):
            place = place * extent + position
        return start + place


def plane_slots(lines, splits):
    sent, got, local = Slots(), Slots(), Slots()
    for table in (sent, got):
        table.add("pair", splits, 2)
        table.add("near_x", 2, 2)
        table.add("near_y", 2, 2)
        table.add("far", 2, 2)
        table.add("core_tokens", 2, 3)
        table.add("core_up", splits, lines)
        table.add("core_pre", splits)
        table.add("spread_y", splits, 2)
        table.add("spread_x", splits, 2, 2)
        table.add("share", 3)
        table.add("core_share")
        table.add("core_extra")
        table.add("core_norms")
        table.add("reduce", 2, splits, 2, lines)
    sent.add("norms", 2, 2, lines)
    got.add("norms", lines, 4)
    sent.add("line_up", splits, 2, 2, lines)
    sent.add("line_down", splits, 2, 2, lines)
    got.add("line", splits, 2, 2, lines)
    local.add("tokens", 2)
    local.add("weights", splits, 2)
    local.add("core_share")
    local.add("core_extra")
    local.add("up", splits, 4)
    local.add("down", splits)
    return sent, got, local


def plane_kernel(
    lines, splits, sent, got, local,
    tokens_hbm, cot_hbm, up_hbm, down_hbm,
    share_out, extra_out, up_out, down_out, up_norms, down_norms,
    acts, ups, downs, other_up, rectified, pre_grad, other_pre, turned,
    leaving, inbox, partial, spread, spread_far, share_leaving, share_got, share_sum,
    row_norms, col_norms, up_turned,
    send_sems, got_sems, local_sems,
):
    rows, width = tokens_hbm.shape
    depth, units = up_hbm.shape
    mine = units // 4
    step = mine // splits
    wide = 2 * depth
    half = rows // 2
    part = half // 4
    near = lines // 2
    mid = width // 2

    x = lax.axis_index("rep")
    fs = lax.axis_index("fs")
    core = lax.axis_index("tp")
    z, y = fs // 2, fs % 2
    me = 2 * x + y
    at_x, at_y, at_far = 2 * (1 - x) + y, 2 * x + 1 - y, 2 * (1 - x) + 1 - y
    to_x = (1 - x, fs, core)
    to_y = (x, 2 * z + 1 - y, core)
    to_far = (1 - x, 2 * z + 1 - y, core)
    to_core = (x, fs, 1 - core)
    to_up = (x, fs + 2, core)
    to_down = (x, fs - 2, core)
    has_up, has_down = z < lines - 1, z > 0
    middle = jnp.logical_and(has_up, has_down)
    end = jnp.logical_not(middle)
    pending = []

    def when(cond, act):
        if cond is None:
            act()
        else:
            pl.when(cond)(act)

    def remote(src, dst, to, key, *index, got_key=None):
        return pltpu.make_async_remote_copy(
            src_ref=src, dst_ref=dst,
            send_sem=send_sems.at[sent.at(key, *index)],
            recv_sem=got_sems.at[got.at(got_key or key, *index)],
            device_id=to, device_id_type=MESH,
        )

    def send(src, dst, to, key, *index, cond=None, got_key=None):
        copy = remote(src, dst, to, key, *index, got_key=got_key)
        when(cond, copy.start)
        pending.append((cond, copy))

    def arrived(dst, key, *index):
        return pltpu.make_async_remote_copy(
            src_ref=dst, dst_ref=dst, send_sem=send_sems.at[0],
            recv_sem=got_sems.at[got.at(key, *index)],
            device_id=to_core, device_id_type=MESH,
        )

    def fetch(src, dst, key, *index):
        copy = pltpu.make_async_copy(src, dst, local_sems.at[local.at(key, *index)])
        copy.start()
        return copy

    def up_piece(k, line, side):
        return ups.at[k, line, pl.ds(pl.multiple_of(side * depth, depth), depth), :]

    def down_piece(k, line, side):
        return downs.at[k, line, :, pl.ds(pl.multiple_of(side * depth, depth), depth)]

    def piece(w, k, line, side):
        return (up_piece, down_piece)[w](k, line, side)

    def own(w, owner, k):
        at = pl.ds(pl.multiple_of(owner * mine + k * step, step), step)
        return up_hbm.at[:, at] if w == 0 else down_hbm.at[at, :]

    def band(t, owner, first, count):
        return acts.at[t, pl.ds(pl.multiple_of(owner * rows + first, part), count), :]

    gets = {}
    for k in range(splits):
        for w in range(2):
            gets[k, w] = fetch(own(w, me, k), piece(w, k, z, y), "weights", k, w)
        if k == 0:
            for t, src in ((0, tokens_hbm), (1, cot_hbm)):
                gets[t] = fetch(src, band(t, me, 0, rows), "tokens", t)

    others = [
        (i, j, d, ((x + i) % 2, (z + d) % lines * 2 + (y + j) % 2, core))
        for i in range(2)
        for j in range(2)
        for d in range(lines)
        if i or j or d
    ]
    barrier = pltpu.get_barrier_semaphore()
    for to in (to_x, to_y, to_core):
        pl.semaphore_signal(barrier, inc=1, device_id=to, device_id_type=MESH)
    for cond, to in ((has_up, to_up), (has_down, to_down)):

        @pl.when(cond)
        def _():
            pl.semaphore_signal(barrier, inc=1, device_id=to, device_id_type=MESH)

    pl.semaphore_wait(barrier, 3 + has_up.astype(jnp.int32) + has_down.astype(jnp.int32))

    def pair_send(k):
        for w in range(2):
            send(own(w, at_y, k), piece(w, k, z, y), to_y, "pair", k, w)

    def line_send(k, side):
        for w in range(2):
            ref = piece(w, k, z, side)
            send(ref, ref, to_up, "line_up", k, w, side, z, cond=has_up, got_key="line")
            send(ref, ref, to_down, "line_down", k, w, side, z, cond=has_down, got_key="line")

    def pair_wait(k):
        for w in range(2):
            arrived(piece(w, k, z, 1 - y), "pair", k, w).wait_recv()

    first = core * half

    cuts = ((0, part), (part, half - part))

    def cut(t, owner, p):
        return band(t, owner, first + cuts[p][0], cuts[p][1])

    def near_send(t):
        for p in range(2):
            ref = cut(t, me, p)
            send(ref, ref, to_x, "near_x", t, p)
            ref = cut(t, me, 1 - p)
            send(ref, ref, to_y, "near_y", t, 1 - p)

    def relay(t):
        ref = cut(t, at_x, 0)
        arrived(ref, "near_x", t, 0).wait_recv()
        send(ref, ref, to_y, "far", t, 0)
        ref = cut(t, at_y, 1)
        arrived(ref, "near_y", t, 1).wait_recv()
        send(ref, ref, to_x, "far", t, 1)

    def near_wait(t):
        arrived(cut(t, at_x, 1), "near_x", t, 1).wait_recv()
        arrived(cut(t, at_y, 0), "near_y", t, 0).wait_recv()
        for i, owner in enumerate((at_x, at_y)):
            ref = band(t, owner, first, half)
            send(ref, ref, to_core, "core_tokens", t, i)

    def far_wait(t):
        for p in range(2):
            arrived(cut(t, at_far, p), "far", t, p).wait_recv()
        ref = band(t, at_far, first, half)
        send(ref, ref, to_core, "core_tokens", t, 2)

    def core_wait(t, *which):
        for i in which:
            owner = (at_x, at_y, at_far)[i]
            arrived(band(t, owner, (1 - core) * half, half), "core_tokens", t, i).wait_recv()

    def core_up_send(k, line, cond):
        other = (1 - core) * near
        inside = jnp.logical_and(line >= other, line < other + near)
        if cond is not None:
            inside = jnp.logical_and(inside, cond)
        send(ups.at[k, line], other_up.at[k, line], to_core, "core_up", k, line, cond=inside)

    def beside(d):
        below, above = z - d, z + d
        return (
            (lax.rem(below + lines, lines), below >= 0, has_up, to_up, "line_up"),
            (lax.rem(above, lines), above < lines, has_down, to_down, "line_down"),
        )

    def gather_step(k, d, who=None):
        for line, cond, onward, to, key in beside(d):
            if who is not None:
                cond = jnp.logical_and(cond, who)
            for w in range(2):
                for side in (y, 1 - y):
                    ref = piece(w, k, line, side)
                    when(cond, arrived(ref, "line", k, w, side, line).wait_recv)
                    send(
                        ref, ref, to, key, k, w, side, line,
                        cond=jnp.logical_and(cond, onward), got_key="line",
                    )
            core_up_send(k, line, cond)

    def hidden(k, owner):
        at = pl.ds(pl.multiple_of(owner * rows, rows), rows)
        r = jnp.maximum(dot(acts[0, at, :], ups[k].reshape(width, step), 1, 0), 0.0)
        rectified[at, :] = r
        turned[k, 1, :, at] = (r * r).astype(jnp.bfloat16).T

    def gradient(k, owner):
        at = pl.ds(pl.multiple_of(owner * rows, rows), rows)
        act_grad = dot(acts[1, at, :wide], downs[k, 0], 1, 1)
        for line in range(1, lines):
            act_grad += dot(acts[1, at, line * wide : (line + 1) * wide], downs[k, line], 1, 1)
        g = (2.0 * rectified[at, :] * act_grad).astype(jnp.bfloat16)
        pre_grad[k, at, :] = g
        turned[k, 0, :, at] = g.T

    def compute(k, owner):
        hidden(k, owner)
        gradient(k, owner)

    def every(act, k):
        def body(owner, carry):
            act(k, owner)
            return carry

        lax.fori_loop(0, 4, body, 0)

    def hand_over(k):
        send(pre_grad.at[k], other_pre.at[k], to_core, "core_pre", k)

    def term(k, w, owner):
        cols = pl.ds(pl.multiple_of(owner * wide, wide), wide)
        return dot(turned[k, w], acts[w, :, cols], 1, 0)

    def route(k, w, t):
        turn = lax.rem(t // (lines - 1) + z // near, 2)
        j = lax.rem(t, lines - 1)
        owner = (1 - turn) * (lines - 1 - j) + turn * j
        sign = 1 - 2 * turn
        cond = (owner - z) * sign > 0
        source = z - sign
        has_in = jnp.logical_and(source >= 0, source < lines)
        box = inbox.at[turn, k, w, owner]
        out = leaving.at[k, w, owner]
        copy = pltpu.make_async_remote_copy(
            src_ref=out, dst_ref=box,
            send_sem=send_sems.at[sent.at("reduce", turn, k, w, owner)],
            recv_sem=got_sems.at[got.at("reduce", turn, k, w, owner)],
            device_id=(x, fs + 2 * sign, core), device_id_type=MESH,
        )
        return owner, cond, has_in, box, out, copy

    def pieces(k, turn):
        def body(u, carry):
            w = 1 - lax.rem(u, 2)
            t = turn * (lines - 1) + u // 2
            owner, cond, has_in, box, out, copy = route(k, w, t)

            @pl.when(cond)
            def _():
                partial[...] = term(k, w, owner)

                @pl.when(has_in)
                def _():
                    copy.wait_recv()
                    out[...] = (partial[...] + box[...].astype(jnp.float32)).astype(jnp.bfloat16)

                @pl.when(jnp.logical_not(has_in))
                def _():
                    out[...] = partial[...].astype(jnp.bfloat16)

                copy.start()

            return carry

        lax.fori_loop(0, 2 * (lines - 1), body, 0)

    def pieces_end(k, w):
        def body(t, carry):
            _, cond, _, _, _, copy = route(k, w, t)
            pl.when(cond)(copy.wait_send)
            return carry

        lax.fori_loop(0, 2 * (lines - 1), body, 0)

    def spread_copies(k, w):
        here, there, near_ref = spread.at[w, me, k], spread_far.at[k, w], spread.at[w, at_y, k]
        return (
            remote(there, here, to_y, "spread_y", k, w),
            remote(here, here, to_x, "spread_x", k, w, 0),
            remote(near_ref, near_ref, to_x, "spread_x", k, w, 1),
        )

    def reduce_own(k, w):
        partial[...] = term(k, w, z)
        for turn, cond in ((0, has_down), (1, has_up)):
            box = inbox.at[turn, k, w, z]
            wait = arrived(box, "reduce", turn, k, w, z)

            @pl.when(cond)
            def _():
                wait.wait_recv()
                partial[...] += box[...].astype(jnp.float32)

        if w == 1:
            square = partial[...] * partial[...]
            folded = square[:, :128]
            for at in range(128, wide, 128):
                folded += square[:, at : at + 128]
            row_norms[z, me, :, k * step : (k + 1) * step] = jnp.sum(folded.T, axis=0, keepdims=True)
        here, there = spread.at[w, me, k], spread_far.at[k, w]
        there[...] = partial[:, pl.ds(pl.multiple_of((1 - y) * depth, depth), depth)].astype(jnp.bfloat16)
        here[...] = partial[:, pl.ds(pl.multiple_of(y * depth, depth), depth)].astype(jnp.bfloat16)
        to_near, to_side, _ = spread_copies(k, w)
        to_near.start()
        to_side.start()

    def spread_relay(k, w):
        arrived(spread.at[w, at_y, k], "spread_y", k, w).wait_recv()
        spread_copies(k, w)[2].start()

    def spread_wait(k, w):
        arrived(spread.at[w, at_x, k], "spread_x", k, w, 0).wait_recv()
        arrived(spread.at[w, at_far, k], "spread_x", k, w, 1).wait_recv()

    def norm_copies():
        ref = row_norms.at[z, me]
        for i, j, d, to in others:
            yield pltpu.make_async_remote_copy(
                src_ref=ref, dst_ref=ref,
                send_sem=send_sems.at[sent.at("norms", i, j, d)],
                recv_sem=got_sems.at[got.at("norms", z, me)],
                device_id=to, device_id_type=MESH,
            )

    def norms_send():
        for copy in norm_copies():
            copy.start()

    def norms_end():
        for i, j, d, _ in others:
            line, owner = (z + d) % lines, 2 * ((x + i) % 2) + (y + j) % 2
            arrived(row_norms.at[line, owner], "norms", line, owner).wait_recv()
        for owner in range(4):
            total = row_norms[0, owner, 0:1, :]
            for line in range(1, lines):
                total += row_norms[line, owner, 0:1, :]
            down_norms[:, owner * mine : (owner + 1) * mine] = total

    def deliver(k):
        spread_wait(k, 1)
        copies = [fetch(spread.at[1, :, k], down_out.at[:, k], "down", k)]
        spread_wait(k, 0)
        total = jnp.zeros((8, depth), jnp.float32) if k == 0 else col_norms[0]
        for owner in range(4):
            block = spread[0, owner, k]
            wider = block.astype(jnp.float32)
            total += jnp.sum((wider * wider).reshape(step // 8, 8, depth), axis=0)
            at = pl.ds(owner * mine + k * step, step)
            up_turned[:, at] = block.T
            copies.append(fetch(up_turned.at[:, at], up_out.at[:, at], "up", k, owner))
        if k == splits - 1:
            total = jnp.broadcast_to(jnp.sum(total, axis=0, keepdims=True), (8, depth))
        col_norms[0] = total
        if k == splits - 1:
            send(col_norms.at[0], col_norms.at[1], to_core, "core_norms")
        return copies

    def col_end():
        arrived(col_norms.at[1], "core_norms").wait_recv()
        up_norms[...] = col_norms[0, 0:1, :] + col_norms[1, 0:1, :]

    def share_term(owner):
        at = pl.ds(pl.multiple_of(owner * rows, rows), rows)
        parts = []
        for i in range(near):
            line = core * near + i
            total = None
            for k in range(splits):
                for grads, weights in ((pre_grad, ups), (other_pre, other_up)):
                    a = dot(grads[k, at, :], weights[k, line], 1, 1)
                    total = a if total is None else total + a
            parts.append(total)
        return parts

    def share_send():
        for k in range(splits):
            arrived(other_pre.at[k], "core_pre", k).wait_recv()
            for i in range(near):
                line = core * near + i
                arrived(other_up.at[k, line], "core_up", k, line).wait_recv()
        for j, (owner, to) in enumerate(((at_far, to_far), (at_x, to_x), (at_y, to_y))):
            for i, part in enumerate(share_term(owner)):
                share_leaving[j, :, i * wide : (i + 1) * wide] = part.astype(jnp.bfloat16)
            send(share_leaving.at[j], share_got.at[j], to, "share", j)
        for i, part in enumerate(share_term(me)):
            share_sum[:, i * wide : (i + 1) * wide] = part

    share_keys = ("core_share", "core_extra")

    def share_end():
        for j in range(3):
            arrived(share_got.at[j], "share", j).wait_recv()
            if j:
                share_sum[...] += share_got[j].astype(jnp.float32)
        copies = []
        for src, ref, key in zip((share_sum, share_got.at[0]), (share_out, extra_out), share_keys, strict=True):
            place = ref.at[:, pl.ds(pl.multiple_of(core * mid, mid), mid)]
            send(src, place, to_core, key)
            copies.append(fetch(src, place, key))
        return copies

    def line_own(k, side):
        if side is not y:
            pair_wait(k)
        line_send(k, side)
        if side is not y:
            core_up_send(k, z, None)

    def gets_wait(k):
        for w in range(2):
            gets[k, w].wait()

    def own_pair(k):
        for w in (1, 0):
            if k:
                spread_relay(k - 1, w)
            reduce_own(k, w)
            if w == 1 and k == splits - 1:
                norms_send()

    def finish(k):
        pieces(k, 1)
        own_pair(k)

    other = 1 - y
    pair_send(0)
    gets_wait(0)
    line_own(0, y)
    gets[0].wait()
    near_send(0)
    if splits > 1:
        pair_send(1)
    gets[1].wait()
    near_send(1)
    for k in range(2, splits):
        pair_send(k)
    line_own(0, other)
    if splits > 1:
        gets_wait(1)
        line_own(1, y)
    relay(0)
    gather_step(0, 1)
    near_wait(0)
    for d in range(2, lines - 1):
        gather_step(0, d)
    if splits > 1:
        line_own(1, other)
        gather_step(1, 1, middle)
    relay(1)
    for k in range(2, splits):
        gets_wait(k)
        line_own(k, y)
    near_wait(1)
    gather_step(0, lines - 1)
    core_wait(0, 0, 1)
    core_wait(1, 0, 1)
    if splits > 1:
        for d in range(2, lines - 1):
            gather_step(1, d, middle)
    for owner in (me, at_x, at_y):
        compute(0, owner)
    for k in range(2, splits):
        line_own(k, other)
    far_wait(0)
    core_wait(0, 2)
    hidden(0, at_far)
    far_wait(1)
    core_wait(1, 2)
    gradient(0, at_far)
    hand_over(0)

    grads = [(k, w) for k in range(splits) for w in range(2)]
    jobs = []
    for k in range(splits):
        jobs.append(functools.partial(pieces, k, 0))
        if k:
            jobs.append(functools.partial(finish, k - 1))
    jobs.append(functools.partial(pieces, splits - 1, 1))

    def end_pieces(k):
        @pl.when(end)
        def _():
            pieces(k, 0)

    end_pieces(0)
    for k in range(1, splits):
        if k + 1 < splits:
            for d in range(1, lines - 1):
                gather_step(k + 1, d, middle)
        for d in range(1, lines):
            gather_step(k, d, end)
        every(compute, k)
        hand_over(k)
        end_pieces(k)
    share_send()

    @pl.when(middle)
    def _():
        for job in jobs:
            job()

    @pl.when(end)
    def _():
        for k in range(splits - 1):
            own_pair(k)

    ends = share_end()
    for k in range(splits - 2):
        ends += deliver(k)
    own_pair(splits - 1)
    if splits > 1:
        ends += deliver(splits - 2)
    for w in (1, 0):
        spread_relay(splits - 1, w)
    norms_end()
    ends += deliver(splits - 1)
    col_end()
    for ref in (share_out, extra_out):
        arrived(ref.at[:, pl.ds(pl.multiple_of((1 - core) * mid, mid), mid)], share_keys[ref is extra_out]).wait_recv()
    for cond, copy in pending:
        when(cond, copy.wait_send)
    for copy in norm_copies():
        copy.wait_send()
    for k, w in grads:
        pieces_end(k, w)
        for copy in spread_copies(k, w):
            copy.wait_send()
    for copy in ends:
        copy.wait()


def plane_fits(inputs, up_weight, down_weight):
    reps, groups, cores = (lax.axis_size(axis) for axis in ("rep", "fs", "tp"))
    if reps != 2 or cores != 2 or groups % 4:
        return False
    rows, width = inputs.shape
    depth, units = up_weight.shape
    step = units // 4 // SPLITS
    even = rows % 128 == 0 and depth % 128 == 0 and step % 128 == 0 and width == groups * depth
    held = 2 * 4 * rows * width * 2 + 4 * (units // 4) * width * 2
    return even and held <= 16 * 2**20


def plane_plan(inputs, cotangent, up_weight, down_weight):
    groups = lax.axis_size("fs")
    lines, splits = groups // 2, SPLITS
    rows, width = inputs.shape
    depth, units = up_weight.shape
    step = units // 4 // splits
    wide = 2 * depth
    plane = 4 * rows
    sent, got, local = plane_slots(lines, splits)
    narrow, full = jnp.bfloat16, jnp.float32
    anywhere = pl.BlockSpec(memory_space=pl.ANY)
    share, extra, up, down, norms_up, norms_down = pl.pallas_call(
        functools.partial(plane_kernel, lines, splits, sent, got, local),
        out_shape=(
            jax.ShapeDtypeStruct((rows, width), full),
            jax.ShapeDtypeStruct((rows, width), narrow),
            jax.ShapeDtypeStruct((depth, units), narrow),
            jax.ShapeDtypeStruct((4, splits, step, depth), narrow),
            jax.ShapeDtypeStruct((1, depth), full),
            jax.ShapeDtypeStruct((1, units), full),
        ),
        in_specs=[anywhere] * 4,
        out_specs=(anywhere,) * 4 + (pl.BlockSpec(memory_space=pltpu.VMEM),) * 2,
        scratch_shapes=[
            pltpu.VMEM((2, plane, width), narrow),
            pltpu.VMEM((splits, lines, wide, step), narrow),
            pltpu.VMEM((splits, lines, step, wide), narrow),
            pltpu.VMEM((splits, lines, wide, step), narrow),
            pltpu.VMEM((plane, step), full),
            pltpu.VMEM((splits, plane, step), narrow),
            pltpu.VMEM((splits, plane, step), narrow),
            pltpu.VMEM((splits, 2, step, plane), narrow),
            pltpu.VMEM((splits, 2, lines, step, wide), narrow),
            pltpu.VMEM((2, splits, 2, lines, step, wide), narrow),
            pltpu.VMEM((step, wide), full),
            pltpu.VMEM((2, 4, splits, step, depth), narrow),
            pltpu.VMEM((splits, 2, step, depth), narrow),
            pltpu.VMEM((3, rows, width // 2), narrow),
            pltpu.VMEM((3, rows, width // 2), narrow),
            pltpu.VMEM((rows, width // 2), full),
            pltpu.VMEM((lines, 4, 1, units // 4), full),
            pltpu.VMEM((2, 8, depth), full),
            pltpu.VMEM((depth, units), narrow),
            pltpu.SemaphoreType.DMA((sent.size,)),
            pltpu.SemaphoreType.DMA((got.size,)),
            pltpu.SemaphoreType.DMA((local.size,)),
        ],
        compiler_params=pltpu.CompilerParams(
            collective_id=0, has_side_effects=True, vmem_limit_bytes=63 * 2**20
        ),
        name="plane",
    )(inputs, cotangent, up_weight, down_weight)
    grad_up = up.astype(full)
    share = share + extra.astype(full)
    grad_down = down.reshape(units, depth).astype(full)
    return (share, grad_up, grad_down, norms_up.reshape(depth), norms_down.reshape(units))


def shards(inputs, cotangent, up_weight, down_weight):
    tokens = inputs.size * lax.axis_size("fs") // lax.axis_size("tp")
    weights = up_weight.size * lax.axis_size("fs")
    plan = token_plan if tokens <= weights else weight_plan
    if plane_fits(inputs, up_weight, down_weight):
        plan = plane_plan
    return plan(inputs, cotangent, up_weight, down_weight)


def solution(mesh):
    return jax.shard_map(
        shards,
        mesh=mesh,
        in_specs=(P(("rep", "fs"), None), P(("rep", "fs"), None), P("fs", "tp"), P("tp", "fs")),
        out_specs=(P(("rep", "fs"), None), P("fs", "tp"), P("tp", "fs"), P("fs"), P("tp")),
        check_vma=False,
    )
```

```python
import functools

import jax
import jax.numpy as jnp
from jax import lax
from jax.experimental import pallas as pl
from jax.experimental.pallas import tpu as pltpu
from jax.sharding import PartitionSpec as P

NARROW = jnp.bfloat16
CHUNKS = 2


def contract(left, right, left_dim, right_dim):
    return lax.dot_general(
        left, right, (((left_dim,), (right_dim,)), ((), ())), preferred_element_type=jnp.float32
    )


def own_block(blocks, axis, shift=0):
    size = lax.axis_size(axis)
    return lax.dynamic_index_in_dim(
        blocks, lax.rem(lax.axis_index(axis) + shift, size), 0, keepdims=False
    )


def rotate(block, axis, shift):
    size = lax.axis_size(axis)
    return lax.ppermute(block, axis, [(at, (at + shift) % size) for at in range(size)])


def scatter_sum(blocks, axis):
    total = own_block(blocks, axis)
    for shift in range(1, lax.axis_size(axis)):
        sent = own_block(blocks, axis, shift).astype(NARROW)
        total = total + rotate(sent, axis, shift).astype(jnp.float32)
    return total


def gather_blocks(block, axis):
    size = lax.axis_size(axis)
    me = lax.axis_index(axis)
    held = [block] + [rotate(block, axis, shift) for shift in range(1, size)]
    placed = []
    for at in range(size):
        pick = held[0]
        for shift in range(1, size):
            pick = jnp.where(lax.rem(me - at + size, size) == shift, held[shift], pick)
        placed.append(pick)
    return jnp.stack(placed)


def fs_sum(blocks, ahead=None):
    groups = lax.axis_size("fs")
    pair = 2 if groups % 2 == 0 else 1
    far = groups // pair
    me = lax.axis_index("fs")
    blocks = blocks.reshape((far, pair) + blocks.shape[1:])

    def near_block(shift):
        return lax.dynamic_index_in_dim(
            blocks, lax.rem(lax.rem(me, pair) + shift, pair), 1, keepdims=False
        )

    held = near_block(0)
    for shift in range(1, pair):
        perm = [(at, at - at % pair + (at + shift) % pair) for at in range(groups)]
        got = lax.ppermute(near_block(shift).astype(NARROW), "fs", perm)
        held = held + got.astype(jnp.float32)

    if ahead is not None:
        held, ahead = lax.optimization_barrier((held, ahead))

    def far_block(shift):
        return lax.dynamic_index_in_dim(held, lax.rem(me // pair + shift, far), 0, keepdims=False)

    total = far_block(0)
    for shift in range(1, far):
        perm = [(at, (at + shift * pair) % groups) for at in range(groups)]
        got = lax.ppermute(far_block(shift).astype(NARROW), "fs", perm)
        total = total + got.astype(jnp.float32)
    return total, ahead


def exchange(blocks, axis):
    return lax.all_to_all(blocks, axis, 0, 0)


def small_sum(value, axis):
    size = lax.axis_size(axis)
    if size & (size - 1):
        return lax.psum(value, axis)
    bit = 1
    while bit < size:
        value = value + lax.ppermute(value, axis, [(at, at ^ bit) for at in range(size)])
        bit *= 2
    return value


def token_plan(inputs, cotangent, up_weight, down_weight):
    reps, groups, cores = (lax.axis_size(axis) for axis in ("rep", "fs", "tp"))
    rows, width = inputs.shape
    depth, units = up_weight.shape
    mine = units // groups
    part = depth // reps
    half = width // cores

    few = mine // reps
    up = own_block(up_weight.reshape(reps, part, groups, mine).transpose(0, 2, 1, 3), "rep")
    down = own_block(down_weight.reshape(groups, reps, few, depth).transpose(1, 0, 2, 3), "rep")
    both = jnp.concatenate([up, down.reshape(groups, part, mine)], axis=1)
    both = gather_blocks(exchange(both, "fs"), "rep")
    up = both[:, :, :part].transpose(1, 0, 2, 3).reshape(width, mine)
    down = both[:, :, part:].reshape(reps, groups, few, depth)
    down = down.transpose(0, 2, 1, 3).reshape(mine, width)
    tokens = lax.all_gather(
        own_block(inputs.reshape(cores, rows // cores, width), "tp"), ("fs", "tp"), axis=0, tiled=True
    )
    cot = lax.all_gather(
        own_block(cotangent.reshape(cores, rows // cores, width), "tp"), ("fs", "tp"), axis=0, tiled=True
    )

    pre_act = contract(tokens, up, 1, 0)
    act_grad = contract(cot, down, 1, 1)
    rectified = jnp.maximum(pre_act, 0.0)
    hidden = (rectified * rectified).astype(jnp.bfloat16)
    pre_grad = (2.0 * rectified * act_grad).astype(jnp.bfloat16)

    up_rows = up.reshape(cores, half, mine)
    share = contract(pre_grad, own_block(up_rows, "tp"), 1, 1)
    for shift in range(1, cores):
        sent = contract(pre_grad, own_block(up_rows, "tp", shift), 1, 1).astype(NARROW)
        share = share + rotate(sent, "tp", shift).astype(jnp.float32)
    chunks = CHUNKS if half % (128 * CHUNKS) == 0 else 1
    share = share.reshape(groups, rows, half)
    step = half // chunks
    def spread(term):
        term = term.reshape(groups, reps, part, mine).transpose(1, 0, 2, 3)
        return exchange(scatter_sum(term, "rep").astype(NARROW), "fs")

    def whole(term):
        term = gather_blocks(term, "rep")
        return term.transpose(0, 2, 1, 3).reshape(depth, units).astype(jnp.float32)

    spreads = (spread(contract(cot, hidden, 0, 0)), spread(contract(tokens, pre_grad, 0, 0)))
    sums = []
    for at in range(chunks):
        ahead = spreads if at == chunks - 1 else None
        total, ahead = fs_sum(share[:, :, at * step : (at + 1) * step], ahead)
        sums.append(total)
    share = jnp.concatenate(sums, axis=1)
    share = gather_blocks(share, "tp")
    grad_inputs = share.transpose(1, 0, 2).reshape(rows, width)

    down_turned, grad_up = whole(ahead[0]), whole(ahead[1])
    norms_up = small_sum(jnp.sum(grad_up * grad_up, axis=1), "tp")
    norms_down = small_sum(jnp.sum(down_turned * down_turned, axis=0), "fs")
    return (grad_inputs, grad_up, down_turned.T, norms_up, norms_down)


def weight_plan(inputs, cotangent, up_weight, down_weight):
    up_whole = lax.all_gather(up_weight, "fs", axis=0, tiled=True)
    pre_act = jnp.dot(inputs, up_whole, preferred_element_type=jnp.float32)
    act_grad = contract(cotangent, lax.all_gather(down_weight, "fs", axis=1, tiled=True), 1, 1)
    rectified = jnp.maximum(pre_act, 0.0)
    hidden = (rectified * rectified).astype(jnp.bfloat16)
    pre_grad = (2.0 * rectified * act_grad).astype(jnp.bfloat16)
    up_part = lax.psum_scatter(
        contract(inputs, pre_grad, 0, 0), "fs", scatter_dimension=0, tiled=True
    )
    down_part = lax.psum_scatter(
        contract(cotangent, hidden, 0, 0), "fs", scatter_dimension=0, tiled=True
    )
    grad_up, down_turned = lax.psum((up_part, down_part), "rep")
    grad_inputs = lax.psum(contract(pre_grad, up_whole, 1, 1), "tp")
    norms_up = lax.psum(jnp.sum(grad_up * grad_up, axis=1), "tp")
    norms_down = lax.psum(jnp.sum(down_turned * down_turned, axis=0), "fs")
    grad_down = down_turned.T
    return (grad_inputs, grad_up, grad_down, norms_up, norms_down)


MESH = pl.DeviceIdType.MESH
SPLITS = 4


def dot(left, right, left_dim, right_dim):
    return lax.dot_general(
        left, right, (((left_dim,), (right_dim,)), ((), ())), preferred_element_type=jnp.float32
    )


class Slots:
    def __init__(self):
        self.size = 0
        self.base = {}

    def add(self, name, *shape):
        self.base[name] = (self.size, shape)
        count = 1
        for extent in shape:
            count *= extent
        self.size += count

    def at(self, name, *index):
        start, shape = self.base[name]
        place = 0
        for extent, position in zip(shape, index, strict=True):
            place = place * extent + position
        return start + place


def plane_slots(lines, splits):
    sent, got, local = Slots(), Slots(), Slots()
    for table in (sent, got):
        table.add("pair", splits, 2)
        table.add("near_x", 2, 2)
        table.add("near_y", 2, 2)
        table.add("far", 2, 2)
        table.add("core_tokens", 2, 3)
        table.add("core_up", splits, lines)
        table.add("core_pre", splits)
        table.add("spread_y", splits, 2)
        table.add("spread_x", splits, 2, 2)
        table.add("share", 3)
        table.add("core_share")
        table.add("core_extra")
        table.add("core_norms")
        table.add("reduce", 2, splits, 2, lines)
    sent.add("norms", 2, 2, lines)
    got.add("norms", lines, 4)
    sent.add("line_up", splits, 2, 2, lines)
    sent.add("line_down", splits, 2, 2, lines)
    got.add("line", splits, 2, 2, lines)
    local.add("tokens", 2)
    local.add("weights", splits, 2)
    local.add("core_share")
    local.add("core_extra")
    local.add("up", splits, 4)
    local.add("down", splits)
    return sent, got, local


def plane_kernel(
    lines, splits, sent, got, local,
    tokens_hbm, cot_hbm, up_hbm, down_hbm,
    share_out, extra_out, up_out, down_out, up_norms, down_norms,
    acts, ups, downs, other_up, rectified, pre_grad, other_pre, turned,
    leaving, inbox, partial, spread, spread_far, share_leaving, share_got, share_sum, share_all,
    row_norms, col_norms, up_turned,
    send_sems, got_sems, local_sems,
):
    rows, width = tokens_hbm.shape
    depth, units = up_hbm.shape
    mine = units // 4
    step = mine // splits
    wide = 2 * depth
    half = rows // 2
    part = half // 4
    near = lines // 2
    mid = width // 2

    x = lax.axis_index("rep")
    fs = lax.axis_index("fs")
    core = lax.axis_index("tp")
    z, y = fs // 2, fs % 2
    me = 2 * x + y
    at_x, at_y, at_far = 2 * (1 - x) + y, 2 * x + 1 - y, 2 * (1 - x) + 1 - y
    to_x = (1 - x, fs, core)
    to_y = (x, 2 * z + 1 - y, core)
    to_far = (1 - x, 2 * z + 1 - y, core)
    to_core = (x, fs, 1 - core)
    to_up = (x, fs + 2, core)
    to_down = (x, fs - 2, core)
    has_up, has_down = z < lines - 1, z > 0
    middle = jnp.logical_and(has_up, has_down)
    end = jnp.logical_not(middle)
    pending = []

    def when(cond, act):
        if cond is None:
            act()
        else:
            pl.when(cond)(act)

    def remote(src, dst, to, key, *index, got_key=None):
        return pltpu.make_async_remote_copy(
            src_ref=src, dst_ref=dst,
            send_sem=send_sems.at[sent.at(key, *index)],
            recv_sem=got_sems.at[got.at(got_key or key, *index)],
            device_id=to, device_id_type=MESH,
        )

    def send(src, dst, to, key, *index, cond=None, got_key=None):
        copy = remote(src, dst, to, key, *index, got_key=got_key)
        when(cond, copy.start)
        pending.append((cond, copy))

    def arrived(dst, key, *index):
        return pltpu.make_async_remote_copy(
            src_ref=dst, dst_ref=dst, send_sem=send_sems.at[0],
            recv_sem=got_sems.at[got.at(key, *index)],
            device_id=to_core, device_id_type=MESH,
        )

    def fetch(src, dst, key, *index):
        copy = pltpu.make_async_copy(src, dst, local_sems.at[local.at(key, *index)])
        copy.start()
        return copy

    def up_piece(k, line, side):
        return ups.at[k, line, pl.ds(pl.multiple_of(side * depth, depth), depth), :]

    def down_piece(k, line, side):
        return downs.at[k, line, :, pl.ds(pl.multiple_of(side * depth, depth), depth)]

    def piece(w, k, line, side):
        return (up_piece, down_piece)[w](k, line, side)

    def own(w, owner, k):
        at = pl.ds(pl.multiple_of(owner * mine + k * step, step), step)
        return up_hbm.at[:, at] if w == 0 else down_hbm.at[at, :]

    def band(t, owner, first, count):
        return acts.at[t, pl.ds(pl.multiple_of(owner * rows + first, part), count), :]

    gets = {}
    for k in range(splits):
        for w in range(2):
            gets[k, w] = fetch(own(w, me, k), piece(w, k, z, y), "weights", k, w)
        if k == 0:
            for t, src in ((0, tokens_hbm), (1, cot_hbm)):
                gets[t] = fetch(src, band(t, me, 0, rows), "tokens", t)

    others = [
        (i, j, d, ((x + i) % 2, (z + d) % lines * 2 + (y + j) % 2, core))
        for i in range(2)
        for j in range(2)
        for d in range(lines)
        if i or j or d
    ]
    barrier = pltpu.get_barrier_semaphore()
    for to in (to_x, to_y, to_core):
        pl.semaphore_signal(barrier, inc=1, device_id=to, device_id_type=MESH)
    for cond, to in ((has_up, to_up), (has_down, to_down)):

        @pl.when(cond)
        def _():
            pl.semaphore_signal(barrier, inc=1, device_id=to, device_id_type=MESH)

    pl.semaphore_wait(barrier, 3 + has_up.astype(jnp.int32) + has_down.astype(jnp.int32))

    def pair_send(k):
        for w in range(2):
            send(own(w, at_y, k), piece(w, k, z, y), to_y, "pair", k, w)

    def line_send(k, side):
        for w in range(2):
            ref = piece(w, k, z, side)
            send(ref, ref, to_up, "line_up", k, w, side, z, cond=has_up, got_key="line")
            send(ref, ref, to_down, "line_down", k, w, side, z, cond=has_down, got_key="line")

    def pair_wait(k):
        for w in range(2):
            arrived(piece(w, k, z, 1 - y), "pair", k, w).wait_recv()

    first = core * half

    cuts = ((0, part), (part, half - part))

    def cut(t, owner, p):
        return band(t, owner, first + cuts[p][0], cuts[p][1])

    def near_send(t):
        for p in range(2):
            ref = cut(t, me, p)
            send(ref, ref, to_x, "near_x", t, p)
            ref = cut(t, me, 1 - p)
            send(ref, ref, to_y, "near_y", t, 1 - p)

    def relay(t):
        ref = cut(t, at_x, 0)
        arrived(ref, "near_x", t, 0).wait_recv()
        send(ref, ref, to_y, "far", t, 0)
        ref = cut(t, at_y, 1)
        arrived(ref, "near_y", t, 1).wait_recv()
        send(ref, ref, to_x, "far", t, 1)

    def near_wait(t):
        arrived(cut(t, at_x, 1), "near_x", t, 1).wait_recv()
        arrived(cut(t, at_y, 0), "near_y", t, 0).wait_recv()
        for i, owner in enumerate((at_x, at_y)):
            ref = band(t, owner, first, half)
            send(ref, ref, to_core, "core_tokens", t, i)

    def far_wait(t):
        for p in range(2):
            arrived(cut(t, at_far, p), "far", t, p).wait_recv()
        ref = band(t, at_far, first, half)
        send(ref, ref, to_core, "core_tokens", t, 2)

    def core_wait(t, *which):
        for i in which:
            owner = (at_x, at_y, at_far)[i]
            arrived(band(t, owner, (1 - core) * half, half), "core_tokens", t, i).wait_recv()

    def core_up_send(k, line, cond):
        other = (1 - core) * near
        inside = jnp.logical_and(line >= other, line < other + near)
        if cond is not None:
            inside = jnp.logical_and(inside, cond)
        send(ups.at[k, line], other_up.at[k, line], to_core, "core_up", k, line, cond=inside)

    def beside(d):
        below, above = z - d, z + d
        return (
            (lax.rem(below + lines, lines), below >= 0, has_up, to_up, "line_up"),
            (lax.rem(above, lines), above < lines, has_down, to_down, "line_down"),
        )

    def gather_step(k, d, who=None):
        for line, cond, onward, to, key in beside(d):
            if who is not None:
                cond = jnp.logical_and(cond, who)
            for w in range(2):
                for side in (y, 1 - y):
                    ref = piece(w, k, line, side)
                    when(cond, arrived(ref, "line", k, w, side, line).wait_recv)
                    send(
                        ref, ref, to, key, k, w, side, line,
                        cond=jnp.logical_and(cond, onward), got_key="line",
                    )
            core_up_send(k, line, cond)

    def hidden(k, owner):
        at = pl.ds(pl.multiple_of(owner * rows, rows), rows)
        r = jnp.maximum(dot(acts[0, at, :], ups[k].reshape(width, step), 1, 0), 0.0)
        rectified[at, :] = r
        turned[k, 1, :, at] = (r * r).astype(jnp.bfloat16).T

    def gradient(k, owner):
        at = pl.ds(pl.multiple_of(owner * rows, rows), rows)
        act_grad = dot(acts[1, at, :wide], downs[k, 0], 1, 1)
        for line in range(1, lines):
            act_grad += dot(acts[1, at, line * wide : (line + 1) * wide], downs[k, line], 1, 1)
        g = (2.0 * rectified[at, :] * act_grad).astype(jnp.bfloat16)
        pre_grad[k, at, :] = g
        turned[k, 0, :, at] = g.T

    def compute(k, owner):
        hidden(k, owner)
        gradient(k, owner)

    def every(act, k):
        def body(owner, carry):
            act(k, owner)
            return carry

        lax.fori_loop(0, 4, body, 0)

    def hand_over(k):
        send(pre_grad.at[k], other_pre.at[k], to_core, "core_pre", k)

    def term(k, w, owner):
        cols = pl.ds(pl.multiple_of(owner * wide, wide), wide)
        return dot(turned[k, w], acts[w, :, cols], 1, 0)

    def route(k, w, t):
        turn = lax.rem(t // (lines - 1) + z // near, 2)
        j = lax.rem(t, lines - 1)
        owner = (1 - turn) * (lines - 1 - j) + turn * j
        sign = 1 - 2 * turn
        cond = (owner - z) * sign > 0
        source = z - sign
        has_in = jnp.logical_and(source >= 0, source < lines)
        box = inbox.at[turn, k, w, owner]
        out = leaving.at[k, w, owner]
        copy = pltpu.make_async_remote_copy(
            src_ref=out, dst_ref=box,
            send_sem=send_sems.at[sent.at("reduce", turn, k, w, owner)],
            recv_sem=got_sems.at[got.at("reduce", turn, k, w, owner)],
            device_id=(x, fs + 2 * sign, core), device_id_type=MESH,
        )
        return owner, cond, has_in, box, out, copy

    def pieces(k, turn):
        def body(u, carry):
            w = 1 - lax.rem(u, 2)
            t = turn * (lines - 1) + u // 2
            owner, cond, has_in, box, out, copy = route(k, w, t)

            @pl.when(cond)
            def _():
                partial[...] = term(k, w, owner)

                @pl.when(has_in)
                def _():
                    copy.wait_recv()
                    out[...] = (partial[...] + box[...].astype(jnp.float32)).astype(jnp.bfloat16)

                @pl.when(jnp.logical_not(has_in))
                def _():
                    out[...] = partial[...].astype(jnp.bfloat16)

                copy.start()

            return carry

        lax.fori_loop(0, 2 * (lines - 1), body, 0)

    def pieces_end(k, w):
        def body(t, carry):
            _, cond, _, _, _, copy = route(k, w, t)
            pl.when(cond)(copy.wait_send)
            return carry

        lax.fori_loop(0, 2 * (lines - 1), body, 0)

    def spread_copies(k, w):
        here, there, near_ref = spread.at[w, me, k], spread_far.at[k, w], spread.at[w, at_y, k]
        return (
            remote(there, here, to_y, "spread_y", k, w),
            remote(here, here, to_x, "spread_x", k, w, 0),
            remote(near_ref, near_ref, to_x, "spread_x", k, w, 1),
        )

    def reduce_own(k, w):
        partial[...] = term(k, w, z)
        for turn, cond in ((0, has_down), (1, has_up)):
            box = inbox.at[turn, k, w, z]
            wait = arrived(box, "reduce", turn, k, w, z)

            @pl.when(cond)
            def _():
                wait.wait_recv()
                partial[...] += box[...].astype(jnp.float32)

        if w == 1:
            square = partial[...] * partial[...]
            folded = square[:, :128]
            for at in range(128, wide, 128):
                folded += square[:, at : at + 128]
            row_norms[z, me, :, k * step : (k + 1) * step] = jnp.sum(folded.T, axis=0, keepdims=True)
        here, there = spread.at[w, me, k], spread_far.at[k, w]
        there[...] = partial[:, pl.ds(pl.multiple_of((1 - y) * depth, depth), depth)].astype(jnp.bfloat16)
        here[...] = partial[:, pl.ds(pl.multiple_of(y * depth, depth), depth)].astype(jnp.bfloat16)
        to_near, to_side, _ = spread_copies(k, w)
        to_near.start()
        to_side.start()

    def spread_relay(k, w):
        arrived(spread.at[w, at_y, k], "spread_y", k, w).wait_recv()
        spread_copies(k, w)[2].start()

    def spread_wait(k, w):
        arrived(spread.at[w, at_x, k], "spread_x", k, w, 0).wait_recv()
        arrived(spread.at[w, at_far, k], "spread_x", k, w, 1).wait_recv()

    def norm_copies():
        ref = row_norms.at[z, me]
        for i, j, d, to in others:
            yield pltpu.make_async_remote_copy(
                src_ref=ref, dst_ref=ref,
                send_sem=send_sems.at[sent.at("norms", i, j, d)],
                recv_sem=got_sems.at[got.at("norms", z, me)],
                device_id=to, device_id_type=MESH,
            )

    def norms_send():
        for copy in norm_copies():
            copy.start()

    def norms_end():
        for i, j, d, _ in others:
            line, owner = (z + d) % lines, 2 * ((x + i) % 2) + (y + j) % 2
            arrived(row_norms.at[line, owner], "norms", line, owner).wait_recv()
        for owner in range(4):
            total = row_norms[0, owner, 0:1, :]
            for line in range(1, lines):
                total += row_norms[line, owner, 0:1, :]
            down_norms[:, owner * mine : (owner + 1) * mine] = total

    def deliver(k):
        spread_wait(k, 1)
        copies = [fetch(spread.at[1, :, k], down_out.at[:, k], "down", k)]
        spread_wait(k, 0)
        total = jnp.zeros((8, depth), jnp.float32) if k == 0 else col_norms[0]
        for owner in range(4):
            block = spread[0, owner, k]
            wider = block.astype(jnp.float32)
            total += jnp.sum((wider * wider).reshape(step // 8, 8, depth), axis=0)
            at = pl.ds(owner * mine + k * step, step)
            up_turned[:, at] = block.T
            copies.append(fetch(up_turned.at[:, at], up_out.at[:, at], "up", k, owner))
        if k == splits - 1:
            total = jnp.broadcast_to(jnp.sum(total, axis=0, keepdims=True), (8, depth))
        col_norms[0] = total
        if k == splits - 1:
            send(col_norms.at[0], col_norms.at[1], to_core, "core_norms")
        return copies

    def col_end():
        arrived(col_norms.at[1], "core_norms").wait_recv()
        up_norms[...] = col_norms[0, 0:1, :] + col_norms[1, 0:1, :]

    def share_add(k):
        arrived(other_pre.at[k], "core_pre", k).wait_recv()
        for i in range(near):
            line = core * near + i
            arrived(other_up.at[k, line], "core_up", k, line).wait_recv()

        def body(owner, carry):
            at = pl.ds(pl.multiple_of(owner * rows, rows), rows)
            for i in range(near):
                line = core * near + i
                cols = slice(i * wide, (i + 1) * wide)
                total = dot(pre_grad[k, at, :], ups[k, line], 1, 1)
                total += dot(other_pre[k, at, :], other_up[k, line], 1, 1)
                share_all[at, cols] = total if k == 0 else share_all[at, cols] + total
            return carry

        lax.fori_loop(0, 4, body, 0)

    def share_send():
        share_add(splits - 1)
        for j, (owner, to) in enumerate(((at_far, to_far), (at_x, to_x), (at_y, to_y))):
            at = pl.ds(pl.multiple_of(owner * rows, rows), rows)
            share_leaving[j] = share_all[at, :].astype(jnp.bfloat16)
            send(share_leaving.at[j], share_got.at[j], to, "share", j)
        share_sum[...] = share_all[pl.ds(pl.multiple_of(me * rows, rows), rows), :]

    share_keys = ("core_share", "core_extra")

    def share_end():
        for j in range(3):
            arrived(share_got.at[j], "share", j).wait_recv()
            if j:
                share_sum[...] += share_got[j].astype(jnp.float32)
        copies = []
        for src, ref, key in zip((share_sum, share_got.at[0]), (share_out, extra_out), share_keys, strict=True):
            place = ref.at[:, pl.ds(pl.multiple_of(core * mid, mid), mid)]
            send(src, place, to_core, key)
            copies.append(fetch(src, place, key))
        return copies

    def line_own(k, side):
        if side is not y:
            pair_wait(k)
        line_send(k, side)
        if side is not y:
            core_up_send(k, z, None)

    def gets_wait(k):
        for w in range(2):
            gets[k, w].wait()

    def own_pair(k):
        for w in (1, 0):
            if k:
                spread_relay(k - 1, w)
            reduce_own(k, w)
            if w == 1 and k == splits - 1:
                norms_send()

    def finish(k):
        pieces(k, 1)
        own_pair(k)

    other = 1 - y
    pair_send(0)
    gets_wait(0)
    line_own(0, y)
    gets[0].wait()
    near_send(0)
    if splits > 1:
        pair_send(1)
    gets[1].wait()
    near_send(1)
    for k in range(2, splits):
        pair_send(k)
    line_own(0, other)
    if splits > 1:
        gets_wait(1)
        line_own(1, y)
    relay(0)
    gather_step(0, 1)
    near_wait(0)
    for d in range(2, lines - 1):
        gather_step(0, d)
    if splits > 1:
        line_own(1, other)
        gather_step(1, 1, middle)
    relay(1)
    for k in range(2, splits):
        gets_wait(k)
        line_own(k, y)
    near_wait(1)
    gather_step(0, lines - 1)
    core_wait(0, 0, 1)
    core_wait(1, 0, 1)
    if splits > 1:
        for d in range(2, lines - 1):
            gather_step(1, d, middle)
    for owner in (me, at_x, at_y):
        compute(0, owner)
    for k in range(2, splits):
        line_own(k, other)
    far_wait(0)
    core_wait(0, 2)
    hidden(0, at_far)
    far_wait(1)
    core_wait(1, 2)
    gradient(0, at_far)
    hand_over(0)

    grads = [(k, w) for k in range(splits) for w in range(2)]
    jobs = []
    for k in range(splits):
        jobs.append(functools.partial(pieces, k, 0))
        if k:
            jobs.append(functools.partial(finish, k - 1))
    jobs.append(functools.partial(pieces, splits - 1, 1))

    def end_pieces(k):
        @pl.when(end)
        def _():
            pieces(k, 0)

    end_pieces(0)
    for k in range(1, splits):
        if k + 1 < splits:
            for d in range(1, lines - 1):
                gather_step(k + 1, d, middle)
        share_add(k - 1)
        for d in range(1, lines):
            gather_step(k, d, end)
        every(compute, k)
        hand_over(k)
        end_pieces(k)
    share_send()

    @pl.when(middle)
    def _():
        for job in jobs:
            job()

    @pl.when(end)
    def _():
        for k in range(splits - 1):
            own_pair(k)

    ends = share_end()
    for k in range(splits - 2):
        ends += deliver(k)
    own_pair(splits - 1)
    if splits > 1:
        ends += deliver(splits - 2)
    for w in (1, 0):
        spread_relay(splits - 1, w)
    norms_end()
    ends += deliver(splits - 1)
    col_end()
    for ref in (share_out, extra_out):
        arrived(ref.at[:, pl.ds(pl.multiple_of((1 - core) * mid, mid), mid)], share_keys[ref is extra_out]).wait_recv()
    for cond, copy in pending:
        when(cond, copy.wait_send)
    for copy in norm_copies():
        copy.wait_send()
    for k, w in grads:
        pieces_end(k, w)
        for copy in spread_copies(k, w):
            copy.wait_send()
    for copy in ends:
        copy.wait()


def plane_fits(inputs, up_weight, down_weight):
    reps, groups, cores = (lax.axis_size(axis) for axis in ("rep", "fs", "tp"))
    if reps != 2 or cores != 2 or groups % 4:
        return False
    rows, width = inputs.shape
    depth, units = up_weight.shape
    step = units // 4 // SPLITS
    even = rows % 128 == 0 and depth % 128 == 0 and step % 128 == 0 and width == groups * depth
    held = 2 * 4 * rows * width * 2 + 4 * (units // 4) * width * 2
    return even and held <= 16 * 2**20


def plane_plan(inputs, cotangent, up_weight, down_weight):
    groups = lax.axis_size("fs")
    lines, splits = groups // 2, SPLITS
    rows, width = inputs.shape
    depth, units = up_weight.shape
    step = units // 4 // splits
    wide = 2 * depth
    plane = 4 * rows
    sent, got, local = plane_slots(lines, splits)
    narrow, full = jnp.bfloat16, jnp.float32
    anywhere = pl.BlockSpec(memory_space=pl.ANY)
    share, extra, up, down, norms_up, norms_down = pl.pallas_call(
        functools.partial(plane_kernel, lines, splits, sent, got, local),
        out_shape=(
            jax.ShapeDtypeStruct((rows, width), full),
            jax.ShapeDtypeStruct((rows, width), narrow),
            jax.ShapeDtypeStruct((depth, units), narrow),
            jax.ShapeDtypeStruct((4, splits, step, depth), narrow),
            jax.ShapeDtypeStruct((1, depth), full),
            jax.ShapeDtypeStruct((1, units), full),
        ),
        in_specs=[anywhere] * 4,
        out_specs=(anywhere,) * 4 + (pl.BlockSpec(memory_space=pltpu.VMEM),) * 2,
        scratch_shapes=[
            pltpu.VMEM((2, plane, width), narrow),
            pltpu.VMEM((splits, lines, wide, step), narrow),
            pltpu.VMEM((splits, lines, step, wide), narrow),
            pltpu.VMEM((splits, lines, wide, step), narrow),
            pltpu.VMEM((plane, step), full),
            pltpu.VMEM((splits, plane, step), narrow),
            pltpu.VMEM((splits, plane, step), narrow),
            pltpu.VMEM((splits, 2, step, plane), narrow),
            pltpu.VMEM((splits, 2, lines, step, wide), narrow),
            pltpu.VMEM((2, splits, 2, lines, step, wide), narrow),
            pltpu.VMEM((step, wide), full),
            pltpu.VMEM((2, 4, splits, step, depth), narrow),
            pltpu.VMEM((splits, 2, step, depth), narrow),
            pltpu.VMEM((3, rows, width // 2), narrow),
            pltpu.VMEM((3, rows, width // 2), narrow),
            pltpu.VMEM((rows, width // 2), full),
            pltpu.VMEM((plane, width // 2), full),
            pltpu.VMEM((lines, 4, 1, units // 4), full),
            pltpu.VMEM((2, 8, depth), full),
            pltpu.VMEM((depth, units), narrow),
            pltpu.SemaphoreType.DMA((sent.size,)),
            pltpu.SemaphoreType.DMA((got.size,)),
            pltpu.SemaphoreType.DMA((local.size,)),
        ],
        compiler_params=pltpu.CompilerParams(
            collective_id=0, has_side_effects=True, vmem_limit_bytes=63 * 2**20
        ),
        name="plane",
    )(inputs, cotangent, up_weight, down_weight)
    grad_up = up.astype(full)
    share = share + extra.astype(full)
    grad_down = down.reshape(units, depth).astype(full)
    return (share, grad_up, grad_down, norms_up.reshape(depth), norms_down.reshape(units))


def shards(inputs, cotangent, up_weight, down_weight):
    tokens = inputs.size * lax.axis_size("fs") // lax.axis_size("tp")
    weights = up_weight.size * lax.axis_size("fs")
    plan = token_plan if tokens <= weights else weight_plan
    if plane_fits(inputs, up_weight, down_weight):
        plan = plane_plan
    return plan(inputs, cotangent, up_weight, down_weight)


def solution(mesh):
    return jax.shard_map(
        shards,
        mesh=mesh,
        in_specs=(P(("rep", "fs"), None), P(("rep", "fs"), None), P("fs", "tp"), P("tp", "fs")),
        out_specs=(P(("rep", "fs"), None), P("fs", "tp"), P("tp", "fs"), P("fs"), P("tp")),
        check_vma=False,
    )
```
